32 devices in a mesh: sp: 8 (over z, core), tp: 4 (over y, x).
Axes of the slice: x: 2, y: 2, z: 4, core: 2. Of those that a mesh axis runs over, the one named last changes fastest.
Arguments:
- query_proj: bfloat16 [2048, 2048], P('sp', 'tp'), may hold values from -4 to 4
- key_proj: bfloat16 [2048, 1024], P('sp', 'tp'), may hold values from -4 to 4
- value_proj: bfloat16 [2048, 1024], P('sp', 'tp'), may hold values from -48 to 48
- query_gain: float32 [32, 64], P('tp'), may hold values from 1 to 6
- key_gain: float32 [16, 64], P('tp'), may hold values from 1 to 6
- residual: bfloat16 [2048, 2048], P('sp', 'tp'), may hold values from -48 to 48
- out_weight: bfloat16 [2048, 2048], P(None, 'tp'), may hold values from -0.125 to 0.125
- route_expert: int32 [2048, 8], P('sp'), may hold values from 0 to 15, all different within a row; in each aligned block of 256 rows (0 to 255, 256 to 511, ...) at most 192 rows name the same one
- route_weight: float32 [2048, 8], P('sp'), may hold values from 0.25 to 1.25
- expert_gate: bfloat16 [32, 2048, 256], P(('sp', 'tp')), may hold values from -0.125 to 0.125
- expert_up: bfloat16 [32, 2048, 256], P(('sp', 'tp')), may hold values from -0.125 to 0.125
- expert_down: bfloat16 [32, 256, 2048], P(('sp', 'tp')), may hold values from -0.25 to 0.25
Outputs:
- block_out: bfloat16 [2048, 2048], P('sp', 'tp')
The draws below stay inside these ranges and needn't reach their ends.
Inputs may be any that keep to these rules, and one draw needn't show every extreme that they name: `route_expert`: A row names 8 different experts; among the rows of one index of sp no expert is named by more than 192 rows, a bound that some block reaches of them.
All inputs are finite; a program needn't handle non-finite values.
Results may differ from the reference program's by a relative error of at most 0.012.
The reference program's roundings to bfloat16 on the way count: a program that leaves them out, or rounds other values in their place, can miss the bound.
Values may be sent and summed in bfloat16 or wider, within the bound.
A program may use at most 64 MiB of HBM per device.

```python
import math
import jax
import jax.numpy as jnp
import numpy as np
from jax import lax

D = 2048
HEADS = 32
KV_HEADS = 16
HEAD_DIM = 64
FF = 512
TOP_K = 8
GRID_W = 64
TOK_DEV = 256
TOKENS = 2048
EXPERTS = 16
CAP = 192
N_SP = 8


def attention_pair(key):
    seeded = jax.random.fold_in(key, 11)
    first_key, second_key = jax.random.split(seeded, 2)
    key_rows = jnp.clip(jax.random.normal(first_key, (TOKENS, KV_HEADS, HEAD_DIM), jnp.float32), -4.0, 4.0)
    query_rows = jnp.clip(jax.random.normal(second_key, (TOKENS, HEADS, HEAD_DIM), jnp.float32), -4.0, 4.0)
    return (query_rows.reshape(TOKENS, HEADS * HEAD_DIM), key_rows.reshape(TOKENS, KV_HEADS * HEAD_DIM))


def draw_query_proj(key, part):
    return attention_pair(key)[0].astype(jnp.bfloat16)


def draw_key_proj(key, part):
    return attention_pair(key)[1].astype(jnp.bfloat16)


def draw_query_gain(key, part):
    seeded = jax.random.fold_in(key, 31)
    return jnp.exp(jax.random.uniform(seeded, (HEADS, HEAD_DIM), jnp.float32, 0.0, 0.6931))


def draw_key_gain(key, part):
    seeded = jax.random.fold_in(key, 37)
    return jnp.exp(jax.random.uniform(seeded, (KV_HEADS, HEAD_DIM), jnp.float32, 0.0, 0.6931))


def draw_residual(key, part):
    seeded = jax.random.fold_in(key, 41)
    first_key, second_key = jax.random.split(seeded, 2)
    fraction = jnp.arange(D, dtype=jnp.float32) / D
    row_scale = jnp.exp(jax.random.uniform(second_key, (TOKENS, 1), jnp.float32, -0.6931, 1.6094))
    column_scale = 0.6 * 3.0 ** fraction
    pattern = jnp.clip(jax.random.normal(first_key, (TOKENS, D), jnp.float32), -4.0, 4.0)
    return (pattern * row_scale * column_scale[None, :]).astype(jnp.bfloat16)


def block_scale(rng, extent, pieces, low, top_value):
    def one(dim, shards_of):
        steps = jax.random.uniform(jax.random.fold_in(jax.random.fold_in(rng, 6), dim), (shards_of,), jnp.float32, low / len(pieces), top_value / len(pieces))
        return jnp.repeat(jnp.exp(steps), extent[dim] // shards_of).reshape((-1,) + (1,) * (len(extent) - dim - 1))

    factor_of = one(*pieces[0])
    for cut in pieces[1:]:
        factor_of = factor_of * one(*cut)
    return factor_of


def assign_block(key, own, number, rows, amount, top, most, skew):
    ranking = jax.random.permutation(key, amount)
    crowded, usual = shares(amount, rows * top, most, skew, True), shares(amount, rows * top, most, skew, False)
    places = jnp.arange(amount)

    def named(sizes, turn):
        used = int((sizes > 0).sum())
        fixed = max(1, used // 4)
        passed = fixed + (places - fixed + turn * (used - fixed)) % max(1, amount - fixed)
        return jnp.zeros((amount,), jnp.int32).at[ranking[jnp.where(places < fixed, places, passed)]].set(jnp.asarray(sizes, jnp.int32))

    sizes = jnp.where(number % 4 == 0, named(crowded, number // 4), named(usual, number - number // 4 - 1))
    mixed = jax.random.permutation(jax.random.fold_in(own, 3), amount)
    giver, receiver = mixed[0:amount // 2 * 2:2], mixed[1:amount // 2 * 2:2]
    margin = jnp.minimum(sizes[giver] - 1, most - sizes[receiver]) // 2
    margin = jnp.where((giver == ranking[0]) | (receiver == ranking[0]) | (sizes[receiver] == 0), 0, jnp.maximum(margin, 0))
    passed = jax.random.randint(jax.random.fold_in(own, 4), (amount // 2,), 0, 1 << 20) % (margin + 1)
    sizes = sizes.at[giver].add(-passed).at[receiver].add(passed)
    labels = jnp.searchsorted(jnp.cumsum(sizes), jnp.arange(rows * top), side="right").astype(jnp.int32)
    grid = labels.reshape(top, rows).T
    grid = grid[jax.random.permutation(jax.random.fold_in(own, 1), rows)]
    turn = jax.random.randint(jax.random.fold_in(own, 2), (rows, 1), 0, top)
    return jnp.take_along_axis(grid, (jnp.arange(top)[None, :] + turn) % top, axis=1)


def shares(count, total, limit, skew, full):
    weights = [(1 << 20) // math.isqrt(grade ** skew) + 1 for grade in range(1, count + 1)]
    largest = limit if full else min(limit, max(-(-total // count), total * weights[0] // sum(weights)))
    least = 1 if total - largest >= count - 1 else 0
    holding, spare = [largest] + [least] * (count - 1), total - largest - least * (count - 1)
    while spare > 0:
        movable = [i for i in range(1, count) if holding[i] < largest] or [i for i in range(1, count) if holding[i] < limit]
        pool, remaining = sum([weights[i] for i in movable]), spare
        for i in movable:
            more = min(limit - holding[i], max(1, remaining * weights[i] // pool), spare)
            holding[i] = holding[i] + more
            spare = spare - more
    return np.array(holding)


def centred(own_key, shape, deviation, most, cuts=(), kind=jnp.bfloat16):
    level = block_scale(own_key, shape, cuts, -0.22, 0.18) if cuts else 1.0
    entries = jax.random.normal(own_key, shape, jnp.float32) * deviation * level
    return jnp.minimum(jnp.maximum(entries, -most), most).astype(kind)


def setup_inputs(seed: int = 0) -> dict:
    key_of = jax.random.split(jax.random.key(seed), 13)
    query_proj = draw_query_proj(jax.random.fold_in(key_of[12], 71), 0)
    key_proj = draw_key_proj(jax.random.fold_in(key_of[12], 71), 0)
    value_proj = centred(key_of[2], (TOKENS, KV_HEADS * HEAD_DIM), 8.0, 48.0, ((0, 8), (1, 4)))
    query_gain = draw_query_gain(jax.random.fold_in(key_of[12], 71), 0)
    key_gain = draw_key_gain(jax.random.fold_in(key_of[12], 71), 0)
    residual = draw_residual(jax.random.fold_in(key_of[12], 71), 0)
    out_weight = centred(key_of[6], (HEADS * HEAD_DIM, D), (HEADS * HEAD_DIM) ** -0.5, 0.125, ((1, 4),))
    route_expert_keys = jax.random.split(jax.random.fold_in(key_of[7], 1), TOKENS // TOK_DEV)
    route_expert_turns = jax.random.permutation(jax.random.fold_in(key_of[7], 3), TOKENS // TOK_DEV)
    route_expert = jax.vmap(lambda own, number: assign_block(jax.random.fold_in(key_of[7], 2), own, number, TOK_DEV, EXPERTS, TOP_K, CAP, 1))(route_expert_keys, route_expert_turns).reshape((TOKENS, TOP_K))
    route_weight = jnp.clip(0.25 + 1.0 * jax.random.uniform(key_of[8], (TOKENS, TOP_K), jnp.float32) ** block_scale(key_of[8], (TOKENS, TOP_K), ((0, 8),), -0.2, 0.2), 0.25, 1.25)
    expert_gate = centred(key_of[9], (2 * EXPERTS, D, FF // 2), D ** -0.5, 0.125, ((0, 32),))
    expert_up = centred(key_of[10], (2 * EXPERTS, D, FF // 2), D ** -0.5, 0.125, ((0, 32),))
    expert_down = centred(key_of[11], (2 * EXPERTS, FF // 2, D), FF ** -0.5, 0.25, ((0, 32),))
    return dict(query_proj=query_proj, key_proj=key_proj, value_proj=value_proj, query_gain=query_gain, key_gain=key_gain, residual=residual, out_weight=out_weight, route_expert=route_expert, route_weight=route_weight, expert_gate=expert_gate, expert_up=expert_up, expert_down=expert_down)


EPSILON = 1e-06
ROPE_BASE = 10000.0

def rotation_tables(offset, count):
    pair_count = HEAD_DIM // 4
    position = offset + jnp.arange(count, dtype=jnp.int32)
    grid_row = (position // GRID_W).astype(jnp.float32)
    grid_col = (position % GRID_W).astype(jnp.float32)
    inverse = ROPE_BASE ** (-jnp.arange(pair_count, dtype=jnp.float32) / pair_count)
    angles = jnp.stack([grid_row[:, None] * inverse, grid_col[:, None] * inverse], axis=1)
    return (jnp.cos(angles), jnp.sin(angles))

def rotate(vectors, cosine_table, sine_table):
    pair_count = HEAD_DIM // 4
    shaped = vectors.reshape(vectors.shape[:-1] + (2, 2, pair_count))
    first_half = shaped[..., 0, :]
    second_half = shaped[..., 1, :]
    cosine_row = cosine_table[:, None]
    sine_row = sine_table[:, None]
    turned = jnp.stack([first_half * cosine_row - second_half * sine_row, first_half * sine_row + second_half * cosine_row], axis=-2)
    return turned.reshape(vectors.shape)

def head_norm(vectors, gain):
    scaled = vectors.astype(jnp.float32)
    scaled = scaled * lax.rsqrt(lax.optimization_barrier(jnp.mean(scaled * scaled, axis=-1, keepdims=True)) + EPSILON)
    return scaled * gain.astype(jnp.float32)

def slot_layout(choices, weights):
    token_count = choices.shape[0]
    flat_choice = choices.reshape(token_count * TOP_K).astype(jnp.int32)
    onehot = (flat_choice[:, None] == jnp.arange(EXPERTS, dtype=jnp.int32)[None, :]).astype(jnp.int32)
    earlier = jnp.cumsum(onehot, axis=0) - onehot
    slot_rank = lax.optimization_barrier(jnp.sum(earlier * onehot, axis=1))
    position = (flat_choice * CAP + slot_rank).astype(jnp.int32)
    owner = (jnp.arange(token_count * TOP_K, dtype=jnp.int32) // TOP_K).astype(jnp.int32)
    slot_token = jnp.full((EXPERTS * CAP,), token_count, jnp.int32).at[position].set(owner)
    slot_weight = jnp.zeros((EXPERTS * CAP,), jnp.float32).at[position].set(weights.reshape(token_count * TOP_K).astype(jnp.float32))
    return (slot_token, slot_weight)

def reference(query_proj, key_proj, value_proj, query_gain, key_gain, residual, out_weight, route_expert, route_weight, expert_gate, expert_up, expert_down):
    token_total = query_proj.shape[0]
    group_size = HEADS // KV_HEADS
    cosine_table, sine_table = rotation_tables(0, token_total)
    query_rot = rotate(head_norm(query_proj.reshape(token_total, HEADS, HEAD_DIM), query_gain), cosine_table, sine_table).astype(jnp.bfloat16)
    key_rot = rotate(head_norm(key_proj.reshape(token_total, KV_HEADS, HEAD_DIM), key_gain), cosine_table, sine_table).astype(jnp.bfloat16)
    value_heads = value_proj.reshape(token_total, KV_HEADS, HEAD_DIM)
    block_len = math.gcd(token_total, 1024)

    def one_head(head_index):
        query_head = lax.dynamic_index_in_dim(query_rot, head_index, 1, keepdims=False)
        key_head = lax.dynamic_index_in_dim(key_rot, head_index // group_size, 1, keepdims=False)
        value_head = lax.dynamic_index_in_dim(value_heads, head_index // group_size, 1, keepdims=False)
        query_blocks = query_head.reshape(token_total // block_len, block_len, HEAD_DIM)

        def one_block(query_block):
            scores = jnp.dot(query_block, key_head.T, preferred_element_type=jnp.float32) * HEAD_DIM ** (-0.5)
            weights = jnp.exp(scores - lax.optimization_barrier(jnp.max(scores, axis=-1, keepdims=True))).astype(jnp.bfloat16)
            weight_sum = lax.optimization_barrier(jnp.sum(weights.astype(jnp.float32), axis=-1, keepdims=True))
            summed = jnp.dot(weights, value_head, preferred_element_type=jnp.float32)
            return (summed / weight_sum).astype(jnp.bfloat16)
        return lax.map(one_block, query_blocks).reshape(token_total, HEAD_DIM)
    attended = lax.map(one_head, jnp.arange(HEADS, dtype=jnp.int32))
    attended = jnp.transpose(attended, (1, 0, 2)).reshape(token_total, HEADS * HEAD_DIM)
    mixed_sum = residual.astype(jnp.float32) + jnp.dot(attended, out_weight, preferred_element_type=jnp.float32)
    mixed_rows = mixed_sum.astype(jnp.bfloat16)
    slot_token, slot_weight = jax.vmap(slot_layout)(route_expert.reshape(N_SP, TOK_DEV, TOP_K), route_weight.reshape(N_SP, TOK_DEV, TOP_K))
    source_base = (jnp.arange(N_SP, dtype=jnp.int32) * TOK_DEV)[:, None]
    global_index = jnp.where(slot_token == TOK_DEV, token_total, slot_token + source_base).astype(jnp.int32)
    grouped_rows = mixed_rows.reshape(N_SP, TOK_DEV, D)
    padded_rows = jnp.concatenate([grouped_rows, jnp.zeros((N_SP, 1, D), jnp.bfloat16)], axis=1)

    def one_expert(routed, expert_index):
        token_ids = lax.dynamic_slice_in_dim(slot_token, expert_index * CAP, CAP, 1)
        expert_rows = jax.vmap(lambda table, index: table[index])(padded_rows, token_ids).reshape(N_SP * CAP, D)
        squares = lax.optimization_barrier(jnp.mean(jnp.square(expert_rows.astype(jnp.float32)), axis=-1, keepdims=True))
        norm_scale = lax.rsqrt(squares + EPSILON)
        total = jnp.zeros((N_SP * CAP, D), jnp.float32)
        for half in range(2):
            block = 2 * expert_index + half
            gate_value = jnp.dot(expert_rows, lax.dynamic_index_in_dim(expert_gate, block, 0, keepdims=False), preferred_element_type=jnp.float32) * norm_scale
            up_value = jnp.dot(expert_rows, lax.dynamic_index_in_dim(expert_up, block, 0, keepdims=False), preferred_element_type=jnp.float32) * norm_scale
            hidden = (jax.nn.silu(gate_value) * up_value).astype(jnp.bfloat16)
            produced = jnp.dot(hidden, lax.dynamic_index_in_dim(expert_down, block, 0, keepdims=False), preferred_element_type=jnp.float32).astype(jnp.bfloat16)
            total = total + lax.optimization_barrier(produced).astype(jnp.float32)
        slot_weights = lax.dynamic_slice_in_dim(slot_weight, expert_index * CAP, CAP, 1).reshape(N_SP * CAP)
        targets = lax.dynamic_slice_in_dim(global_index, expert_index * CAP, CAP, 1).reshape(N_SP * CAP)
        routed = routed.at[targets].add(total * slot_weights[:, None])
        return (routed, None)
    routed, unused = lax.scan(one_expert, jnp.zeros((token_total + 1, D), jnp.float32), jnp.arange(EXPERTS, dtype=jnp.int32))
    return (mixed_sum + routed[:token_total]).astype(jnp.bfloat16)
```

```python
import functools
import math

import jax
import jax.numpy as jnp
from jax import lax
from jax.experimental import pallas as pl
from jax.experimental.pallas import tpu as pltpu
from jax.sharding import PartitionSpec as P

HEAD_DIM = 64
TOP_K = 8
GRID_W = 64


EPSILON = 1e-06
ROPE_BASE = 10000.0
KEY_BLOCK = 1024


def rotation_tables(offset, count):
    pair_count = HEAD_DIM // 4
    position = offset + jnp.arange(count, dtype=jnp.int32)
    grid_row = (position // GRID_W).astype(jnp.float32)
    grid_col = (position % GRID_W).astype(jnp.float32)
    inverse = ROPE_BASE ** (-jnp.arange(pair_count, dtype=jnp.float32) / pair_count)
    angles = jnp.stack([grid_row[:, None] * inverse, grid_col[:, None] * inverse], axis=1)
    return (jnp.cos(angles), jnp.sin(angles))


def rotate(vectors, cosine_table, sine_table):
    pair_count = HEAD_DIM // 4
    shaped = vectors.reshape(vectors.shape[:-1] + (2, 2, pair_count))
    first_half = shaped[..., 0, :]
    second_half = shaped[..., 1, :]
    cosine_row = cosine_table[:, None]
    sine_row = sine_table[:, None]
    turned = jnp.stack(
        [
            first_half * cosine_row - second_half * sine_row,
            first_half * sine_row + second_half * cosine_row,
        ],
        axis=-2,
    )
    return turned.reshape(vectors.shape)


def head_norm(vectors, gain):
    scaled = vectors.astype(jnp.float32)
    scaled = scaled * lax.rsqrt(jnp.mean(scaled * scaled, axis=-1, keepdims=True) + EPSILON)
    return scaled * gain


def online_update(running, query_groups, key_block, value_block):
    running_max, running_sum, running_acc = running
    scores = jnp.einsum(
        "tkgd,nkd->kgtn", query_groups, key_block, preferred_element_type=jnp.float32
    ) * HEAD_DIM ** (-0.5)
    new_max = jnp.maximum(running_max, jnp.max(scores, axis=-1))
    rescale = jnp.exp(running_max - new_max)
    weights = jnp.exp(scores - new_max[..., None]).astype(jnp.bfloat16)
    new_sum = running_sum * rescale + jnp.sum(weights.astype(jnp.float32), axis=-1)
    update = jnp.einsum("kgtn,nkd->kgtd", weights, value_block, preferred_element_type=jnp.float32)
    return (new_max, new_sum, running_acc * rescale[..., None] + update)


def local(
    query_proj,
    key_proj,
    value_proj,
    query_gain,
    key_gain,
    residual,
    out_weight,
    route_expert,
    route_weight,
    expert_gate,
    expert_up,
    expert_down,
):
    token_count = query_proj.shape[0]
    local_heads = query_gain.shape[0]
    local_kv = key_gain.shape[0]
    group_size = local_heads // local_kv
    sp_size = lax.axis_size("sp")
    tp_size = lax.axis_size("tp")
    tp_place = lax.axis_index("tp")
    offset = lax.axis_index("sp") * token_count
    cosine_table, sine_table = rotation_tables(offset, token_count)
    query_rot = rotate(
        head_norm(query_proj.reshape(token_count, local_heads, HEAD_DIM), query_gain),
        cosine_table,
        sine_table,
    ).astype(jnp.bfloat16)
    key_rot = rotate(
        head_norm(key_proj.reshape(token_count, local_kv, HEAD_DIM), key_gain),
        cosine_table,
        sine_table,
    ).astype(jnp.bfloat16)
    packed = jnp.concatenate(
        [key_rot.reshape(token_count, local_kv * HEAD_DIM), value_proj], axis=1
    )
    query_groups = query_rot.reshape(token_count, local_kv, group_size, HEAD_DIM)
    initial = (
        jnp.full((local_kv, group_size, token_count), -1e30, jnp.float32),
        jnp.zeros((local_kv, group_size, token_count), jnp.float32),
        jnp.zeros((local_kv, group_size, token_count, HEAD_DIM), jnp.float32),
    )
    incoming = lax.all_gather(packed, "sp", axis=0, tiled=True)
    incoming_len = incoming.shape[0]
    step_len = math.gcd(incoming_len, KEY_BLOCK)

    def one_step(step_index, running):
        block_rows = lax.dynamic_slice_in_dim(incoming, step_index * step_len, step_len, 0)
        key_block = block_rows[:, : local_kv * HEAD_DIM].reshape(step_len, local_kv, HEAD_DIM)
        value_block = block_rows[:, local_kv * HEAD_DIM :].reshape(step_len, local_kv, HEAD_DIM)
        return online_update(running, query_groups, key_block, value_block)

    final_max, final_sum, final_acc = lax.fori_loop(0, incoming_len // step_len, one_step, initial)
    attended = final_acc / final_sum[..., None]
    attended = jnp.transpose(attended, (2, 0, 1, 3)).reshape(token_count, local_heads * HEAD_DIM)
    attended = attended.astype(jnp.bfloat16)
    projected = jnp.dot(
        lax.all_gather(attended, "tp", axis=1, tiled=True),
        out_weight,
        preferred_element_type=jnp.float32,
    )
    mixed_sum = residual.astype(jnp.float32) + projected
    mixed_rows = mixed_sum.astype(jnp.bfloat16)
    full_rows = lax.all_gather(mixed_rows, "tp", axis=1, tiled=True)
    width_total = full_rows.shape[1]
    per_sp = tp_size // 2
    column = tp_place // 2
    experts_total = per_sp * sp_size
    capacity = 3 * token_count * TOP_K // (2 * experts_total)
    slot_count = sp_size * capacity
    flat_choice = route_expert.reshape(token_count * TOP_K)
    onehot = (flat_choice[:, None] == jnp.arange(experts_total, dtype=jnp.int32)[None, :]).astype(
        jnp.int32
    )
    earlier = jnp.cumsum(onehot, axis=0) - onehot
    slot_rank = jnp.sum(earlier * onehot, axis=1)
    mine = flat_choice % per_sp == column
    target = flat_choice // per_sp * capacity + slot_rank
    owner = jnp.arange(token_count * TOP_K, dtype=jnp.int32) // TOP_K
    slot_token = (
        jnp.full((slot_count + 1,), token_count, jnp.int32)
        .at[jnp.where(mine, target, slot_count)]
        .set(owner)[:slot_count]
    )
    padded = jnp.concatenate([full_rows, jnp.zeros((1, width_total), jnp.bfloat16)], axis=0)
    selected = padded[slot_token].reshape(sp_size, capacity, width_total)
    arrived = lax.all_to_all(selected, "sp", split_axis=0, concat_axis=0, tiled=True)
    expert_rows = arrived.reshape(slot_count, width_total)
    squares = jnp.mean(jnp.square(expert_rows.astype(jnp.float32)), axis=-1, keepdims=True)
    norm_scale = lax.rsqrt(squares + EPSILON)
    gate_value = (
        jnp.dot(expert_rows, expert_gate[0], preferred_element_type=jnp.float32) * norm_scale
    )
    up_value = jnp.dot(expert_rows, expert_up[0], preferred_element_type=jnp.float32) * norm_scale
    hidden = (jax.nn.silu(gate_value) * up_value).astype(jnp.bfloat16)
    half_result = jnp.dot(hidden, expert_down[0], preferred_element_type=jnp.float32).astype(
        jnp.bfloat16
    )
    returned = lax.all_to_all(
        half_result.reshape(sp_size, capacity, width_total),
        "sp",
        split_axis=0,
        concat_axis=0,
        tiled=True,
    )
    slot_results = returned.reshape(slot_count, width_total)
    mine_grid = mine.reshape(token_count, TOP_K)
    target_grid = target.reshape(token_count, TOP_K)
    gathered_sum = jnp.zeros((token_count, width_total), jnp.float32)
    for choice_index in range(TOP_K):
        chosen = mine_grid[:, choice_index]
        index = jnp.where(chosen, target_grid[:, choice_index], 0)
        factor = jnp.where(chosen, route_weight[:, choice_index], 0.0)
        picked = slot_results[index].astype(jnp.float32)
        gathered_sum = gathered_sum + factor[:, None] * picked
    routed = lax.psum_scatter(
        gathered_sum.astype(jnp.bfloat16), "tp", scatter_dimension=1, tiled=True
    ).astype(jnp.float32)
    return (mixed_sum + routed).astype(jnp.bfloat16)


def flip_index(index, mask):
    bit = 1
    while bit <= mask:
        if mask & bit:
            index = index + bit - 2 * bit * ((index // bit) % 2)
        bit *= 2
    return index


LANES = 128
SLOTS = 4
SEMS = 160


class Links:
    def __init__(self, send_sem, recv_sem, conditions):
        self.send_sem, self.recv_sem = send_sem, recv_sem
        self.conditions = conditions
        self.send_ids, self.recv_ids = {}, {}
        self.sent = []

    def copy(self, src, dst, device, send_key, recv_key):
        send_id = self.send_ids.setdefault(send_key, len(self.send_ids))
        recv_id = self.recv_ids.setdefault(recv_key, len(self.recv_ids))
        return pltpu.make_async_remote_copy(
            src_ref=src,
            dst_ref=dst,
            send_sem=self.send_sem.at[send_id],
            recv_sem=self.recv_sem.at[recv_id],
            device_id=device,
            device_id_type=pl.DeviceIdType.MESH,
        )

    def send(self, key, src, dst, device, recv_key=None, only=None):
        copy = self.copy(src, dst, device, key, key if recv_key is None else recv_key)
        self.when(only, copy.start)
        self.sent.append((copy, only))

    def arrived(self, key, dst, device, only=None):
        self.when(only, self.copy(dst, dst, device, "none", key).wait_recv)

    def when(self, only, act):
        if only is None:
            act()
        else:
            pl.when(self.conditions[only])(act)


def fused_kernel(
    q_ref,
    k_ref,
    v_ref,
    q_gain_ref,
    k_gain_ref,
    cos_ref,
    sin_ref,
    residual_ref,
    table_ref,
    out_weight_hbm,
    gate_hbm,
    up_hbm,
    down_hbm,
    out_ref,
    kv,
    queries,
    run_max,
    run_acc,
    attended,
    mixed,
    rows,
    out_weight,
    gate_up,
    down,
    tables,
    hid,
    hid_other,
    part_send,
    part_in,
    local_sem,
    send_sem,
    recv_sem,
):
    f32, bf16 = jnp.float32, jnp.bfloat16
    count, width = q_ref.shape
    pairs = width // LANES
    halves = pairs // 2
    hidden_units = gate_hbm.shape[2]
    capacity = hid.shape[3]
    upper_tok, lower_tok = pl.ds(0, count // 2), pl.ds(count // 2, count // 2)
    upper_cap, lower_cap = pl.ds(0, capacity // 2), pl.ds(capacity // 2, capacity // 2)

    sp_place, tp_place = lax.axis_index("sp"), lax.axis_index("tp")
    plane, core_place = sp_place // 2, sp_place % 2
    is_mid = (plane == 1) | (plane == 2)
    is_end = (plane == 0) | (plane == 3)

    def at(sp_mask, tp_mask):
        return {"sp": flip_index(sp_place, sp_mask), "tp": flip_index(tp_place, tp_mask)}

    core, near, far = at(1, 0), at(2, 0), at(6, 0)
    across = [None, at(0, 1), at(0, 2), at(0, 3)]
    across_core = [core, at(1, 1), at(1, 2)]
    links = Links(send_sem, recv_sem, {"mid": is_mid, "end": is_end})

    quarters = [flip_index(tp_place, q) * width for q in range(4)]

    def columns(q):
        return pl.ds(pl.multiple_of(quarters[q], width), width)

    loads = [
        pltpu.make_async_copy(out_weight_hbm, out_weight, local_sem.at[0]),
        pltpu.make_async_copy(
            gate_hbm.at[0], gate_up.at[:, pl.ds(0, hidden_units)], local_sem.at[1]
        ),
        pltpu.make_async_copy(
            up_hbm.at[0], gate_up.at[:, pl.ds(hidden_units, hidden_units)], local_sem.at[2]
        ),
        pltpu.make_async_copy(down_hbm.at[0, :, columns(0)], down.at[0, 0], local_sem.at[3]),
    ]

    barrier = pltpu.get_barrier_semaphore()
    partners = [core, near, far] + across[1:] + across_core[1:]
    for partner in partners:
        pl.semaphore_signal(
            barrier, inc=1, device_id=partner, device_id_type=pl.DeviceIdType.MESH
        )

    lane = lax.broadcasted_iota(jnp.int32, (count, LANES), 1)
    first_head = lane < HEAD_DIM
    even_quarter = (lane // (HEAD_DIM // 4)) % 2 == 0

    def pair_gain(gain_ref, pair):
        return jnp.concatenate(
            [gain_ref[2 * pair : 2 * pair + 1, :], gain_ref[2 * pair + 1 : 2 * pair + 2, :]],
            axis=1,
        )

    def norm_rotate(block, gain):
        wide = block.astype(f32)
        squares = wide * wide
        low = jnp.sum(jnp.where(first_head, squares, 0.0), axis=-1, keepdims=True)
        high = jnp.sum(jnp.where(first_head, 0.0, squares), axis=-1, keepdims=True)
        mean = jnp.where(first_head, low, high) * (1.0 / HEAD_DIM)
        scaled = wide * lax.rsqrt(mean + EPSILON) * gain
        quarter = HEAD_DIM // 4
        ahead = pltpu.roll(scaled, LANES - quarter, 1)
        behind = pltpu.roll(scaled, quarter, 1)
        swapped = jnp.where(even_quarter, ahead, behind)
        return scaled * cos_ref[...] + swapped * sin_ref[...]

    for h in range(halves):
        block = pl.ds(h * LANES, LANES)
        kv[h, 0, 0, 1] = v_ref[:, block]
        kv[h, 0, 0, 0] = norm_rotate(k_ref[:, block], pair_gain(k_gain_ref, h)).astype(bf16)
    tables[0, 0] = table_ref[...]

    pl.semaphore_wait(barrier, len(partners))

    def line_start(name, ref_at):
        links.send((name, "a01"), ref_at(0), ref_at(1), near, (name, 1))
        links.send((name, "b02"), ref_at(0), ref_at(2), far, (name, 2), "mid")

    def line_wait(name, slot, ref_at, only=None):
        links.arrived((name, slot), ref_at(slot), near, only)

    def line_forward(name, slot, ref_at):
        if slot == 1:
            links.send((name, "b13"), ref_at(1), ref_at(3), far, (name, 3), "mid")
        else:
            links.send((name, slot, "a"), ref_at(slot), ref_at(slot), near, (name, slot), "mid")

    def kv_at(h):
        return lambda slot: kv.at[h, slot, 0]

    def kv_swap(h, slot):
        links.send(("kvc", h, slot), kv.at[h, slot, 0], kv.at[h, slot, 1], core)

    def table_at(slot):
        return tables.at[slot, 0]

    def table_swap(slot):
        links.send(("tabc", slot), tables.at[slot, 0], tables.at[slot, 1], core)

    for h in range(halves):
        line_start(("kv", h), kv_at(h))
    for h in range(halves):
        kv_swap(h, 0)
    line_start("tab", table_at)
    table_swap(0)
    for q in (1, 2, 3):
        links.send(("down", q), down_hbm.at[0, :, columns(q)], down.at[0, q], across[q])
    for load in loads:
        load.start()

    for g in range(pairs):
        turned = norm_rotate(q_ref[:, pl.ds(g * LANES, LANES)], pair_gain(q_gain_ref, g))
        turned = turned.astype(bf16).astype(f32)
        other = pltpu.roll(turned, HEAD_DIM, 1)
        if g % 2 == 0:
            top, bottom = jnp.where(first_head, turned, 0.0), jnp.where(first_head, other, 0.0)
        else:
            top, bottom = jnp.where(first_head, 0.0, other), jnp.where(first_head, 0.0, turned)
        queries[g, pl.ds(0, count), :] = top.astype(bf16)
        queries[g, pl.ds(count, count), :] = bottom.astype(bf16)

    value_lane = lax.broadcasted_iota(jnp.int32, (2 * count, LANES), 1) // HEAD_DIM

    def attend(h, slot):
        def one(i, carry):
            g = 2 * h + i
            keys = kv[h, slot, :, 0].reshape(2 * count, LANES)
            values = kv[h, slot, :, 1].reshape(2 * count, LANES)
            values = jnp.where(value_lane == i, values.astype(f32), 1.0).astype(bf16)
            scores = lax.dot_general(
                queries[g], keys, (((1,), (1,)), ((), ())), preferred_element_type=f32
            )
            block_max = jnp.max(scores, axis=-1, keepdims=True)
            if slot == 0:
                new_max = block_max
            else:
                old_max = run_max[g]
                new_max = jnp.maximum(old_max, block_max)
            weights = jnp.exp((scores - new_max) * HEAD_DIM ** (-0.5)).astype(bf16)
            update = jnp.dot(weights, values, preferred_element_type=f32)
            if slot:
                rescale = jnp.exp((old_max - new_max) * HEAD_DIM ** (-0.5))
                update = update + run_acc[g] * rescale
            run_max[g] = new_max
            run_acc[g] = update
            return carry

        lax.fori_loop(0, 2, one, 0)

    def own_half(q, h):
        offset = quarters[q] + h * 2 * LANES
        return pl.ds(pl.multiple_of(offset, 2 * LANES), 2 * LANES)

    def attend_end(h):
        tiles = []
        for i in range(2):
            total = run_acc[2 * h + i]
            out = total / pltpu.roll(total, HEAD_DIM, 1)
            turned = pltpu.roll(out, HEAD_DIM, 1)
            if i == 0:
                tile = jnp.where(first_head, out[:count], turned[count:])
            else:
                tile = jnp.where(first_head, turned[:count], out[count:])
            tiles.append(tile.astype(bf16))
        attended[:, own_half(0, h)] = jnp.concatenate(tiles, axis=1)
        for q in (1, 2, 3):
            block = attended.at[:, own_half(0, h)]
            links.send(("att", h, q), block, block, across[q])

    chunks = [(h, slot) for slot in range(SLOTS) for h in range(halves)]
    for index in range(len(chunks) + 1):
        if index < len(chunks):
            h, slot = chunks[index]
            if slot:
                line_wait(("kv", h), slot, kv_at(h))
                line_forward(("kv", h), slot, kv_at(h))
                kv_swap(h, slot)
                if h == halves - 1:
                    line_wait("tab", slot, table_at)
                    line_forward("tab", slot, table_at)
                    table_swap(slot)
            if index == len(chunks) - 2:
                loads[3].wait()
                for q in (1, 2, 3):
                    links.arrived(("down", q), down.at[0, q], across[q])
                links.send("downc", down.at[0], down.at[1], core)
        if index:
            h, slot = chunks[index - 1]
            links.arrived(("kvc", h, slot), kv.at[h, slot, 1], core)
            attend(h, slot)
            if slot == SLOTS - 1:
                attend_end(h)

    loads[0].wait()
    mixed[...] = residual_ref[...].astype(f32)
    pieces = [(0, h) for h in range(halves)]
    pieces += [(q, h) for h in range(halves) for q in (1, 2, 3)]
    for q, h in pieces:
        if q:
            block = attended.at[:, own_half(q, h)]
            links.arrived(("att", h, q), block, across[q])
        mixed[...] += jnp.dot(
            attended[:, own_half(q, h)],
            out_weight[own_half(q, h), :],
            preferred_element_type=f32,
        )
    rows[0, 0, :, columns(0)] = mixed[...].astype(bf16)

    def rows_at(slot):
        return rows.at[slot, 0, :, columns(0)]

    def to_core(slot, q):
        links.send(
            ("rowc", slot, q),
            rows.at[slot, 0, :, columns(q)],
            rows.at[slot, 1, :, columns(q)],
            core,
        )

    def spread(slot):
        block = rows.at[slot, 0, :, columns(0)]
        links.send(("x1", slot), block, block, across[1])
        links.send(("y1", slot), block, block, across[2])
        to_core(slot, 0)

    def spread_on(slot):
        links.arrived(("y1", slot), rows.at[slot, 0, :, columns(2)], across[2])
        block = rows.at[slot, 0, upper_tok, columns(2)]
        links.send(("x2", slot), block, block, across[1])
        to_core(slot, 2)
        links.arrived(("x1", slot), rows.at[slot, 0, :, columns(1)], across[1])
        block = rows.at[slot, 0, lower_tok, columns(1)]
        links.send(("y2", slot), block, block, across[2])
        to_core(slot, 1)

    def spread_end(slot):
        links.arrived(("x2", slot), rows.at[slot, 0, upper_tok, columns(3)], across[1])
        links.arrived(("y2", slot), rows.at[slot, 0, lower_tok, columns(3)], across[2])
        to_core(slot, 3)

    def take(slot, mid):
        line_wait("row", slot, rows_at, "mid" if mid else "end")
        if mid:
            line_forward("row", slot, rows_at)

    experts_total = table_ref.shape[0]
    before = lax.broadcasted_iota(jnp.int32, (count, count), 0) < lax.broadcasted_iota(
        jnp.int32, (count, count), 1
    )
    before = before.astype(f32).astype(bf16)

    def ranks(table):
        chosen = table > 0.0
        marks = chosen.astype(f32).astype(bf16)
        rank = jnp.dot(marks, before, preferred_element_type=f32)
        return jnp.where(chosen, rank, -1.0)

    slot_of = lax.broadcasted_iota(jnp.int32, (capacity, count), 0).astype(f32)
    slot_in = lax.broadcasted_iota(jnp.int32, (count, capacity), 1).astype(f32)
    pair_count = experts_total // SLOTS
    my_expert = plane * pair_count + core_place * 2 + tp_place // 2
    expert_row = lax.broadcasted_iota(jnp.int32, (experts_total, count), 0)

    def hidden(slot):
        if slot == 0:
            loads[1].wait()
            loads[2].wait()

        def one(side, carry):
            block = rows[slot, side]
            wide = block.astype(f32)
            squares = jnp.mean(wide * wide, axis=-1, keepdims=True)
            norm_scale = lax.rsqrt(squares + EPSILON)
            both = jnp.dot(block, gate_up[...], preferred_element_type=f32) * norm_scale
            gate_value, up_value = both[:, :hidden_units], both[:, hidden_units:]
            result = (gate_value / (1.0 + jnp.exp(-gate_value)) * up_value).astype(bf16)
            rank = ranks(tables[slot, side])
            mine = jnp.sum(
                jnp.where(expert_row == my_expert, rank, 0.0), axis=0, keepdims=True
            )
            pick = (slot_of == mine).astype(f32).astype(bf16)
            packed = jnp.dot(pick, result, preferred_element_type=f32).astype(bf16)
            hid_other[slot, side] = packed
            return carry

        if slot == 0:
            links.arrived(("tabc", slot), tables.at[slot, 1], core)
        for q in range(4):
            links.arrived(("rowc", slot, q), rows.at[slot, 1, :, columns(q)], core)
        lax.fori_loop(0, 2, one, 0)

    def hid_send(slot):
        for q in (1, 2):
            links.send(("h", slot, q, 0), hid_other.at[slot, 0], hid.at[slot, q, 0], across[q])
            links.send(
                ("h", slot, q, 1), hid_other.at[slot, 1], hid.at[slot, q, 1], across_core[q]
            )
        links.send(("h", slot, 0, 1), hid_other.at[slot, 1], hid.at[slot, 0, 1], core)

    def hid_relay(slot):
        for cc in range(2):
            links.arrived(("h", slot, 2, cc), hid.at[slot, 2, cc], across[2])
        links.send(
            ("hx", slot),
            hid.at[slot, 2, :, upper_cap, :],
            hid.at[slot, 3, :, upper_cap, :],
            across[1],
        )
        for cc in range(2):
            links.arrived(("h", slot, 1, cc), hid.at[slot, 1, cc], across[1])
        links.send(
            ("hy", slot),
            hid.at[slot, 1, :, lower_cap, :],
            hid.at[slot, 3, :, lower_cap, :],
            across[2],
        )

    def partial(slot):
        links.arrived(("h", slot, 0, 1), hid.at[slot, 0, 1], core)
        links.arrived(("hx", slot), hid.at[slot, 3, :, upper_cap, :], across[1])
        links.arrived(("hy", slot), hid.at[slot, 3, :, lower_cap, :], across[2])
        hid[slot, 0, 0] = hid_other[slot, 0]
        table = tables[slot, 0]
        rank_column = jnp.transpose(ranks(table))
        weight_column = jnp.transpose(table)
        column = lax.broadcasted_iota(jnp.int32, (count, experts_total), 1)
        mixed_in = jnp.zeros((count, width), f32)
        for cc in range(2):
            for qy in range(2):
                results = [
                    jnp.dot(
                        hid[slot, 2 * qy + qx, cc],
                        down[cc, 2 * qy + qx],
                        preferred_element_type=f32,
                    ).astype(bf16)
                    for qx in range(2)
                ]
                expert = (
                    plane * pair_count
                    + flip_index(core_place, cc) * 2
                    + flip_index(tp_place // 2, qy)
                )
                this = column == expert
                rank = jnp.sum(jnp.where(this, rank_column, 0.0), axis=1, keepdims=True)
                weight = jnp.sum(jnp.where(this, weight_column, 0.0), axis=1, keepdims=True)
                place = (slot_in == rank).astype(f32).astype(bf16)
                both = jnp.dot(place, results[0], preferred_element_type=f32) + jnp.dot(
                    place, results[1], preferred_element_type=f32
                )
                mixed_in = mixed_in + both * weight
        return mixed_in

    def reduce_line(slot, value):
        if slot == 0:
            links.arrived("m1", part_in.at[0], near, "end")
            links.arrived("e1", part_in.at[0], near, "mid")
            mixed[...] += value + part_in[0].astype(f32)
            links.arrived("m2", part_in.at[3], far, "mid")

            @pl.when(is_mid)
            def _():
                mixed[...] += part_in[3].astype(f32)

            out_ref[...] = mixed[...]
            return
        part_send[slot] = value.astype(bf16)
        links.send(
            ("e", slot), part_send.at[slot], part_in.at[slot - 1], near, f"e{slot}", "end"
        )
        source = 4 if slot == 1 else slot - 1
        if slot == 1:
            links.arrived("m3", part_in.at[source], far, "mid")
        else:
            links.arrived(f"e{slot}", part_in.at[source], near, "mid")

        @pl.when(is_mid)
        def _():
            total = part_send[slot].astype(f32) + part_in[source].astype(f32)
            part_send[slot] = total.astype(bf16)

        if slot == 1:
            links.send(("m", 1), part_send.at[1], part_in.at[0], near, "m1", "mid")
        else:
            links.send(
                ("m", slot), part_send.at[slot], part_in.at[1 + slot], far, f"m{slot}", "mid"
            )

    line_start("row", rows_at)
    spread(0)
    line_wait("row", 1, rows_at)
    line_forward("row", 1, rows_at)
    spread_on(0)
    spread(1)
    spread_end(0)
    take(2, True)
    hidden(0)
    take(3, True)
    take(2, False)
    spread(2)
    spread_on(1)
    take(3, False)
    spread(3)
    for slot in range(1, SLOTS):
        links.arrived(("tabc", slot), tables.at[slot, 1], core)
    spread_end(1)
    spread_on(2)
    hidden(1)
    spread_on(3)
    spread_end(2)
    hidden(2)
    hid_send(2)
    spread_end(3)
    hidden(3)
    hid_send(3)
    links.arrived("downc", down.at[1], core)
    hid_relay(2)
    hid_send(1)
    hid_relay(3)
    reduce_line(3, partial(3))
    hid_send(0)
    reduce_line(2, partial(2))
    hid_relay(1)
    reduce_line(1, partial(1))
    hid_relay(0)
    reduce_line(0, partial(0))

    for copy, only in links.sent:
        links.when(only, copy.wait_send)


def local_fused(
    query_proj,
    key_proj,
    value_proj,
    query_gain,
    key_gain,
    residual,
    out_weight,
    route_expert,
    route_weight,
    expert_gate,
    expert_up,
    expert_down,
):
    token_count, width = query_proj.shape
    local_kv = key_gain.shape[0]
    total = out_weight.shape[0]
    hidden_units = expert_gate.shape[2]
    experts_total = lax.axis_size("sp") * lax.axis_size("tp") // 2
    capacity = 3 * token_count * TOP_K // (2 * experts_total)
    pair_count = HEAD_DIM // 4
    f32, bf16 = jnp.float32, jnp.bfloat16

    position = lax.axis_index("sp") * token_count + jnp.arange(token_count, dtype=jnp.int32)
    lane = jnp.arange(LANES, dtype=jnp.int32)
    quarter = (lane // pair_count) % 4
    place = jnp.where((quarter < 2)[None, :], (position // GRID_W)[:, None], (position % GRID_W)[:, None])
    inverse = ROPE_BASE ** (-(lane % pair_count).astype(f32) / pair_count)
    angles = place.astype(f32) * inverse[None, :]
    cosine = jnp.cos(angles)
    sine = jnp.sin(angles) * jnp.where(quarter % 2 == 0, -1.0, 1.0)[None, :]

    ids = jnp.arange(experts_total, dtype=jnp.int32)
    chosen = route_expert.T[None, :, :] == ids[:, None, None]
    table = jnp.sum(jnp.where(chosen, route_weight.T[None, :, :], 0.0), axis=1)

    vmem = pl.BlockSpec(memory_space=pltpu.VMEM)
    hbm = pl.BlockSpec(memory_space=pl.ANY)
    halves = local_kv // 2
    scratch = [
        pltpu.VMEM((halves, SLOTS, 2, 2, token_count, LANES), bf16),
        pltpu.VMEM((local_kv, 2 * token_count, LANES), bf16),
        pltpu.VMEM((local_kv, 2 * token_count, 1), f32),
        pltpu.VMEM((local_kv, 2 * token_count, LANES), f32),
        pltpu.VMEM((token_count, total), bf16),
        pltpu.VMEM((token_count, width), f32),
        pltpu.VMEM((SLOTS, 2, token_count, total), bf16),
        pltpu.VMEM((total, width), bf16),
        pltpu.VMEM((total, 2 * hidden_units), bf16),
        pltpu.VMEM((2, 4, hidden_units, width), bf16),
        pltpu.VMEM((SLOTS, 2, experts_total, token_count), f32),
        pltpu.VMEM((SLOTS, 4, 2, capacity, hidden_units), bf16),
        pltpu.VMEM((SLOTS, 2, capacity, hidden_units), bf16),
        pltpu.VMEM((SLOTS, token_count, width), bf16),
        pltpu.VMEM((5, token_count, width), bf16),
        pltpu.SemaphoreType.DMA((4,)),
        pltpu.SemaphoreType.DMA((SEMS,)),
        pltpu.SemaphoreType.DMA((SEMS,)),
    ]
    result = pl.pallas_call(
        fused_kernel,
        out_shape=jax.ShapeDtypeStruct((token_count, width), f32),
        in_specs=[vmem] * 9 + [hbm] * 4,
        out_specs=vmem,
        scratch_shapes=scratch,
        compiler_params=pltpu.CompilerParams(
            collective_id=0, has_side_effects=True, vmem_limit_bytes=56 * 1024 * 1024
        ),
    )(
        query_proj,
        key_proj,
        value_proj,
        query_gain,
        key_gain,
        cosine,
        sine,
        residual,
        table,
        out_weight,
        expert_gate,
        expert_up,
        expert_down,
    )
    return result.astype(bf16)


def takes_fused(mesh):
    chips = mesh.shape["sp"] // 2
    experts_total = mesh.shape["sp"] * mesh.shape["tp"] // 2
    return mesh.shape["tp"] == 4 and chips == SLOTS and experts_total == 2 * TOP_K


def solution(mesh):
    in_specs = (
        P("sp", "tp"),
        P("sp", "tp"),
        P("sp", "tp"),
        P("tp", None),
        P("tp", None),
        P("sp", "tp"),
        P(None, "tp"),
        P("sp", None),
        P("sp", None),
        P(("sp", "tp"), None, None),
        P(("sp", "tp"), None, None),
        P(("sp", "tp"), None, None),
    )
    out_specs = P("sp", "tp")
    body = local_fused if takes_fused(mesh) else local
    return jax.shard_map(body, mesh=mesh, in_specs=in_specs, out_specs=out_specs, check_vma=False)
```

```python
import functools
import math

import jax
import jax.numpy as jnp
from jax import lax
from jax.experimental import pallas as pl
from jax.experimental.pallas import tpu as pltpu
from jax.sharding import PartitionSpec as P

HEAD_DIM = 64
TOP_K = 8
GRID_W = 64


EPSILON = 1e-06
ROPE_BASE = 10000.0
KEY_BLOCK = 1024


def rotation_tables(offset, count):
    pair_count = HEAD_DIM // 4
    position = offset + jnp.arange(count, dtype=jnp.int32)
    grid_row = (position // GRID_W).astype(jnp.float32)
    grid_col = (position % GRID_W).astype(jnp.float32)
    inverse = ROPE_BASE ** (-jnp.arange(pair_count, dtype=jnp.float32) / pair_count)
    angles = jnp.stack([grid_row[:, None] * inverse, grid_col[:, None] * inverse], axis=1)
    return (jnp.cos(angles), jnp.sin(angles))


def rotate(vectors, cosine_table, sine_table):
    pair_count = HEAD_DIM // 4
    shaped = vectors.reshape(vectors.shape[:-1] + (2, 2, pair_count))
    first_half = shaped[..., 0, :]
    second_half = shaped[..., 1, :]
    cosine_row = cosine_table[:, None]
    sine_row = sine_table[:, None]
    turned = jnp.stack(
        [
            first_half * cosine_row - second_half * sine_row,
            first_half * sine_row + second_half * cosine_row,
        ],
        axis=-2,
    )
    return turned.reshape(vectors.shape)


def head_norm(vectors, gain):
    scaled = vectors.astype(jnp.float32)
    scaled = scaled * lax.rsqrt(jnp.mean(scaled * scaled, axis=-1, keepdims=True) + EPSILON)
    return scaled * gain


def online_update(running, query_groups, key_block, value_block):
    running_max, running_sum, running_acc = running
    scores = jnp.einsum(
        "tkgd,nkd->kgtn", query_groups, key_block, preferred_element_type=jnp.float32
    ) * HEAD_DIM ** (-0.5)
    new_max = jnp.maximum(running_max, jnp.max(scores, axis=-1))
    rescale = jnp.exp(running_max - new_max)
    weights = jnp.exp(scores - new_max[..., None]).astype(jnp.bfloat16)
    new_sum = running_sum * rescale + jnp.sum(weights.astype(jnp.float32), axis=-1)
    update = jnp.einsum("kgtn,nkd->kgtd", weights, value_block, preferred_element_type=jnp.float32)
    return (new_max, new_sum, running_acc * rescale[..., None] + update)


def local(
    query_proj,
    key_proj,
    value_proj,
    query_gain,
    key_gain,
    residual,
    out_weight,
    route_expert,
    route_weight,
    expert_gate,
    expert_up,
    expert_down,
):
    token_count = query_proj.shape[0]
    local_heads = query_gain.shape[0]
    local_kv = key_gain.shape[0]
    group_size = local_heads // local_kv
    sp_size = lax.axis_size("sp")
    tp_size = lax.axis_size("tp")
    tp_place = lax.axis_index("tp")
    offset = lax.axis_index("sp") * token_count
    cosine_table, sine_table = rotation_tables(offset, token_count)
    query_rot = rotate(
        head_norm(query_proj.reshape(token_count, local_heads, HEAD_DIM), query_gain),
        cosine_table,
        sine_table,
    ).astype(jnp.bfloat16)
    key_rot = rotate(
        head_norm(key_proj.reshape(token_count, local_kv, HEAD_DIM), key_gain),
        cosine_table,
        sine_table,
    ).astype(jnp.bfloat16)
    packed = jnp.concatenate(
        [key_rot.reshape(token_count, local_kv * HEAD_DIM), value_proj], axis=1
    )
    query_groups = query_rot.reshape(token_count, local_kv, group_size, HEAD_DIM)
    initial = (
        jnp.full((local_kv, group_size, token_count), -1e30, jnp.float32),
        jnp.zeros((local_kv, group_size, token_count), jnp.float32),
        jnp.zeros((local_kv, group_size, token_count, HEAD_DIM), jnp.float32),
    )
    incoming = lax.all_gather(packed, "sp", axis=0, tiled=True)
    incoming_len = incoming.shape[0]
    step_len = math.gcd(incoming_len, KEY_BLOCK)

    def one_step(step_index, running):
        block_rows = lax.dynamic_slice_in_dim(incoming, step_index * step_len, step_len, 0)
        key_block = block_rows[:, : local_kv * HEAD_DIM].reshape(step_len, local_kv, HEAD_DIM)
        value_block = block_rows[:, local_kv * HEAD_DIM :].reshape(step_len, local_kv, HEAD_DIM)
        return online_update(running, query_groups, key_block, value_block)

    final_max, final_sum, final_acc = lax.fori_loop(0, incoming_len // step_len, one_step, initial)
    attended = final_acc / final_sum[..., None]
    attended = jnp.transpose(attended, (2, 0, 1, 3)).reshape(token_count, local_heads * HEAD_DIM)
    attended = attended.astype(jnp.bfloat16)
    projected = jnp.dot(
        lax.all_gather(attended, "tp", axis=1, tiled=True),
        out_weight,
        preferred_element_type=jnp.float32,
    )
    mixed_sum = residual.astype(jnp.float32) + projected
    mixed_rows = mixed_sum.astype(jnp.bfloat16)
    full_rows = lax.all_gather(mixed_rows, "tp", axis=1, tiled=True)
    width_total = full_rows.shape[1]
    per_sp = tp_size // 2
    column = tp_place // 2
    experts_total = per_sp * sp_size
    capacity = 3 * token_count * TOP_K // (2 * experts_total)
    slot_count = sp_size * capacity
    flat_choice = route_expert.reshape(token_count * TOP_K)
    onehot = (flat_choice[:, None] == jnp.arange(experts_total, dtype=jnp.int32)[None, :]).astype(
        jnp.int32
    )
    earlier = jnp.cumsum(onehot, axis=0) - onehot
    slot_rank = jnp.sum(earlier * onehot, axis=1)
    mine = flat_choice % per_sp == column
    target = flat_choice // per_sp * capacity + slot_rank
    owner = jnp.arange(token_count * TOP_K, dtype=jnp.int32) // TOP_K
    slot_token = (
        jnp.full((slot_count + 1,), token_count, jnp.int32)
        .at[jnp.where(mine, target, slot_count)]
        .set(owner)[:slot_count]
    )
    padded = jnp.concatenate([full_rows, jnp.zeros((1, width_total), jnp.bfloat16)], axis=0)
    selected = padded[slot_token].reshape(sp_size, capacity, width_total)
    arrived = lax.all_to_all(selected, "sp", split_axis=0, concat_axis=0, tiled=True)
    expert_rows = arrived.reshape(slot_count, width_total)
    squares = jnp.mean(jnp.square(expert_rows.astype(jnp.float32)), axis=-1, keepdims=True)
    norm_scale = lax.rsqrt(squares + EPSILON)
    gate_value = (
        jnp.dot(expert_rows, expert_gate[0], preferred_element_type=jnp.float32) * norm_scale
    )
    up_value = jnp.dot(expert_rows, expert_up[0], preferred_element_type=jnp.float32) * norm_scale
    hidden = (jax.nn.silu(gate_value) * up_value).astype(jnp.bfloat16)
    half_result = jnp.dot(hidden, expert_down[0], preferred_element_type=jnp.float32).astype(
        jnp.bfloat16
    )
    returned = lax.all_to_all(
        half_result.reshape(sp_size, capacity, width_total),
        "sp",
        split_axis=0,
        concat_axis=0,
        tiled=True,
    )
    slot_results = returned.reshape(slot_count, width_total)
    mine_grid = mine.reshape(token_count, TOP_K)
    target_grid = target.reshape(token_count, TOP_K)
    gathered_sum = jnp.zeros((token_count, width_total), jnp.float32)
    for choice_index in range(TOP_K):
        chosen = mine_grid[:, choice_index]
        index = jnp.where(chosen, target_grid[:, choice_index], 0)
        factor = jnp.where(chosen, route_weight[:, choice_index], 0.0)
        picked = slot_results[index].astype(jnp.float32)
        gathered_sum = gathered_sum + factor[:, None] * picked
    routed = lax.psum_scatter(
        gathered_sum.astype(jnp.bfloat16), "tp", scatter_dimension=1, tiled=True
    ).astype(jnp.float32)
    return (mixed_sum + routed).astype(jnp.bfloat16)


def flip_index(index, mask):
    bit = 1
    while bit <= mask:
        if mask & bit:
            index = index + bit - 2 * bit * ((index // bit) % 2)
        bit *= 2
    return index


LANES = 128
SLOTS = 4
SEMS = 200
ORDER = (
    ("start",),
    ("x1", 0),
    ("z", 1, 0, None),
    ("z", 2, 0, "mid"),
    ("z", 1, 1, None),
    ("x1", 1),
    ("z", 2, 1, "end"),
    ("z", 2, 1, "mid"),
    ("z", 2, 0, "end"),
    ("x1", 2),
    ("z", 3, 1, "end"),
    ("z", 3, 0, "end"),
    ("z", 3, 0, "mid"),
    ("z", 3, 1, "mid"),
    ("x1", 3),
    ("x2", 2),
    ("x2", 3),
    ("c3", 2),
    ("x2", 1),
    ("hid", 2),
    ("hs", 2),
    ("c3", 3),
    ("hid", 3),
    ("hs", 3),
    ("hr", 2),
    ("hr", 3),
    ("x2", 0),
    ("c3", 1),
    ("hid", 1),
    ("hs", 1),
    ("part", 3),
    ("c3", 0),
    ("part", 2),
    ("hid", 0),
    ("hr", 1),
    ("red", 3),
    ("hs", 0),
    ("part", 1),
    ("red", 1),
    ("red", 2),
    ("hr", 0),
    ("part", 0),
    ("red", 0),
)


class Links:
    def __init__(self, send_sem, recv_sem, conditions):
        self.send_sem, self.recv_sem = send_sem, recv_sem
        self.conditions = conditions
        self.send_ids, self.recv_ids = {}, {}
        self.sent = []

    def copy(self, src, dst, device, send_key, recv_key):
        send_id = self.send_ids.setdefault(send_key, len(self.send_ids))
        recv_id = self.recv_ids.setdefault(recv_key, len(self.recv_ids))
        return pltpu.make_async_remote_copy(
            src_ref=src,
            dst_ref=dst,
            send_sem=self.send_sem.at[send_id],
            recv_sem=self.recv_sem.at[recv_id],
            device_id=device,
            device_id_type=pl.DeviceIdType.MESH,
        )

    def send(self, key, src, dst, device, recv_key=None, only=None):
        copy = self.copy(src, dst, device, key, key if recv_key is None else recv_key)
        self.when(only, copy.start)
        self.sent.append((copy, only))

    def arrived(self, key, dst, device, only=None):
        self.when(only, self.copy(dst, dst, device, "none", key).wait_recv)

    def when(self, only, act):
        if only is None:
            act()
        else:
            pl.when(self.conditions[only])(act)


def fused_kernel(
    q_ref,
    k_ref,
    v_ref,
    q_gain_ref,
    k_gain_ref,
    residual_ref,
    expert_ref,
    weight_ref,
    out_weight_hbm,
    gate_hbm,
    up_hbm,
    down_hbm,
    out_ref,
    kv,
    queries,
    run_max,
    run_acc,
    attended,
    mixed,
    rows,
    out_weight,
    gate_up,
    down,
    tables,
    hid,
    hid_other,
    part_own,
    part_send,
    part_in,
    local_sem,
    send_sem,
    recv_sem,
):
    f32, bf16 = jnp.float32, jnp.bfloat16
    count, width = q_ref.shape
    pairs = width // LANES
    halves = pairs // 2
    hidden_units = gate_hbm.shape[2]
    capacity = hid.shape[3]
    upper_tok, lower_tok = pl.ds(0, count // 2), pl.ds(count // 2, count // 2)
    upper_cap, lower_cap = pl.ds(0, capacity // 2), pl.ds(capacity // 2, capacity // 2)

    sp_place, tp_place = lax.axis_index("sp"), lax.axis_index("tp")
    plane, core_place = sp_place // 2, sp_place % 2
    is_mid = (plane == 1) | (plane == 2)
    is_end = (plane == 0) | (plane == 3)

    def at(sp_mask, tp_mask):
        return {"sp": flip_index(sp_place, sp_mask), "tp": flip_index(tp_place, tp_mask)}

    core, near, far = at(1, 0), at(2, 0), at(6, 0)
    across = [None, at(0, 1), at(0, 2), at(0, 3)]
    across_core = [core, at(1, 1), at(1, 2)]
    links = Links(send_sem, recv_sem, {"mid": is_mid, "end": is_end})

    quarters = [flip_index(tp_place, q) * width for q in range(4)]

    def columns(q):
        return pl.ds(pl.multiple_of(quarters[q], width), width)

    loads = [
        pltpu.make_async_copy(out_weight_hbm, out_weight, local_sem.at[0]),
        pltpu.make_async_copy(
            gate_hbm.at[0], gate_up.at[:, pl.ds(0, hidden_units)], local_sem.at[1]
        ),
        pltpu.make_async_copy(
            up_hbm.at[0], gate_up.at[:, pl.ds(hidden_units, hidden_units)], local_sem.at[2]
        ),
        pltpu.make_async_copy(down_hbm.at[0, :, columns(0)], down.at[0, 0], local_sem.at[3]),
    ]

    barrier = pltpu.get_barrier_semaphore()
    partners = [core, near, far] + across[1:] + across_core[1:]
    for partner in partners:
        pl.semaphore_signal(
            barrier, inc=1, device_id=partner, device_id_type=pl.DeviceIdType.MESH
        )

    lane = lax.broadcasted_iota(jnp.int32, (count, LANES), 1)
    first_head = lane < HEAD_DIM
    quarter = HEAD_DIM // 4
    even_quarter = (lane // quarter) % 2 == 0

    grid_rows = count // GRID_W
    token = lax.broadcasted_iota(jnp.int32, (GRID_W + 8, LANES), 0)
    lane_short = lax.broadcasted_iota(jnp.int32, (GRID_W + 8, LANES), 1)
    place = jnp.where(token < GRID_W, token, sp_place * grid_rows + token - GRID_W)
    power = (lane_short % quarter).astype(f32) * (-math.log(ROPE_BASE) / quarter)
    angle = place.astype(f32) * jnp.exp(power)
    sign = jnp.where((lane_short // quarter) % 2 == 0, -1.0, 1.0)

    def over_tokens(short):
        parts = []
        by_row = ((lane_short[:GRID_W] // quarter) % 4) < 2
        for r in range(grid_rows):
            line = short[GRID_W + r : GRID_W + r + 1, :]
            parts.append(jnp.where(by_row, line, short[:GRID_W, :]))
        return jnp.concatenate(parts, axis=0)

    cosine = over_tokens(jnp.cos(angle))
    sine = over_tokens(jnp.sin(angle) * sign)

    def pair_gain(gain_ref, pair):
        return jnp.concatenate(
            [gain_ref[2 * pair : 2 * pair + 1, :], gain_ref[2 * pair + 1 : 2 * pair + 2, :]],
            axis=1,
        )

    def norm_rotate(block, gain):
        wide = block.astype(f32)
        squares = wide * wide
        low = jnp.sum(jnp.where(first_head, squares, 0.0), axis=-1, keepdims=True)
        high = jnp.sum(jnp.where(first_head, 0.0, squares), axis=-1, keepdims=True)
        mean = jnp.where(first_head, low, high) * (1.0 / HEAD_DIM)
        scaled = wide * lax.rsqrt(mean + EPSILON) * gain
        ahead = pltpu.roll(scaled, LANES - quarter, 1)
        behind = pltpu.roll(scaled, quarter, 1)
        swapped = jnp.where(even_quarter, ahead, behind)
        return scaled * cosine + swapped * sine

    for h in range(halves):
        block = pl.ds(h * LANES, LANES)
        flipped = jnp.transpose(v_ref[:, block].astype(f32)).astype(bf16)
        for part in range(count // LANES):
            kv[h, 0, 0, 1, pl.ds(part * LANES, LANES), :] = flipped[
                :, part * LANES : (part + 1) * LANES
            ]
        kv[h, 0, 0, 0] = norm_rotate(k_ref[:, block], pair_gain(k_gain_ref, h)).astype(bf16)

    pl.semaphore_wait(barrier, len(partners))

    def line_start(name, ref_at):
        links.send((name, "a01"), ref_at(0), ref_at(1), near, (name, 1))
        links.send((name, "b02"), ref_at(0), ref_at(2), far, (name, 2), "mid")

    def line_wait(name, slot, ref_at, only=None):
        links.arrived((name, slot), ref_at(slot), near, only)
        if only == "end":
            return
        if slot == 1:
            links.send((name, "b13"), ref_at(1), ref_at(3), far, (name, 3), "mid")
        else:
            links.send((name, slot, "a"), ref_at(slot), ref_at(slot), near, (name, slot), "mid")

    def kv_at(h):
        return lambda slot: kv.at[h, slot, 0]

    def kv_swap(h, slot, only=None):
        links.send(("kvc", h, slot), kv.at[h, slot, 0], kv.at[h, slot, 1], core, only=only)

    def table_at(slot):
        return tables.at[slot, 0]

    def table_swap(slot, only=None):
        links.send(("tabc", slot), tables.at[slot, 0], tables.at[slot, 1], core, only=only)

    def take_kv(h, slot, only=None):
        line_wait(("kv", h), slot, kv_at(h), only)
        kv_swap(h, slot, only)
        if h == halves - 1:
            line_wait("tab", slot, table_at, only)
            table_swap(slot, only)

    for h in range(halves):
        line_start(("kv", h), kv_at(h))
    for h in range(halves):
        kv_swap(h, 0)
    experts_total = tables.shape[2]
    names, factors = expert_ref[...], weight_ref[...]
    wanted = lax.broadcasted_iota(jnp.int32, (experts_total, count), 0)
    table = jnp.zeros((experts_total, count), f32)
    for k in range(TOP_K):
        table = table + jnp.where(names[k : k + 1, :] == wanted, factors[k : k + 1, :], 0.0)
    tables[0, 0] = table
    line_start("tab", table_at)
    table_swap(0)
    for q in (1, 2, 3):
        links.send(("down", q), down_hbm.at[0, :, columns(q)], down.at[0, q], across[q])
    for load in loads:
        load.start()

    for g in range(pairs):
        turned = norm_rotate(q_ref[:, pl.ds(g * LANES, LANES)], pair_gain(q_gain_ref, g))
        turned = turned.astype(bf16).astype(f32)
        other = pltpu.roll(turned, HEAD_DIM, 1)
        if g % 2 == 0:
            top, bottom = jnp.where(first_head, turned, 0.0), jnp.where(first_head, other, 0.0)
        else:
            top, bottom = jnp.where(first_head, 0.0, other), jnp.where(first_head, 0.0, turned)
        queries[g, pl.ds(0, count), :] = top.astype(bf16)
        queries[g, pl.ds(count, count), :] = bottom.astype(bf16)

    ones = jnp.ones((16, 2 * count), bf16)
    exponent = math.log2(math.e) * HEAD_DIM ** (-0.5)

    def attend(h, slot):
        def one(i, carry):
            g = 2 * h + i
            keys = kv[h, slot, :, 0].reshape(2 * count, LANES)
            values = [
                kv[h, slot, side, 1, pl.ds(part * LANES, LANES), :]
                for side in range(2)
                for part in range(count // LANES)
            ]
            values = jnp.concatenate(values, axis=1)
            values = jnp.concatenate([values, ones], axis=0)
            scores = lax.dot_general(
                keys, queries[g], (((1,), (1,)), ((), ())), preferred_element_type=f32
            )
            block_max = jnp.max(scores, axis=0, keepdims=True)
            if slot == 0:
                new_max = block_max
            else:
                old_max = run_max[g]
                new_max = jnp.maximum(old_max, block_max)
            weights = jnp.exp2((scores - new_max) * exponent).astype(bf16)
            update = jnp.dot(values, weights, preferred_element_type=f32)
            if slot:
                rescale = jnp.exp2((old_max - new_max) * exponent)
                update = update + run_acc[g] * rescale
            run_max[g] = new_max
            run_acc[g] = update
            return carry

        lax.fori_loop(0, 2, one, 0)

    def own_half(q, h):
        offset = quarters[q] + h * 2 * LANES
        return pl.ds(pl.multiple_of(offset, 2 * LANES), 2 * LANES)

    def attend_end(h):
        tiles = []
        for i in range(2):
            total = run_acc[2 * h + i]
            out = total[i * HEAD_DIM : (i + 1) * HEAD_DIM] / total[LANES : LANES + 1]
            heads = jnp.concatenate([out[:, :count], out[:, count:]], axis=0)
            tiles.append(jnp.transpose(heads).astype(bf16))
        attended[:, own_half(0, h)] = jnp.concatenate(tiles, axis=1)
        block = attended.at[:, own_half(0, h)]
        for q in (1, 2):
            links.send(("att", h, q), block, block, across[q])

    def attend_relay(h):
        links.arrived(("att", h, 2), attended.at[:, own_half(2, h)], across[2])
        block = attended.at[upper_tok, own_half(2, h)]
        links.send(("attx", h), block, block, across[1])
        links.arrived(("att", h, 1), attended.at[:, own_half(1, h)], across[1])
        block = attended.at[lower_tok, own_half(1, h)]
        links.send(("atty", h), block, block, across[2])

    def attend_chunk(h, slot):
        links.arrived(("kvc", h, slot), kv.at[h, slot, 1], core)
        attend(h, slot)

    attend_chunk(0, 0)
    take_kv(0, 1)
    take_kv(0, 2, "mid")
    attend_chunk(1, 0)
    attend_chunk(0, 1)
    take_kv(1, 1)
    take_kv(1, 2, "mid")
    attend_chunk(1, 1)
    take_kv(0, 2, "end")
    attend_chunk(0, 2)
    take_kv(0, 3, "mid")
    take_kv(1, 2, "end")
    attend_chunk(1, 2)
    loads[3].wait()
    for q in (1, 2, 3):
        links.arrived(("down", q), down.at[0, q], across[q])
    links.send("downc", down.at[0], down.at[1], core)
    take_kv(1, 3, "mid")
    take_kv(0, 3, "end")
    attend_chunk(0, 3)
    attend_end(0)
    take_kv(1, 3, "end")
    attend_chunk(1, 3)
    attend_end(1)

    loads[0].wait()
    mixed[...] = residual_ref[...].astype(f32)

    def project(q, h):
        mixed[...] += jnp.dot(
            attended[:, own_half(q, h)],
            out_weight[own_half(q, h), :],
            preferred_element_type=f32,
        )

    for h in range(halves):
        project(0, h)
    for h in range(halves):
        attend_relay(h)
        project(1, h)
        project(2, h)
    for h in range(halves):
        links.arrived(("attx", h), attended.at[upper_tok, own_half(3, h)], across[1])
        links.arrived(("atty", h), attended.at[lower_tok, own_half(3, h)], across[2])
        project(3, h)
    rows[0, 0, :, columns(0)] = mixed[...].astype(bf16)

    def rows_at(part):
        return lambda slot: rows.at[slot, 0, (upper_tok, lower_tok)[part], columns(0)]

    def to_core(slot, q):
        links.send(
            ("rowc", slot, q),
            rows.at[slot, 0, :, columns(q)],
            rows.at[slot, 1, :, columns(q)],
            core,
        )

    def spread(slot):
        block = rows.at[slot, 0, :, columns(0)]
        links.send(("x1", slot), block, block, across[1])
        links.send(("y1", slot), block, block, across[2])
        to_core(slot, 0)

    def spread_on(slot):
        links.arrived(("y1", slot), rows.at[slot, 0, :, columns(2)], across[2])
        block = rows.at[slot, 0, upper_tok, columns(2)]
        links.send(("x2", slot), block, block, across[1])
        to_core(slot, 2)
        links.arrived(("x1", slot), rows.at[slot, 0, :, columns(1)], across[1])
        block = rows.at[slot, 0, lower_tok, columns(1)]
        links.send(("y2", slot), block, block, across[2])
        to_core(slot, 1)

    def spread_end(slot):
        links.arrived(("x2", slot), rows.at[slot, 0, upper_tok, columns(3)], across[1])
        links.arrived(("y2", slot), rows.at[slot, 0, lower_tok, columns(3)], across[2])
        to_core(slot, 3)

    def take(slot, part, only=None):
        line_wait(("row", part), slot, rows_at(part), only)

    before = lax.broadcasted_iota(jnp.int32, (count, count), 0) < lax.broadcasted_iota(
        jnp.int32, (count, count), 1
    )
    before = before.astype(f32).astype(bf16)

    def ranks(table):
        chosen = table > 0.0
        marks = chosen.astype(f32).astype(bf16)
        rank = jnp.dot(marks, before, preferred_element_type=f32)
        return jnp.where(chosen, rank, -1.0)

    slot_of = lax.broadcasted_iota(jnp.int32, (capacity, count), 0).astype(f32)
    slot_in = lax.broadcasted_iota(jnp.int32, (count, capacity), 1).astype(f32)
    pair_count = experts_total // SLOTS
    my_expert = plane * pair_count + core_place * 2 + tp_place // 2
    expert_row = lax.broadcasted_iota(jnp.int32, (experts_total, count), 0)

    def hidden(slot):
        def one(side, carry):
            block = rows[slot, side]
            wide = block.astype(f32)
            squares = jnp.mean(wide * wide, axis=-1, keepdims=True)
            norm_scale = lax.rsqrt(squares + EPSILON)
            both = jnp.dot(block, gate_up[...], preferred_element_type=f32) * norm_scale
            gate_value, up_value = both[:, :hidden_units], both[:, hidden_units:]
            result = (gate_value / (1.0 + jnp.exp(-gate_value)) * up_value).astype(bf16)
            rank = ranks(tables[slot, side])
            mine = jnp.sum(
                jnp.where(expert_row == my_expert, rank, 0.0), axis=0, keepdims=True
            )
            pick = (slot_of == mine).astype(f32).astype(bf16)
            packed = jnp.dot(pick, result, preferred_element_type=f32).astype(bf16)
            hid_other[slot, side] = packed
            return carry

        links.arrived(("tabc", slot), tables.at[slot, 1], core)
        for q in range(4):
            links.arrived(("rowc", slot, q), rows.at[slot, 1, :, columns(q)], core)
        lax.fori_loop(0, 2, one, 0)

    def hid_send(slot):
        for q in (1, 2):
            links.send(("h", slot, q, 0), hid_other.at[slot, 0], hid.at[slot, q, 0], across[q])
            links.send(
                ("h", slot, q, 1), hid_other.at[slot, 1], hid.at[slot, q, 1], across_core[q]
            )
        links.send(("h", slot, 0, 1), hid_other.at[slot, 1], hid.at[slot, 0, 1], core)

    def hid_relay(slot):
        for cc in range(2):
            links.arrived(("h", slot, 2, cc), hid.at[slot, 2, cc], across[2])
        links.send(
            ("hx", slot),
            hid.at[slot, 2, :, upper_cap, :],
            hid.at[slot, 3, :, upper_cap, :],
            across[1],
        )
        for cc in range(2):
            links.arrived(("h", slot, 1, cc), hid.at[slot, 1, cc], across[1])
        links.send(
            ("hy", slot),
            hid.at[slot, 1, :, lower_cap, :],
            hid.at[slot, 3, :, lower_cap, :],
            across[2],
        )

    def partial(slot):
        links.arrived(("h", slot, 0, 1), hid.at[slot, 0, 1], core)
        links.arrived(("hx", slot), hid.at[slot, 3, :, upper_cap, :], across[1])
        links.arrived(("hy", slot), hid.at[slot, 3, :, lower_cap, :], across[2])
        hid[slot, 0, 0] = hid_other[slot, 0]
        table = tables[slot, 0]
        rank_column = jnp.transpose(ranks(table))
        weight_column = jnp.transpose(table)
        column = lax.broadcasted_iota(jnp.int32, (count, experts_total), 1)
        mixed_in = jnp.zeros((count, width), f32)
        for cc in range(2):
            for qy in range(2):
                results = [
                    jnp.dot(
                        hid[slot, 2 * qy + qx, cc],
                        down[cc, 2 * qy + qx],
                        preferred_element_type=f32,
                    ).astype(bf16)
                    for qx in range(2)
                ]
                expert = (
                    plane * pair_count
                    + flip_index(core_place, cc) * 2
                    + flip_index(tp_place // 2, qy)
                )
                this = column == expert
                rank = jnp.sum(jnp.where(this, rank_column, 0.0), axis=1, keepdims=True)
                weight = jnp.sum(jnp.where(this, weight_column, 0.0), axis=1, keepdims=True)
                place = (slot_in == rank).astype(f32).astype(bf16)
                both = jnp.dot(place, results[0], preferred_element_type=f32) + jnp.dot(
                    place, results[1], preferred_element_type=f32
                )
                mixed_in = mixed_in + both * weight
        return mixed_in

    tokens = (upper_tok, lower_tok)

    def send_back(slot):
        value = partial(slot)
        if slot == 0:
            mixed[...] += value
            return
        part_own[slot] = value
        part_send[slot] = value.astype(bf16)
        for p, span in enumerate(tokens):
            links.send(
                ("e", slot, p),
                part_send.at[slot, span],
                part_in.at[slot - 1, span],
                near,
                ("pe", slot, p),
                "end",
            )

    def pass_back(slot):
        for p, span in enumerate(tokens):
            if slot == 0:
                links.arrived(("pm", 1, p), part_in.at[0, span], near, "end")
                links.arrived(("pe", 1, p), part_in.at[0, span], near, "mid")
                links.arrived(("pm", 2, p), part_in.at[3, span], far, "mid")
                continue
            source = 4 if slot == 1 else slot - 1
            if slot == 1:
                links.arrived(("pm", 3, p), part_in.at[source, span], far, "mid")
            else:
                links.arrived(("pe", slot, p), part_in.at[source, span], near, "mid")

            @pl.when(is_mid)
            def _():
                total = part_own[slot, span] + part_in[source, span].astype(f32)
                part_send[slot, span] = total.astype(bf16)

            block = part_send.at[slot, span]
            if slot == 1:
                links.send(("m", 1, p), block, part_in.at[0, span], near, ("pm", 1, p), "mid")
            else:
                target = part_in.at[1 + slot, span]
                links.send(("m", slot, p), block, target, far, ("pm", slot, p), "mid")
        if slot == 0:
            total = mixed[...] + part_in[0].astype(f32)
            out_ref[...] = total.astype(bf16)

            @pl.when(is_mid)
            def _():
                out_ref[...] = (total + part_in[3].astype(f32)).astype(bf16)

    def start_rows():
        for part in range(2):
            line_start(("row", part), rows_at(part))

    steps = {
        "start": start_rows,
        "z": take,
        "x1": spread,
        "x2": spread_on,
        "c3": spread_end,
        "hid": hidden,
        "hs": hid_send,
        "hr": hid_relay,
        "part": send_back,
        "red": pass_back,
    }
    loads[1].wait()
    loads[2].wait()
    links.arrived("downc", down.at[1], core)
    for step, *where in ORDER:
        steps[step](*where)

    for copy, only in links.sent:
        links.when(only, copy.wait_send)


def local_fused(
    query_proj,
    key_proj,
    value_proj,
    query_gain,
    key_gain,
    residual,
    out_weight,
    route_expert,
    route_weight,
    expert_gate,
    expert_up,
    expert_down,
):
    token_count, width = query_proj.shape
    local_kv = key_gain.shape[0]
    total = out_weight.shape[0]
    hidden_units = expert_gate.shape[2]
    experts_total = lax.axis_size("sp") * lax.axis_size("tp") // 2
    capacity = 3 * token_count * TOP_K // (2 * experts_total)
    f32, bf16 = jnp.float32, jnp.bfloat16

    vmem = pl.BlockSpec(memory_space=pltpu.VMEM)
    hbm = pl.BlockSpec(memory_space=pl.ANY)
    halves = local_kv // 2
    scratch = [
        pltpu.VMEM((halves, SLOTS, 2, 2, token_count, LANES), bf16),
        pltpu.VMEM((local_kv, 2 * token_count, LANES), bf16),
        pltpu.VMEM((local_kv, 1, 2 * token_count), f32),
        pltpu.VMEM((local_kv, LANES + 16, 2 * token_count), f32),
        pltpu.VMEM((token_count, total), bf16),
        pltpu.VMEM((token_count, width), f32),
        pltpu.VMEM((SLOTS, 2, token_count, total), bf16),
        pltpu.VMEM((total, width), bf16),
        pltpu.VMEM((total, 2 * hidden_units), bf16),
        pltpu.VMEM((2, 4, hidden_units, width), bf16),
        pltpu.VMEM((SLOTS, 2, experts_total, token_count), f32),
        pltpu.VMEM((SLOTS, 4, 2, capacity, hidden_units), bf16),
        pltpu.VMEM((SLOTS, 2, capacity, hidden_units), bf16),
        pltpu.VMEM((SLOTS, token_count, width), f32),
        pltpu.VMEM((SLOTS, token_count, width), bf16),
        pltpu.VMEM((5, token_count, width), bf16),
        pltpu.SemaphoreType.DMA((4,)),
        pltpu.SemaphoreType.DMA((SEMS,)),
        pltpu.SemaphoreType.DMA((SEMS,)),
    ]
    result = pl.pallas_call(
        fused_kernel,
        out_shape=jax.ShapeDtypeStruct((token_count, width), bf16),
        in_specs=[vmem] * 8 + [hbm] * 4,
        out_specs=vmem,
        scratch_shapes=scratch,
        compiler_params=pltpu.CompilerParams(
            collective_id=0, has_side_effects=True, vmem_limit_bytes=56 * 1024 * 1024
        ),
    )(
        query_proj,
        key_proj,
        value_proj,
        query_gain,
        key_gain,
        residual,
        route_expert.T,
        route_weight.T,
        out_weight,
        expert_gate,
        expert_up,
        expert_down,
    )
    return result


def takes_fused(mesh):
    chips = mesh.shape["sp"] // 2
    experts_total = mesh.shape["sp"] * mesh.shape["tp"] // 2
    return mesh.shape["tp"] == 4 and chips == SLOTS and experts_total == 2 * TOP_K


def solution(mesh):
    in_specs = (
        P("sp", "tp"),
        P("sp", "tp"),
        P("sp", "tp"),
        P("tp", None),
        P("tp", None),
        P("sp", "tp"),
        P(None, "tp"),
        P("sp", None),
        P("sp", None),
        P(("sp", "tp"), None, None),
        P(("sp", "tp"), None, None),
        P(("sp", "tp"), None, None),
    )
    out_specs = P("sp", "tp")
    body = local_fused if takes_fused(mesh) else local
    return jax.shard_map(body, mesh=mesh, in_specs=in_specs, out_specs=out_specs, check_vma=False)
```

```python
import functools
import math

import jax
import jax.numpy as jnp
from jax import lax
from jax.experimental import pallas as pl
from jax.experimental.pallas import tpu as pltpu
from jax.sharding import PartitionSpec as P

HEAD_DIM = 64
TOP_K = 8
GRID_W = 64


EPSILON = 1e-06
ROPE_BASE = 10000.0
KEY_BLOCK = 1024


def rotation_tables(offset, count):
    pair_count = HEAD_DIM // 4
    position = offset + jnp.arange(count, dtype=jnp.int32)
    grid_row = (position // GRID_W).astype(jnp.float32)
    grid_col = (position % GRID_W).astype(jnp.float32)
    inverse = ROPE_BASE ** (-jnp.arange(pair_count, dtype=jnp.float32) / pair_count)
    angles = jnp.stack([grid_row[:, None] * inverse, grid_col[:, None] * inverse], axis=1)
    return (jnp.cos(angles), jnp.sin(angles))


def rotate(vectors, cosine_table, sine_table):
    pair_count = HEAD_DIM // 4
    shaped = vectors.reshape(vectors.shape[:-1] + (2, 2, pair_count))
    first_half = shaped[..., 0, :]
    second_half = shaped[..., 1, :]
    cosine_row = cosine_table[:, None]
    sine_row = sine_table[:, None]
    turned = jnp.stack(
        [
            first_half * cosine_row - second_half * sine_row,
            first_half * sine_row + second_half * cosine_row,
        ],
        axis=-2,
    )
    return turned.reshape(vectors.shape)


def head_norm(vectors, gain):
    scaled = vectors.astype(jnp.float32)
    scaled = scaled * lax.rsqrt(jnp.mean(scaled * scaled, axis=-1, keepdims=True) + EPSILON)
    return scaled * gain


def online_update(running, query_groups, key_block, value_block):
    running_max, running_sum, running_acc = running
    scores = jnp.einsum(
        "tkgd,nkd->kgtn", query_groups, key_block, preferred_element_type=jnp.float32
    ) * HEAD_DIM ** (-0.5)
    new_max = jnp.maximum(running_max, jnp.max(scores, axis=-1))
    rescale = jnp.exp(running_max - new_max)
    weights = jnp.exp(scores - new_max[..., None]).astype(jnp.bfloat16)
    new_sum = running_sum * rescale + jnp.sum(weights.astype(jnp.float32), axis=-1)
    update = jnp.einsum("kgtn,nkd->kgtd", weights, value_block, preferred_element_type=jnp.float32)
    return (new_max, new_sum, running_acc * rescale[..., None] + update)


def local(
    query_proj,
    key_proj,
    value_proj,
    query_gain,
    key_gain,
    residual,
    out_weight,
    route_expert,
    route_weight,
    expert_gate,
    expert_up,
    expert_down,
):
    token_count = query_proj.shape[0]
    local_heads = query_gain.shape[0]
    local_kv = key_gain.shape[0]
    group_size = local_heads // local_kv
    sp_size = lax.axis_size("sp")
    tp_size = lax.axis_size("tp")
    tp_place = lax.axis_index("tp")
    offset = lax.axis_index("sp") * token_count
    cosine_table, sine_table = rotation_tables(offset, token_count)
    query_rot = rotate(
        head_norm(query_proj.reshape(token_count, local_heads, HEAD_DIM), query_gain),
        cosine_table,
        sine_table,
    ).astype(jnp.bfloat16)
    key_rot = rotate(
        head_norm(key_proj.reshape(token_count, local_kv, HEAD_DIM), key_gain),
        cosine_table,
        sine_table,
    ).astype(jnp.bfloat16)
    packed = jnp.concatenate(
        [key_rot.reshape(token_count, local_kv * HEAD_DIM), value_proj], axis=1
    )
    query_groups = query_rot.reshape(token_count, local_kv, group_size, HEAD_DIM)
    initial = (
        jnp.full((local_kv, group_size, token_count), -1e30, jnp.float32),
        jnp.zeros((local_kv, group_size, token_count), jnp.float32),
        jnp.zeros((local_kv, group_size, token_count, HEAD_DIM), jnp.float32),
    )
    incoming = lax.all_gather(packed, "sp", axis=0, tiled=True)
    incoming_len = incoming.shape[0]
    step_len = math.gcd(incoming_len, KEY_BLOCK)

    def one_step(step_index, running):
        block_rows = lax.dynamic_slice_in_dim(incoming, step_index * step_len, step_len, 0)
        key_block = block_rows[:, : local_kv * HEAD_DIM].reshape(step_len, local_kv, HEAD_DIM)
        value_block = block_rows[:, local_kv * HEAD_DIM :].reshape(step_len, local_kv, HEAD_DIM)
        return online_update(running, query_groups, key_block, value_block)

    final_max, final_sum, final_acc = lax.fori_loop(0, incoming_len // step_len, one_step, initial)
    attended = final_acc / final_sum[..., None]
    attended = jnp.transpose(attended, (2, 0, 1, 3)).reshape(token_count, local_heads * HEAD_DIM)
    attended = attended.astype(jnp.bfloat16)
    projected = jnp.dot(
        lax.all_gather(attended, "tp", axis=1, tiled=True),
        out_weight,
        preferred_element_type=jnp.float32,
    )
    mixed_sum = residual.astype(jnp.float32) + projected
    mixed_rows = mixed_sum.astype(jnp.bfloat16)
    full_rows = lax.all_gather(mixed_rows, "tp", axis=1, tiled=True)
    width_total = full_rows.shape[1]
    per_sp = tp_size // 2
    column = tp_place // 2
    experts_total = per_sp * sp_size
    capacity = 3 * token_count * TOP_K // (2 * experts_total)
    slot_count = sp_size * capacity
    flat_choice = route_expert.reshape(token_count * TOP_K)
    onehot = (flat_choice[:, None] == jnp.arange(experts_total, dtype=jnp.int32)[None, :]).astype(
        jnp.int32
    )
    earlier = jnp.cumsum(onehot, axis=0) - onehot
    slot_rank = jnp.sum(earlier * onehot, axis=1)
    mine = flat_choice % per_sp == column
    target = flat_choice // per_sp * capacity + slot_rank
    owner = jnp.arange(token_count * TOP_K, dtype=jnp.int32) // TOP_K
    slot_token = (
        jnp.full((slot_count + 1,), token_count, jnp.int32)
        .at[jnp.where(mine, target, slot_count)]
        .set(owner)[:slot_count]
    )
    padded = jnp.concatenate([full_rows, jnp.zeros((1, width_total), jnp.bfloat16)], axis=0)
    selected = padded[slot_token].reshape(sp_size, capacity, width_total)
    arrived = lax.all_to_all(selected, "sp", split_axis=0, concat_axis=0, tiled=True)
    expert_rows = arrived.reshape(slot_count, width_total)
    squares = jnp.mean(jnp.square(expert_rows.astype(jnp.float32)), axis=-1, keepdims=True)
    norm_scale = lax.rsqrt(squares + EPSILON)
    gate_value = (
        jnp.dot(expert_rows, expert_gate[0], preferred_element_type=jnp.float32) * norm_scale
    )
    up_value = jnp.dot(expert_rows, expert_up[0], preferred_element_type=jnp.float32) * norm_scale
    hidden = (jax.nn.silu(gate_value) * up_value).astype(jnp.bfloat16)
    half_result = jnp.dot(hidden, expert_down[0], preferred_element_type=jnp.float32).astype(
        jnp.bfloat16
    )
    returned = lax.all_to_all(
        half_result.reshape(sp_size, capacity, width_total),
        "sp",
        split_axis=0,
        concat_axis=0,
        tiled=True,
    )
    slot_results = returned.reshape(slot_count, width_total)
    mine_grid = mine.reshape(token_count, TOP_K)
    target_grid = target.reshape(token_count, TOP_K)
    gathered_sum = jnp.zeros((token_count, width_total), jnp.float32)
    for choice_index in range(TOP_K):
        chosen = mine_grid[:, choice_index]
        index = jnp.where(chosen, target_grid[:, choice_index], 0)
        factor = jnp.where(chosen, route_weight[:, choice_index], 0.0)
        picked = slot_results[index].astype(jnp.float32)
        gathered_sum = gathered_sum + factor[:, None] * picked
    routed = lax.psum_scatter(
        gathered_sum.astype(jnp.bfloat16), "tp", scatter_dimension=1, tiled=True
    ).astype(jnp.float32)
    return (mixed_sum + routed).astype(jnp.bfloat16)


def flip_index(index, mask):
    bit = 1
    while bit <= mask:
        if mask & bit:
            index = index + bit - 2 * bit * ((index // bit) % 2)
        bit *= 2
    return index


LANES = 128
SLOTS = 4
SEND_SEMS = 11
RECV_SEMS = 82
ORDER = (
    ("start",),
    ("p1",),
    ("x1", 0),
    ("z", 1, 0, None),
    ("p2",),
    ("z", 2, 0, "mid"),
    ("z", 1, 1, None),
    ("x1", 1),
    ("z", 2, 0, "end"),
    ("z", 2, 1, "mid"),
    ("z", 2, 1, "end"),
    ("x1", 2),
    ("z", 3, 0, "mid"),
    ("z", 3, 1, "mid"),
    ("pz",),
    ("z", 3, 1, "end"),
    ("z", 3, 0, "end"),
    ("x1", 3),
    ("x2", 1),
    ("zp", 1, None),
    ("x2", 2),
    ("x2", 0),
    ("zp", 2, "mid"),
    ("x2", 3),
    ("zp", 3, "mid"),
    ("c3", 2),
    ("zp", 2, "end"),
    ("hid", 2, 0),
    ("hs", 2, 0),
    ("c3", 1),
    ("hid", 2, 1),
    ("c3", 0),
    ("hs", 2, 1),
    ("hr", 2, 0),
    ("hr", 2, 1),
    ("zp", 3, "end"),
    ("c3", 3),
    ("hid", 3, 0),
    ("hs", 3, 0),
    ("hid", 3, 1),
    ("hs", 3, 1),
    ("part", 2),
    ("hr", 3, 0),
    ("hid", 1, 1),
    ("hr", 3, 1),
    ("hid", 1, 0),
    ("hs", 1, 0),
    ("hid", 0, 0),
    ("hs", 0, 0),
    ("red", 2),
    ("hs", 1, 1),
    ("part", 3),
    ("hr", 1, 0),
    ("hid", 0, 1),
    ("hr", 1, 1),
    ("hs", 0, 1),
    ("red", 3),
    ("part", 1),
    ("hr", 0, 1),
    ("hr", 0, 0),
    ("red", 1),
    ("part", 0),
    ("red", 0),
)


class Links:
    def __init__(self, send_sem, recv_sem, conditions, counting):
        self.send_sem, self.recv_sem = send_sem, recv_sem
        self.conditions, self.counting = conditions, counting
        self.recv_ids = {}
        self.groups, self.open_group = [], {}

    def copy(self, src, dst, device, send_id, recv_key):
        recv_id = self.recv_ids.setdefault(recv_key, len(self.recv_ids))
        assert recv_id < RECV_SEMS and send_id < SEND_SEMS
        return pltpu.make_async_remote_copy(
            src_ref=src,
            dst_ref=dst,
            send_sem=self.send_sem.at[send_id],
            recv_sem=self.recv_sem.at[recv_id],
            device_id=device,
            device_id_type=pl.DeviceIdType.MESH,
        )

    def counted(self, size):
        lines, width = self.counting.shape
        line = width * 2
        assert size % line == 0 and size // line <= lines
        return self.counting.at[pl.ds(0, size // line), :]

    def send(self, key, src, dst, device, recv_key=None, only=None):
        size = math.prod(src.shape) * jnp.dtype(src.dtype).itemsize
        group = self.open_group.get(only)
        if group is None or self.groups[group][0] + size > math.prod(self.counting.shape) * 2:
            group = self.open_group[only] = len(self.groups)
            self.groups.append([0, only, device])
        self.groups[group][0] += size
        copy = self.copy(src, dst, device, group, key if recv_key is None else recv_key)
        self.when(only, copy.start)

    def arrived(self, key, dst, device, only=None):
        if isinstance(dst, int):
            dst = self.counted(dst)
        self.when(only, self.copy(dst, dst, device, 0, key).wait_recv)

    def settle(self):
        for group, (size, only, device) in enumerate(self.groups):
            block = self.counted(size)
            self.when(only, self.copy(block, block, device, group, next(iter(self.recv_ids))).wait_send)

    def when(self, only, act):
        if only is None:
            act()
        else:
            pl.when(self.conditions[only])(act)


def fused_kernel(
    q_ref,
    k_ref,
    v_ref,
    q_gain_ref,
    k_gain_ref,
    residual_ref,
    expert_ref,
    weight_ref,
    out_weight_hbm,
    gate_hbm,
    up_hbm,
    down_hbm,
    out_ref,
    kv,
    queries,
    run_max,
    run_acc,
    attended,
    mixed,
    rows,
    out_weight,
    gate_up,
    down,
    tables,
    hid,
    hid_own,
    part_own,
    part_send,
    part_in,
    local_sem,
    send_sem,
    recv_sem,
):
    f32, bf16 = jnp.float32, jnp.bfloat16
    count, width = q_ref.shape
    pairs = width // LANES
    halves = pairs // 2
    hidden_units = gate_hbm.shape[2]
    capacity = hid.shape[3]
    upper_tok, lower_tok = pl.ds(0, count // 2), pl.ds(count // 2, count // 2)
    shared = count // 4
    rest = count - shared
    plane_tok, line_tok = pl.ds(0, shared), pl.ds(shared, rest)
    plane_half = [pl.ds(p * (shared // 2), shared // 2) for p in range(2)]
    line_half = [pl.ds(shared + p * (rest // 2), rest // 2) for p in range(2)]
    upper_cap, lower_cap = pl.ds(0, capacity // 2), pl.ds(capacity // 2, capacity // 2)

    sp_place, tp_place = lax.axis_index("sp"), lax.axis_index("tp")
    plane, core_place = sp_place // 2, sp_place % 2
    is_mid = (plane == 1) | (plane == 2)
    is_end = (plane == 0) | (plane == 3)

    def at(sp_mask, tp_mask):
        return {"sp": flip_index(sp_place, sp_mask), "tp": flip_index(tp_place, tp_mask)}

    core, near, far = at(1, 0), at(2, 0), at(6, 0)
    across = [None, at(0, 1), at(0, 2), at(0, 3)]
    across_core = [core, at(1, 1), at(1, 2)]
    links = Links(send_sem, recv_sem, {"mid": is_mid, "end": is_end}, out_weight)

    def size_of(ref):
        return math.prod(ref.shape) * jnp.dtype(ref.dtype).itemsize


    quarters = [flip_index(tp_place, q) * width for q in range(4)]

    def columns(q):
        return pl.ds(pl.multiple_of(quarters[q], width), width)

    loads = [
        pltpu.make_async_copy(out_weight_hbm, out_weight, local_sem.at[0]),
        pltpu.make_async_copy(
            gate_hbm.at[0], gate_up.at[:, pl.ds(0, hidden_units)], local_sem.at[1]
        ),
        pltpu.make_async_copy(
            up_hbm.at[0], gate_up.at[:, pl.ds(hidden_units, hidden_units)], local_sem.at[2]
        ),
        pltpu.make_async_copy(down_hbm.at[0, :, columns(0)], down.at[0, 0], local_sem.at[3]),
    ]

    barrier = pltpu.get_barrier_semaphore()
    partners = [core, near, far] + across[1:] + across_core[1:]
    for partner in partners:
        pl.semaphore_signal(
            barrier, inc=1, device_id=partner, device_id_type=pl.DeviceIdType.MESH
        )

    lane = lax.broadcasted_iota(jnp.int32, (count, LANES), 1)
    first_head = lane < HEAD_DIM
    quarter = HEAD_DIM // 4
    even_quarter = (lane // quarter) % 2 == 0

    grid_rows = count // GRID_W
    token = lax.broadcasted_iota(jnp.int32, (GRID_W + 8, LANES), 0)
    lane_short = lax.broadcasted_iota(jnp.int32, (GRID_W + 8, LANES), 1)
    place = jnp.where(token < GRID_W, token, sp_place * grid_rows + token - GRID_W)
    power = (lane_short % quarter).astype(f32) * (-math.log(ROPE_BASE) / quarter)
    angle = place.astype(f32) * jnp.exp(power)
    sign = jnp.where((lane_short // quarter) % 2 == 0, -1.0, 1.0)

    def over_tokens(short):
        parts = []
        by_row = ((lane_short[:GRID_W] // quarter) % 4) < 2
        for r in range(grid_rows):
            line = short[GRID_W + r : GRID_W + r + 1, :]
            parts.append(jnp.where(by_row, line, short[:GRID_W, :]))
        return jnp.concatenate(parts, axis=0)

    cosine = over_tokens(jnp.cos(angle))
    sine = over_tokens(jnp.sin(angle) * sign)

    def pair_gain(gain_ref, pair):
        return jnp.concatenate(
            [gain_ref[2 * pair : 2 * pair + 1, :], gain_ref[2 * pair + 1 : 2 * pair + 2, :]],
            axis=1,
        )

    def norm_rotate(block, gain):
        wide = block.astype(f32)
        squares = wide * wide
        low = jnp.sum(jnp.where(first_head, squares, 0.0), axis=-1, keepdims=True)
        high = jnp.sum(jnp.where(first_head, 0.0, squares), axis=-1, keepdims=True)
        mean = jnp.where(first_head, low, high) * (1.0 / HEAD_DIM)
        scaled = wide * lax.rsqrt(mean + EPSILON) * gain
        ahead = pltpu.roll(scaled, LANES - quarter, 1)
        behind = pltpu.roll(scaled, quarter, 1)
        swapped = jnp.where(even_quarter, ahead, behind)
        return scaled * cosine + swapped * sine

    for h in range(halves):
        block = pl.ds(h * LANES, LANES)
        flipped = jnp.transpose(v_ref[:, block].astype(f32)).astype(bf16)
        for part in range(count // LANES):
            kv[h, 0, 0, 1, pl.ds(part * LANES, LANES), :] = flipped[
                :, part * LANES : (part + 1) * LANES
            ]
        kv[h, 0, 0, 0] = norm_rotate(k_ref[:, block], pair_gain(k_gain_ref, h)).astype(bf16)

    pl.semaphore_wait(barrier, len(partners))

    def line_start(name, ref_at):
        links.send(None, ref_at(0), ref_at(1), near, (*name, 1))
        links.send(None, ref_at(0), ref_at(2), far, (*name, 2), "mid")

    def line_on(name, slot, ref_at, only=None):
        if only == "end":
            return
        if slot == 1:
            links.send(None, ref_at(1), ref_at(3), far, (*name, 3), "mid")
        else:
            links.send(None, ref_at(slot), ref_at(slot), near, (*name, slot), "mid")

    def line_wait(name, slot, ref_at, only=None):
        links.arrived((*name, slot), ref_at(slot), near, only)
        line_on(name, slot, ref_at, only)

    def kv_at(h):
        return lambda slot: kv.at[h, slot, 0]

    def kv_swap(h, slot, only=None):
        links.send(("kvc", h, slot), kv.at[h, slot, 0], kv.at[h, slot, 1], core, only=only)

    def table_at(slot):
        return tables.at[slot, 0]

    def table_swap(slot, only=None):
        links.send(("kvc", halves - 1, slot), tables.at[slot, 0], tables.at[slot, 1], core, only=only)

    def take_kv(h, slot, only=None):
        last = h == halves - 1
        size = size_of(kv_at(h)(slot)) + (size_of(table_at(slot)) if last else 0)
        links.arrived(("kv", h, slot), size, near, only)
        line_on(("kv", h), slot, kv_at(h), only)
        kv_swap(h, slot, only)
        if last:
            line_on(("kv", h), slot, table_at, only)
            table_swap(slot, only)

    for h in range(halves):
        line_start(("kv", h), kv_at(h))
    for h in range(halves):
        kv_swap(h, 0)
    experts_total = tables.shape[2]
    names, factors = expert_ref[...], weight_ref[...]
    wanted = lax.broadcasted_iota(jnp.int32, (experts_total, count), 0)
    table = jnp.zeros((experts_total, count), f32)
    for k in range(TOP_K):
        table = table + jnp.where(names[k : k + 1, :] == wanted, factors[k : k + 1, :], 0.0)
    tables[0, 0] = table
    line_start(("kv", halves - 1), table_at)
    table_swap(0)
    for q in (1, 2, 3):
        links.send("down", down_hbm.at[0, :, columns(q)], down.at[0, q], across[q])
    for load in loads:
        load.start()

    for g in range(pairs):
        turned = norm_rotate(q_ref[:, pl.ds(g * LANES, LANES)], pair_gain(q_gain_ref, g))
        turned = turned.astype(bf16).astype(f32)
        other = pltpu.roll(turned, HEAD_DIM, 1)
        if g % 2 == 0:
            top, bottom = jnp.where(first_head, turned, 0.0), jnp.where(first_head, other, 0.0)
        else:
            top, bottom = jnp.where(first_head, 0.0, other), jnp.where(first_head, 0.0, turned)
        queries[g, pl.ds(0, count), :] = top.astype(bf16)
        queries[g, pl.ds(count, count), :] = bottom.astype(bf16)

    ones = jnp.ones((16, 2 * count), bf16)
    exponent = math.log2(math.e) * HEAD_DIM ** (-0.5)

    def attend(h, slot):
        def one(i, carry):
            g = 2 * h + i
            keys = kv[h, slot, :, 0].reshape(2 * count, LANES)
            values = [
                kv[h, slot, side, 1, pl.ds(part * LANES, LANES), :]
                for side in range(2)
                for part in range(count // LANES)
            ]
            values = jnp.concatenate(values, axis=1)
            values = jnp.concatenate([values, ones], axis=0)
            scores = lax.dot_general(
                keys, queries[g], (((1,), (1,)), ((), ())), preferred_element_type=f32
            )
            block_max = jnp.max(scores, axis=0, keepdims=True)
            if slot == 0:
                new_max = block_max
            else:
                old_max = run_max[g]
                new_max = jnp.maximum(old_max, block_max)
            weights = jnp.exp2((scores - new_max) * exponent).astype(bf16)
            update = jnp.dot(values, weights, preferred_element_type=f32)
            if slot:
                rescale = jnp.exp2((old_max - new_max) * exponent)
                update = update + run_acc[g] * rescale
            run_max[g] = new_max
            run_acc[g] = update
            return carry

        lax.fori_loop(0, 2, one, 0)

    def own_half(q, h):
        offset = quarters[q] + h * 2 * LANES
        return pl.ds(pl.multiple_of(offset, 2 * LANES), 2 * LANES)

    def attend_end(h):
        tiles = []
        for i in range(2):
            total = run_acc[2 * h + i]
            out = total[i * HEAD_DIM : (i + 1) * HEAD_DIM] / total[LANES : LANES + 1]
            heads = jnp.concatenate([out[:, :count], out[:, count:]], axis=0)
            tiles.append(jnp.transpose(heads).astype(bf16))
        attended[:, own_half(0, h)] = jnp.concatenate(tiles, axis=1)
        block = attended.at[:, own_half(0, h)]
        for q in (1, 2):
            links.send(("att", h, q), block, block, across[q])

    def attend_relay(h):
        links.arrived(("att", h, 2), attended.at[:, own_half(2, h)], across[2])
        block = attended.at[upper_tok, own_half(2, h)]
        links.send(("att", h, 3), block, block, across[1])
        links.arrived(("att", h, 1), attended.at[:, own_half(1, h)], across[1])
        block = attended.at[lower_tok, own_half(1, h)]
        links.send(("att", h, 3), block, block, across[2])

    def attend_chunk(h, slot):
        size = size_of(kv.at[h, slot, 1])
        if h == halves - 1:
            size += size_of(tables.at[slot, 1])
        links.arrived(("kvc", h, slot), size, core)
        attend(h, slot)

    attend_chunk(0, 0)
    take_kv(0, 1)
    take_kv(0, 2, "mid")
    attend_chunk(1, 0)
    attend_chunk(0, 1)
    take_kv(1, 1)
    take_kv(1, 2, "mid")
    attend_chunk(1, 1)
    take_kv(0, 2, "end")
    attend_chunk(0, 2)
    take_kv(0, 3, "mid")
    take_kv(1, 2, "end")
    attend_chunk(1, 2)
    loads[3].wait()
    links.arrived("down", down.at[0, pl.ds(1, 3)], core)
    links.send("downc", down.at[0], down.at[1], core)
    take_kv(1, 3, "mid")
    take_kv(0, 3, "end")
    attend_chunk(0, 3)
    attend_end(0)
    take_kv(1, 3, "end")
    attend_chunk(1, 3)
    attend_end(1)

    loads[0].wait()
    mixed[...] = residual_ref[...].astype(f32)

    def project(q, h):
        mixed[...] += jnp.dot(
            attended[:, own_half(q, h)],
            out_weight[own_half(q, h), :],
            preferred_element_type=f32,
        )

    for h in range(halves):
        project(0, h)
    for h in range(halves):
        attend_relay(h)
        project(1, h)
        project(2, h)
    for h in range(halves):
        links.arrived(("att", h, 3), attended.at[:, own_half(3, h)], across[3])
        project(3, h)
    rows[0, 0, :, columns(0)] = mixed[...].astype(bf16)

    def rows_at(part):
        return lambda slot: rows.at[slot, 0, line_half[part], columns(0)]

    def wide_at(slot):
        return rows.at[slot, 0, plane_tok, :]

    def to_core(slot, q):
        links.send(
            ("rowc", slot),
            rows.at[slot, 0, line_tok, columns(q)],
            rows.at[slot, 1, line_tok, columns(q)],
            core,
        )

    def wide_to_core(slot, only=None):
        links.send(
            ("rowc", slot), wide_at(slot), rows.at[slot, 1, plane_tok, :], core, only=only
        )

    def spread_one(name, slot, span):
        block = rows.at[slot, 0, span, columns(0)]
        links.send((name, "x1", slot), block, block, across[1])
        links.send((name, "y1", slot), block, block, across[2])

    def spread_two(name, slot, span, half):
        links.arrived((name, "y1", slot), rows.at[slot, 0, span, columns(2)], across[2])
        block = rows.at[slot, 0, half[0], columns(2)]
        links.send((name, "xy", slot), block, block, across[1])
        links.arrived((name, "x1", slot), rows.at[slot, 0, span, columns(1)], across[1])
        block = rows.at[slot, 0, half[1], columns(1)]
        links.send((name, "xy", slot), block, block, across[2])

    def spread_three(name, slot, span):
        links.arrived((name, "xy", slot), rows.at[slot, 0, span, columns(3)], across[3])

    def spread(slot):
        spread_one("row", slot, line_tok)
        to_core(slot, 0)

    def spread_on(slot):
        spread_two("row", slot, line_tok, line_half)
        to_core(slot, 1)
        to_core(slot, 2)

    def spread_end(slot):
        spread_three("row", slot, line_tok)
        to_core(slot, 3)

    def take(slot, part, only=None):
        line_wait(("row", part), slot, rows_at(part), only)

    def share():
        spread_one("wide", 0, plane_tok)

    def share_on():
        spread_two("wide", 0, plane_tok, plane_half)

    def share_end():
        spread_three("wide", 0, plane_tok)
        line_start(("wide",), wide_at)
        wide_to_core(0)

    def take_wide(slot, only=None):
        line_wait(("wide",), slot, wide_at, only)
        wide_to_core(slot, only)

    before = lax.broadcasted_iota(jnp.int32, (count, count), 0) < lax.broadcasted_iota(
        jnp.int32, (count, count), 1
    )
    before = before.astype(f32).astype(bf16)

    def ranks(table):
        chosen = table > 0.0
        marks = chosen.astype(f32).astype(bf16)
        rank = jnp.dot(marks, before, preferred_element_type=f32)
        return jnp.where(chosen, rank, -1.0)

    slot_of = lax.broadcasted_iota(jnp.int32, (capacity, count), 0).astype(f32)
    slot_in = lax.broadcasted_iota(jnp.int32, (count, capacity), 1).astype(f32)
    pair_count = experts_total // SLOTS
    my_expert = plane * pair_count + core_place * 2 + tp_place // 2
    expert_row = lax.broadcasted_iota(jnp.int32, (experts_total, count), 0)

    def hidden(slot, side):
        if side:
            links.arrived(("rowc", slot), rows.at[slot, 1], core)
        block = rows[slot, side]
        wide = block.astype(f32)
        squares = jnp.mean(wide * wide, axis=-1, keepdims=True)
        norm_scale = lax.rsqrt(squares + EPSILON)
        both = jnp.dot(block, gate_up[...], preferred_element_type=f32) * norm_scale
        gate_value, up_value = both[:, :hidden_units], both[:, hidden_units:]
        result = (gate_value / (1.0 + jnp.exp(-gate_value)) * up_value).astype(bf16)
        rank = ranks(tables[slot, side])
        mine = jnp.sum(jnp.where(expert_row == my_expert, rank, 0.0), axis=0, keepdims=True)
        pick = (slot_of == mine).astype(f32).astype(bf16)
        packed = jnp.dot(pick, result, preferred_element_type=f32).astype(bf16)
        hid_own[slot, side] = packed

    def hid_send(slot, side):
        for q in (1, 2):
            links.send(
                ("h", slot, q, side),
                hid_own.at[slot, side],
                hid.at[slot, q, side],
                (across, across_core)[side][q],
            )
        if side:
            links.send(("hall", slot), hid_own.at[slot, 1], hid.at[slot, 0, 1], core)

    def hid_relay(slot, cc):
        links.arrived(("h", slot, 2, cc), hid.at[slot, 2, cc], across[2])
        links.send(
            ("hall", slot),
            hid.at[slot, 2, cc, upper_cap, :],
            hid.at[slot, 3, cc, upper_cap, :],
            across[1],
        )
        links.arrived(("h", slot, 1, cc), hid.at[slot, 1, cc], across[1])
        links.send(
            ("hall", slot),
            hid.at[slot, 1, cc, lower_cap, :],
            hid.at[slot, 3, cc, lower_cap, :],
            across[2],
        )

    def partial(slot):
        links.arrived(("hall", slot), 3 * size_of(hid.at[slot, 3, 0]), core)
        table = tables[slot, 0]
        rank_column = jnp.transpose(ranks(table))
        weight_column = jnp.transpose(table)
        column = lax.broadcasted_iota(jnp.int32, (count, experts_total), 1)
        mixed_in = jnp.zeros((count, width), f32)
        for cc in range(2):
            for qy in range(2):
                results = [
                    jnp.dot(
                        hid[slot, 2 * qy + qx, cc] if qx + qy + cc else hid_own[slot, 0],
                        down[cc, 2 * qy + qx],
                        preferred_element_type=f32,
                    ).astype(bf16)
                    for qx in range(2)
                ]
                expert = (
                    plane * pair_count
                    + flip_index(core_place, cc) * 2
                    + flip_index(tp_place // 2, qy)
                )
                this = column == expert
                rank = jnp.sum(jnp.where(this, rank_column, 0.0), axis=1, keepdims=True)
                weight = jnp.sum(jnp.where(this, weight_column, 0.0), axis=1, keepdims=True)
                place = (slot_in == rank).astype(f32).astype(bf16)
                both = jnp.dot(place, results[0], preferred_element_type=f32) + jnp.dot(
                    place, results[1], preferred_element_type=f32
                )
                mixed_in = mixed_in + both * weight
        return mixed_in

    tokens = (upper_tok, lower_tok)

    def send_back(slot):
        value = partial(slot)
        if slot == 0:
            mixed[...] += value
            return
        part_own[slot] = value
        part_send[slot] = value.astype(bf16)
        for p, span in enumerate(tokens):
            links.send(
                ("e", slot, p),
                part_send.at[slot, span],
                part_in.at[slot - 1, span],
                near,
                ("pe", slot, p),
                "end",
            )

    def pass_back(slot):
        for p, span in enumerate(tokens):
            if slot == 0:
                links.arrived(("pm", 1, p), part_in.at[0, span], near, "end")
                links.arrived(("pe", 1, p), part_in.at[0, span], near, "mid")
                links.arrived(("pm", 2, p), part_in.at[3, span], far, "mid")
                continue
            source = 4 if slot == 1 else slot - 1
            if slot == 1:
                links.arrived(("pm", 3, p), part_in.at[source, span], far, "mid")
            else:
                links.arrived(("pe", slot, p), part_in.at[source, span], near, "mid")

            @pl.when(is_mid)
            def _():
                total = part_own[slot, span] + part_in[source, span].astype(f32)
                part_send[slot, span] = total.astype(bf16)

            block = part_send.at[slot, span]
            if slot == 1:
                links.send(("m", 1, p), block, part_in.at[0, span], near, ("pm", 1, p), "mid")
            else:
                target = part_in.at[1 + slot, span]
                links.send(("m", slot, p), block, target, far, ("pm", slot, p), "mid")
        if slot == 0:
            total = mixed[...] + part_in[0].astype(f32)
            out_ref[...] = total.astype(bf16)

            @pl.when(is_mid)
            def _():
                out_ref[...] = (total + part_in[3].astype(f32)).astype(bf16)

    def start_rows():
        for part in range(2):
            line_start(("row", part), rows_at(part))

    steps = {
        "start": start_rows,
        "z": take,
        "p1": share,
        "p2": share_on,
        "pz": share_end,
        "zp": take_wide,
        "x1": spread,
        "x2": spread_on,
        "c3": spread_end,
        "hid": hidden,
        "hs": hid_send,
        "hr": hid_relay,
        "part": send_back,
        "red": pass_back,
    }
    loads[1].wait()
    loads[2].wait()
    links.arrived("downc", down.at[1], core)
    for step, *where in ORDER:
        steps[step](*where)
    links.settle()


def local_fused(
    query_proj,
    key_proj,
    value_proj,
    query_gain,
    key_gain,
    residual,
    out_weight,
    route_expert,
    route_weight,
    expert_gate,
    expert_up,
    expert_down,
):
    token_count, width = query_proj.shape
    local_kv = key_gain.shape[0]
    total = out_weight.shape[0]
    hidden_units = expert_gate.shape[2]
    experts_total = lax.axis_size("sp") * lax.axis_size("tp") // 2
    capacity = 3 * token_count * TOP_K // (2 * experts_total)
    f32, bf16 = jnp.float32, jnp.bfloat16

    vmem = pl.BlockSpec(memory_space=pltpu.VMEM)
    hbm = pl.BlockSpec(memory_space=pltpu.HBM)
    halves = local_kv // 2
    scratch = [
        pltpu.VMEM((halves, SLOTS, 2, 2, token_count, LANES), bf16),
        pltpu.VMEM((local_kv, 2 * token_count, LANES), bf16),
        pltpu.VMEM((local_kv, 1, 2 * token_count), f32),
        pltpu.VMEM((local_kv, LANES + 16, 2 * token_count), f32),
        pltpu.VMEM((token_count, total), bf16),
        pltpu.VMEM((token_count, width), f32),
        pltpu.VMEM((SLOTS, 2, token_count, total), bf16),
        pltpu.VMEM((total, width), bf16),
        pltpu.VMEM((total, 2 * hidden_units), bf16),
        pltpu.VMEM((2, 4, hidden_units, width), bf16),
        pltpu.VMEM((SLOTS, 2, experts_total, token_count), f32),
        pltpu.VMEM((SLOTS, 4, 2, capacity, hidden_units), bf16),
        pltpu.VMEM((SLOTS, 2, capacity, hidden_units), bf16),
        pltpu.VMEM((SLOTS, token_count, width), f32),
        pltpu.VMEM((SLOTS, token_count, width), bf16),
        pltpu.VMEM((5, token_count, width), bf16),
        pltpu.SemaphoreType.DMA((4,)),
        pltpu.SemaphoreType.DMA((SEND_SEMS,)),
        pltpu.SemaphoreType.DMA((RECV_SEMS,)),
    ]
    result = pl.pallas_call(
        fused_kernel,
        out_shape=jax.ShapeDtypeStruct((token_count, width), bf16),
        in_specs=[vmem] * 8 + [hbm] * 4,
        out_specs=vmem,
        scratch_shapes=scratch,
        compiler_params=pltpu.CompilerParams(
            collective_id=0, has_side_effects=True, vmem_limit_bytes=56 * 1024 * 1024
        ),
    )(
        query_proj,
        key_proj,
        value_proj,
        query_gain,
        key_gain,
        residual,
        route_expert.T,
        route_weight.T,
        out_weight,
        expert_gate,
        expert_up,
        expert_down,
    )
    return result


def takes_fused(mesh):
    chips = mesh.shape["sp"] // 2
    experts_total = mesh.shape["sp"] * mesh.shape["tp"] // 2
    return mesh.shape["tp"] == 4 and chips == SLOTS and experts_total == 2 * TOP_K


def solution(mesh):
    in_specs = (
        P("sp", "tp"),
        P("sp", "tp"),
        P("sp", "tp"),
        P("tp", None),
        P("tp", None),
        P("sp", "tp"),
        P(None, "tp"),
        P("sp", None),
        P("sp", None),
        P(("sp", "tp"), None, None),
        P(("sp", "tp"), None, None),
        P(("sp", "tp"), None, None),
    )
    out_specs = P("sp", "tp")
    body = local_fused if takes_fused(mesh) else local
    return jax.shard_map(body, mesh=mesh, in_specs=in_specs, out_specs=out_specs, check_vma=False)
```

```python
import functools
import math

import jax
import jax.numpy as jnp
from jax import lax
from jax.experimental import pallas as pl
from jax.experimental.pallas import tpu as pltpu
from jax.sharding import PartitionSpec as P

HEAD_DIM = 64
TOP_K = 8
GRID_W = 64


EPSILON = 1e-06
ROPE_BASE = 10000.0
KEY_BLOCK = 1024


def rotation_tables(offset, count):
    pair_count = HEAD_DIM // 4
    position = offset + jnp.arange(count, dtype=jnp.int32)
    grid_row = (position // GRID_W).astype(jnp.float32)
    grid_col = (position % GRID_W).astype(jnp.float32)
    inverse = ROPE_BASE ** (-jnp.arange(pair_count, dtype=jnp.float32) / pair_count)
    angles = jnp.stack([grid_row[:, None] * inverse, grid_col[:, None] * inverse], axis=1)
    return (jnp.cos(angles), jnp.sin(angles))


def rotate(vectors, cosine_table, sine_table):
    pair_count = HEAD_DIM // 4
    shaped = vectors.reshape(vectors.shape[:-1] + (2, 2, pair_count))
    first_half = shaped[..., 0, :]
    second_half = shaped[..., 1, :]
    cosine_row = cosine_table[:, None]
    sine_row = sine_table[:, None]
    turned = jnp.stack(
        [
            first_half * cosine_row - second_half * sine_row,
            first_half * sine_row + second_half * cosine_row,
        ],
        axis=-2,
    )
    return turned.reshape(vectors.shape)


def head_norm(vectors, gain):
    scaled = vectors.astype(jnp.float32)
    scaled = scaled * lax.rsqrt(jnp.mean(scaled * scaled, axis=-1, keepdims=True) + EPSILON)
    return scaled * gain


def online_update(running, query_groups, key_block, value_block):
    running_max, running_sum, running_acc = running
    scores = jnp.einsum(
        "tkgd,nkd->kgtn", query_groups, key_block, preferred_element_type=jnp.float32
    ) * HEAD_DIM ** (-0.5)
    new_max = jnp.maximum(running_max, jnp.max(scores, axis=-1))
    rescale = jnp.exp(running_max - new_max)
    weights = jnp.exp(scores - new_max[..., None]).astype(jnp.bfloat16)
    new_sum = running_sum * rescale + jnp.sum(weights.astype(jnp.float32), axis=-1)
    update = jnp.einsum("kgtn,nkd->kgtd", weights, value_block, preferred_element_type=jnp.float32)
    return (new_max, new_sum, running_acc * rescale[..., None] + update)


def local(
    query_proj,
    key_proj,
    value_proj,
    query_gain,
    key_gain,
    residual,
    out_weight,
    route_expert,
    route_weight,
    expert_gate,
    expert_up,
    expert_down,
):
    token_count = query_proj.shape[0]
    local_heads = query_gain.shape[0]
    local_kv = key_gain.shape[0]
    group_size = local_heads // local_kv
    sp_size = lax.axis_size("sp")
    tp_size = lax.axis_size("tp")
    tp_place = lax.axis_index("tp")
    offset = lax.axis_index("sp") * token_count
    cosine_table, sine_table = rotation_tables(offset, token_count)
    query_rot = rotate(
        head_norm(query_proj.reshape(token_count, local_heads, HEAD_DIM), query_gain),
        cosine_table,
        sine_table,
    ).astype(jnp.bfloat16)
    key_rot = rotate(
        head_norm(key_proj.reshape(token_count, local_kv, HEAD_DIM), key_gain),
        cosine_table,
        sine_table,
    ).astype(jnp.bfloat16)
    packed = jnp.concatenate(
        [key_rot.reshape(token_count, local_kv * HEAD_DIM), value_proj], axis=1
    )
    query_groups = query_rot.reshape(token_count, local_kv, group_size, HEAD_DIM)
    initial = (
        jnp.full((local_kv, group_size, token_count), -1e30, jnp.float32),
        jnp.zeros((local_kv, group_size, token_count), jnp.float32),
        jnp.zeros((local_kv, group_size, token_count, HEAD_DIM), jnp.float32),
    )
    incoming = lax.all_gather(packed, "sp", axis=0, tiled=True)
    incoming_len = incoming.shape[0]
    step_len = math.gcd(incoming_len, KEY_BLOCK)

    def one_step(step_index, running):
        block_rows = lax.dynamic_slice_in_dim(incoming, step_index * step_len, step_len, 0)
        key_block = block_rows[:, : local_kv * HEAD_DIM].reshape(step_len, local_kv, HEAD_DIM)
        value_block = block_rows[:, local_kv * HEAD_DIM :].reshape(step_len, local_kv, HEAD_DIM)
        return online_update(running, query_groups, key_block, value_block)

    final_max, final_sum, final_acc = lax.fori_loop(0, incoming_len // step_len, one_step, initial)
    attended = final_acc / final_sum[..., None]
    attended = jnp.transpose(attended, (2, 0, 1, 3)).reshape(token_count, local_heads * HEAD_DIM)
    attended = attended.astype(jnp.bfloat16)
    projected = jnp.dot(
        lax.all_gather(attended, "tp", axis=1, tiled=True),
        out_weight,
        preferred_element_type=jnp.float32,
    )
    mixed_sum = residual.astype(jnp.float32) + projected
    mixed_rows = mixed_sum.astype(jnp.bfloat16)
    full_rows = lax.all_gather(mixed_rows, "tp", axis=1, tiled=True)
    width_total = full_rows.shape[1]
    per_sp = tp_size // 2
    column = tp_place // 2
    experts_total = per_sp * sp_size
    capacity = 3 * token_count * TOP_K // (2 * experts_total)
    slot_count = sp_size * capacity
    flat_choice = route_expert.reshape(token_count * TOP_K)
    onehot = (flat_choice[:, None] == jnp.arange(experts_total, dtype=jnp.int32)[None, :]).astype(
        jnp.int32
    )
    earlier = jnp.cumsum(onehot, axis=0) - onehot
    slot_rank = jnp.sum(earlier * onehot, axis=1)
    mine = flat_choice % per_sp == column
    target = flat_choice // per_sp * capacity + slot_rank
    owner = jnp.arange(token_count * TOP_K, dtype=jnp.int32) // TOP_K
    slot_token = (
        jnp.full((slot_count + 1,), token_count, jnp.int32)
        .at[jnp.where(mine, target, slot_count)]
        .set(owner)[:slot_count]
    )
    padded = jnp.concatenate([full_rows, jnp.zeros((1, width_total), jnp.bfloat16)], axis=0)
    selected = padded[slot_token].reshape(sp_size, capacity, width_total)
    arrived = lax.all_to_all(selected, "sp", split_axis=0, concat_axis=0, tiled=True)
    expert_rows = arrived.reshape(slot_count, width_total)
    squares = jnp.mean(jnp.square(expert_rows.astype(jnp.float32)), axis=-1, keepdims=True)
    norm_scale = lax.rsqrt(squares + EPSILON)
    gate_value = (
        jnp.dot(expert_rows, expert_gate[0], preferred_element_type=jnp.float32) * norm_scale
    )
    up_value = jnp.dot(expert_rows, expert_up[0], preferred_element_type=jnp.float32) * norm_scale
    hidden = (jax.nn.silu(gate_value) * up_value).astype(jnp.bfloat16)
    half_result = jnp.dot(hidden, expert_down[0], preferred_element_type=jnp.float32).astype(
        jnp.bfloat16
    )
    returned = lax.all_to_all(
        half_result.reshape(sp_size, capacity, width_total),
        "sp",
        split_axis=0,
        concat_axis=0,
        tiled=True,
    )
    slot_results = returned.reshape(slot_count, width_total)
    mine_grid = mine.reshape(token_count, TOP_K)
    target_grid = target.reshape(token_count, TOP_K)
    gathered_sum = jnp.zeros((token_count, width_total), jnp.float32)
    for choice_index in range(TOP_K):
        chosen = mine_grid[:, choice_index]
        index = jnp.where(chosen, target_grid[:, choice_index], 0)
        factor = jnp.where(chosen, route_weight[:, choice_index], 0.0)
        picked = slot_results[index].astype(jnp.float32)
        gathered_sum = gathered_sum + factor[:, None] * picked
    routed = lax.psum_scatter(
        gathered_sum.astype(jnp.bfloat16), "tp", scatter_dimension=1, tiled=True
    ).astype(jnp.float32)
    return (mixed_sum + routed).astype(jnp.bfloat16)


def flip_index(index, mask):
    bit = 1
    while bit <= mask:
        if mask & bit:
            index = index + bit - 2 * bit * ((index // bit) % 2)
        bit *= 2
    return index


LANES = 128
SLOTS = 4
SEND_SEMS = 11
RECV_SEMS = 100
PARTS = 4
ORDER = (
    ("start",),
    ("p1",),
    ("x1", 0),
    ("z", 2, 0, "mid"),
    ("p2",),
    ("z", 1, 0, None),
    ("z", 1, 1, None),
    ("z", 2, 1, "mid"),
    ("x1", 1),
    ("z", 3, 0, "mid"),
    ("z", 3, 1, "mid"),
    ("pz",),
    ("z", 2, 0, "end"),
    ("z", 2, 1, "end"),
    ("x1", 2),
    ("z", 3, 0, "end"),
    ("x2", 0),
    ("z", 3, 1, "end"),
    ("x1", 3),
    ("zp", 1, None),
    ("x2", 2),
    ("x2", 1),
    ("zp", 2, "mid"),
    ("x2", 3),
    ("zp", 3, "mid"),
    ("c3", 2),
    ("zp", 2, "end"),
    ("c3", 0),
    ("hid", 2, 0),
    ("hs", 2, 0),
    ("hid", 2, 1),
    ("hs", 2, 1),
    ("c3", 1),
    ("zp", 3, "end"),
    ("c3", 3),
    ("hid", 3, 0),
    ("hs", 3, 0),
    ("hid", 3, 1),
    ("hs", 3, 1),
    ("hr", 3, 0),
    ("hid", 0, 1),
    ("hr", 3, 1),
    ("hr", 2, 1),
    ("hr", 2, 0),
    ("hid", 1, 1),
    ("hid", 1, 0),
    ("hs", 1, 0),
    ("hs", 1, 1),
    ("part", 3),
    ("hs", 0, 1),
    ("hid", 0, 0),
    ("part", 2),
    ("hr", 1, 0),
    ("hr", 1, 1),
    ("hs", 0, 0),
    ("red", 3),
    ("part", 1),
    ("red", 1),
    ("hr", 0, 1),
    ("hr", 0, 0),
    ("red", 2),
    ("part", 0),
    ("red", 0),
)


class Links:
    def __init__(self, send_sem, recv_sem, conditions, counting):
        self.send_sem, self.recv_sem = send_sem, recv_sem
        self.conditions, self.counting = conditions, counting
        self.recv_ids = {}
        self.groups, self.open_group = [], {}

    def copy(self, src, dst, device, send_id, recv_key):
        recv_id = self.recv_ids.setdefault(recv_key, len(self.recv_ids))
        assert recv_id < RECV_SEMS and send_id < SEND_SEMS
        return pltpu.make_async_remote_copy(
            src_ref=src,
            dst_ref=dst,
            send_sem=self.send_sem.at[send_id],
            recv_sem=self.recv_sem.at[recv_id],
            device_id=device,
            device_id_type=pl.DeviceIdType.MESH,
        )

    def counted(self, size):
        lines, width = self.counting.shape
        line = width * 2
        assert size % line == 0 and size // line <= lines
        return self.counting.at[pl.ds(0, size // line), :]

    def send(self, key, src, dst, device, recv_key=None, only=None):
        size = math.prod(src.shape) * jnp.dtype(src.dtype).itemsize
        group = self.open_group.get(only)
        if group is None or self.groups[group][0] + size > math.prod(self.counting.shape) * 2:
            group = self.open_group[only] = len(self.groups)
            self.groups.append([0, only, device])
        self.groups[group][0] += size
        copy = self.copy(src, dst, device, group, key if recv_key is None else recv_key)
        self.when(only, copy.start)

    def arrived(self, key, dst, device, only=None):
        if isinstance(dst, int):
            dst = self.counted(dst)
        self.when(only, self.copy(dst, dst, device, 0, key).wait_recv)

    def settle(self):
        for group, (size, only, device) in enumerate(self.groups):
            block = self.counted(size)
            self.when(only, self.copy(block, block, device, group, next(iter(self.recv_ids))).wait_send)

    def when(self, only, act):
        if only is None:
            act()
        else:
            pl.when(self.conditions[only])(act)


def fused_kernel(
    q_hbm,
    k_hbm,
    v_hbm,
    q_gain_hbm,
    k_gain_hbm,
    residual_hbm,
    expert_hbm,
    weight_hbm,
    out_weight_hbm,
    gate_hbm,
    up_hbm,
    down_hbm,
    out_ref,
    q_ref,
    k_ref,
    v_ref,
    q_gain_ref,
    k_gain_ref,
    residual_ref,
    expert_ref,
    weight_ref,
    kv,
    queries,
    run_max,
    run_acc,
    attended,
    mixed,
    rows,
    out_weight,
    gate_up,
    down,
    tables,
    hid,
    hid_own,
    part_own,
    part_send,
    part_in,
    local_sem,
    send_sem,
    recv_sem,
):
    f32, bf16 = jnp.float32, jnp.bfloat16
    count, width = q_hbm.shape
    pairs = width // LANES
    halves = pairs // 2
    hidden_units = gate_hbm.shape[2]
    capacity = hid.shape[3]
    upper_tok, lower_tok = pl.ds(0, count // 2), pl.ds(count // 2, count // 2)
    shared = count // 4
    rest = count - shared
    plane_tok, line_tok = pl.ds(0, shared), pl.ds(shared, rest)
    plane_half = [pl.ds(p * (shared // 2), shared // 2) for p in range(2)]
    line_half = [pl.ds(shared + p * (rest // 2), rest // 2) for p in range(2)]
    upper_cap, lower_cap = pl.ds(0, capacity // 2), pl.ds(capacity // 2, capacity // 2)

    sp_place, tp_place = lax.axis_index("sp"), lax.axis_index("tp")
    plane, core_place = sp_place // 2, sp_place % 2
    is_mid = (plane == 1) | (plane == 2)
    is_end = (plane == 0) | (plane == 3)

    def at(sp_mask, tp_mask):
        return {"sp": flip_index(sp_place, sp_mask), "tp": flip_index(tp_place, tp_mask)}

    core, near, far = at(1, 0), at(2, 0), at(6, 0)
    across = [None, at(0, 1), at(0, 2), at(0, 3)]
    across_core = [core, at(1, 1), at(1, 2)]
    links = Links(send_sem, recv_sem, {"mid": is_mid, "end": is_end}, out_weight)

    def size_of(ref):
        return math.prod(ref.shape) * jnp.dtype(ref.dtype).itemsize


    quarters = [flip_index(tp_place, q) * width for q in range(4)]

    def columns(q):
        return pl.ds(pl.multiple_of(quarters[q], width), width)

    inputs = [
        (k_hbm, k_ref),
        (k_gain_hbm, k_gain_ref),
        (v_hbm, v_ref),
        (q_hbm, q_ref),
        (q_gain_hbm, q_gain_ref),
        (expert_hbm, expert_ref),
        (weight_hbm, weight_ref),
        (residual_hbm, residual_ref),
    ]
    inputs = [
        pltpu.make_async_copy(src, dst, local_sem.at[4 + i]) for i, (src, dst) in enumerate(inputs)
    ]
    loads = [
        pltpu.make_async_copy(out_weight_hbm, out_weight, local_sem.at[0]),
        pltpu.make_async_copy(
            gate_hbm.at[0], gate_up.at[:, pl.ds(0, hidden_units)], local_sem.at[1]
        ),
        pltpu.make_async_copy(
            up_hbm.at[0], gate_up.at[:, pl.ds(hidden_units, hidden_units)], local_sem.at[2]
        ),
        pltpu.make_async_copy(down_hbm.at[0, :, columns(0)], down.at[0, 0], local_sem.at[3]),
    ]

    for load in inputs:
        load.start()
    barrier = pltpu.get_barrier_semaphore()
    partners = [core, near, far] + across[1:] + across_core[1:]
    for partner in partners:
        pl.semaphore_signal(
            barrier, inc=1, device_id=partner, device_id_type=pl.DeviceIdType.MESH
        )

    lane = lax.broadcasted_iota(jnp.int32, (count, LANES), 1)
    first_head = lane < HEAD_DIM
    quarter = HEAD_DIM // 4
    even_quarter = (lane // quarter) % 2 == 0

    grid_rows = count // GRID_W
    token = lax.broadcasted_iota(jnp.int32, (GRID_W + 8, LANES), 0)
    lane_short = lax.broadcasted_iota(jnp.int32, (GRID_W + 8, LANES), 1)
    place = jnp.where(token < GRID_W, token, sp_place * grid_rows + token - GRID_W)
    power = (lane_short % quarter).astype(f32) * (-math.log(ROPE_BASE) / quarter)
    angle = place.astype(f32) * jnp.exp(power)
    sign = jnp.where((lane_short // quarter) % 2 == 0, -1.0, 1.0)

    def over_tokens(short):
        parts = []
        by_row = ((lane_short[:GRID_W] // quarter) % 4) < 2
        for r in range(grid_rows):
            line = short[GRID_W + r : GRID_W + r + 1, :]
            parts.append(jnp.where(by_row, line, short[:GRID_W, :]))
        return jnp.concatenate(parts, axis=0)

    cosine = over_tokens(jnp.cos(angle))
    sine = over_tokens(jnp.sin(angle) * sign)

    def pair_gain(gain_ref, pair):
        return jnp.concatenate(
            [gain_ref[2 * pair : 2 * pair + 1, :], gain_ref[2 * pair + 1 : 2 * pair + 2, :]],
            axis=1,
        )

    def norm_rotate(block, gain):
        wide = block.astype(f32)
        squares = wide * wide
        low = jnp.sum(jnp.where(first_head, squares, 0.0), axis=-1, keepdims=True)
        high = jnp.sum(jnp.where(first_head, 0.0, squares), axis=-1, keepdims=True)
        mean = jnp.where(first_head, low, high) * (1.0 / HEAD_DIM)
        scaled = wide * lax.rsqrt(mean + EPSILON) * gain
        ahead = pltpu.roll(scaled, LANES - quarter, 1)
        behind = pltpu.roll(scaled, quarter, 1)
        swapped = jnp.where(even_quarter, ahead, behind)
        return scaled * cosine + swapped * sine

    for load in inputs[:3]:
        load.wait()
    for h in range(halves):
        block = pl.ds(h * LANES, LANES)
        flipped = jnp.transpose(v_ref[:, block].astype(f32)).astype(bf16)
        for part in range(count // LANES):
            kv[h, 0, 0, 1, pl.ds(part * LANES, LANES), :] = flipped[
                :, part * LANES : (part + 1) * LANES
            ]
        kv[h, 0, 0, 0] = norm_rotate(k_ref[:, block], pair_gain(k_gain_ref, h)).astype(bf16)

    pl.semaphore_wait(barrier, len(partners))

    def line_start(name, ref_at):
        links.send(None, ref_at(0), ref_at(1), near, (*name, 1))
        links.send(None, ref_at(0), ref_at(2), far, (*name, 2), "mid")

    def line_on(name, slot, ref_at, only=None):
        if only == "end":
            return
        if slot == 1:
            links.send(None, ref_at(1), ref_at(3), far, (*name, 3), "mid")
        else:
            links.send(None, ref_at(slot), ref_at(slot), near, (*name, slot), "mid")

    def line_wait(name, slot, ref_at, only=None):
        links.arrived((*name, slot), ref_at(slot), near, only)
        line_on(name, slot, ref_at, only)

    def kv_at(h):
        return lambda slot: kv.at[h, slot, 0]

    def kv_swap(h, slot, only=None):
        links.send(("kvc", h, slot), kv.at[h, slot, 0], kv.at[h, slot, 1], core, only=only)

    def table_at(slot):
        return tables.at[slot, 0]

    def table_swap(slot, only=None):
        links.send(("kvc", halves - 1, slot), tables.at[slot, 0], tables.at[slot, 1], core, only=only)

    def take_kv(h, slot, only=None):
        last = h == halves - 1
        size = size_of(kv_at(h)(slot)) + (size_of(table_at(slot)) if last else 0)
        links.arrived(("kv", h, slot), size, near, only)
        line_on(("kv", h), slot, kv_at(h), only)
        kv_swap(h, slot, only)
        if last:
            line_on(("kv", h), slot, table_at, only)
            table_swap(slot, only)

    for h in range(halves):
        line_start(("kv", h), kv_at(h))
    for h in range(halves):
        kv_swap(h, 0)
    experts_total = tables.shape[2]
    for load in inputs[5:]:
        load.wait()
    names, factors = expert_ref[...], weight_ref[...]
    wanted = lax.broadcasted_iota(jnp.int32, (experts_total, count), 0)
    table = jnp.zeros((experts_total, count), f32)
    for k in range(TOP_K):
        table = table + jnp.where(names[k : k + 1, :] == wanted, factors[k : k + 1, :], 0.0)
    tables[0, 0] = table
    line_start(("kv", halves - 1), table_at)
    table_swap(0)
    for q in (1, 2, 3):
        links.send("down", down_hbm.at[0, :, columns(q)], down.at[0, q], across[q])
    for load in loads:
        load.start()

    for load in inputs[3:5]:
        load.wait()
    for g in range(pairs):
        turned = norm_rotate(q_ref[:, pl.ds(g * LANES, LANES)], pair_gain(q_gain_ref, g))
        turned = turned.astype(bf16).astype(f32)
        other = pltpu.roll(turned, HEAD_DIM, 1)
        if g % 2 == 0:
            top, bottom = jnp.where(first_head, turned, 0.0), jnp.where(first_head, other, 0.0)
        else:
            top, bottom = jnp.where(first_head, 0.0, other), jnp.where(first_head, 0.0, turned)
        queries[g, pl.ds(0, count), :] = top.astype(bf16)
        queries[g, pl.ds(count, count), :] = bottom.astype(bf16)

    ones = jnp.ones((16, 2 * count), bf16)
    exponent = math.log2(math.e) * HEAD_DIM ** (-0.5)

    def attend(h, slot):
        def one(i, carry):
            g = 2 * h + i
            keys = kv[h, slot, :, 0].reshape(2 * count, LANES)
            values = [
                kv[h, slot, side, 1, pl.ds(part * LANES, LANES), :]
                for side in range(2)
                for part in range(count // LANES)
            ]
            values = jnp.concatenate(values, axis=1)
            values = jnp.concatenate([values, ones], axis=0)
            scores = lax.dot_general(
                keys, queries[g], (((1,), (1,)), ((), ())), preferred_element_type=f32
            )
            block_max = jnp.max(scores, axis=0, keepdims=True)
            if slot == 0:
                new_max = block_max
            else:
                old_max = run_max[g]
                new_max = jnp.maximum(old_max, block_max)
            weights = jnp.exp2((scores - new_max) * exponent).astype(bf16)
            update = jnp.dot(values, weights, preferred_element_type=f32)
            if slot:
                rescale = jnp.exp2((old_max - new_max) * exponent)
                update = update + run_acc[g] * rescale
            run_max[g] = new_max
            run_acc[g] = update
            return carry

        if slot == SLOTS - 1 and h == halves - 1:
            for i in range(2):
                one(i, 0)
                attend_end(h, (i,))
        else:
            lax.fori_loop(0, 2, one, 0)

    def own_half(q, h):
        offset = quarters[q] + h * 2 * LANES
        return pl.ds(pl.multiple_of(offset, 2 * LANES), 2 * LANES)

    def head_columns(q, g):
        return pl.ds(pl.multiple_of(quarters[q] + g * LANES, LANES), LANES)

    def attend_end(h, heads=(0, 1)):
        for i in heads:
            g = 2 * h + i
            total = run_acc[g]
            out = total[i * HEAD_DIM : (i + 1) * HEAD_DIM] / total[LANES : LANES + 1]
            pair = jnp.concatenate([out[:, :count], out[:, count:]], axis=0)
            attended[:, head_columns(0, g)] = jnp.transpose(pair).astype(bf16)
            block = attended.at[:, head_columns(0, g)]
            for q in (1, 2):
                links.send(None, block, block, across[q], ("att", g, q))

    def attend_relay(g):
        links.arrived(("att", g, 2), attended.at[:, head_columns(2, g)], across[2])
        block = attended.at[upper_tok, head_columns(2, g)]
        links.send(None, block, block, across[1], ("att", g, 3))
        links.arrived(("att", g, 1), attended.at[:, head_columns(1, g)], across[1])
        block = attended.at[lower_tok, head_columns(1, g)]
        links.send(None, block, block, across[2], ("att", g, 3))

    def attend_chunk(h, slot):
        size = size_of(kv.at[h, slot, 1])
        if h == halves - 1:
            size += size_of(tables.at[slot, 1])
        links.arrived(("kvc", h, slot), size, core)
        attend(h, slot)

    attend_chunk(0, 0)
    take_kv(0, 1)
    take_kv(0, 2, "mid")
    attend_chunk(1, 0)
    take_kv(1, 1)
    take_kv(1, 2, "mid")
    attend_chunk(0, 1)
    attend_chunk(1, 1)
    take_kv(0, 2, "end")
    attend_chunk(0, 2)
    take_kv(0, 3, "mid")
    take_kv(1, 2, "end")
    attend_chunk(1, 2)
    loads[3].wait()
    links.arrived("down", down.at[0, pl.ds(1, 3)], core)
    links.send("downc", down.at[0], down.at[1], core)
    take_kv(1, 3, "mid")
    take_kv(0, 3, "end")
    attend_chunk(0, 3)
    attend_end(0)
    take_kv(1, 3, "end")
    attend_chunk(1, 3)

    loads[0].wait()
    mixed[...] = residual_ref[...].astype(f32)

    def project(q, h):
        mixed[...] += jnp.dot(
            attended[:, own_half(q, h)],
            out_weight[own_half(q, h), :],
            preferred_element_type=f32,
        )

    for h in range(halves):
        project(0, h)
    for g in range(pairs):
        attend_relay(g)
        if g % 2:
            project(1, g // 2)
            project(2, g // 2)
    for g in range(pairs):
        links.arrived(("att", g, 3), attended.at[:, head_columns(3, g)], across[3])
        if g % 2:
            project(3, g // 2)
    rows[0, 0, :, columns(0)] = mixed[...].astype(bf16)

    def rows_at(part):
        return lambda slot: rows.at[slot, 0, line_half[part], columns(0)]

    def wide_at(slot):
        return rows.at[slot, 0, plane_tok, :]

    def to_core(slot, q):
        links.send(
            ("rowc", slot),
            rows.at[slot, 0, line_tok, columns(q)],
            rows.at[slot, 1, line_tok, columns(q)],
            core,
        )

    def wide_to_core(slot, only=None):
        links.send(
            ("rowc", slot), wide_at(slot), rows.at[slot, 1, plane_tok, :], core, only=only
        )

    def spread_one(name, slot, span):
        block = rows.at[slot, 0, span, columns(0)]
        links.send((name, "x1", slot), block, block, across[1])
        links.send((name, "y1", slot), block, block, across[2])

    def spread_two(name, slot, span, half):
        links.arrived((name, "y1", slot), rows.at[slot, 0, span, columns(2)], across[2])
        block = rows.at[slot, 0, half[0], columns(2)]
        links.send((name, "xy", slot), block, block, across[1])
        links.arrived((name, "x1", slot), rows.at[slot, 0, span, columns(1)], across[1])
        block = rows.at[slot, 0, half[1], columns(1)]
        links.send((name, "xy", slot), block, block, across[2])

    def spread_three(name, slot, span):
        links.arrived((name, "xy", slot), rows.at[slot, 0, span, columns(3)], across[3])

    def spread(slot):
        spread_one("row", slot, line_tok)
        to_core(slot, 0)

    def spread_on(slot):
        spread_two("row", slot, line_tok, line_half)
        to_core(slot, 1)
        to_core(slot, 2)

    def spread_end(slot):
        spread_three("row", slot, line_tok)
        to_core(slot, 3)

    def take(slot, part, only=None):
        line_wait(("row", part), slot, rows_at(part), only)

    def share():
        spread_one("wide", 0, plane_tok)

    def share_on():
        spread_two("wide", 0, plane_tok, plane_half)

    def share_end():
        spread_three("wide", 0, plane_tok)
        line_start(("wide",), wide_at)
        wide_to_core(0)

    def take_wide(slot, only=None):
        line_wait(("wide",), slot, wide_at, only)
        wide_to_core(slot, only)

    before = lax.broadcasted_iota(jnp.int32, (count, count), 0) < lax.broadcasted_iota(
        jnp.int32, (count, count), 1
    )
    before = before.astype(f32).astype(bf16)

    def ranks(table):
        chosen = table > 0.0
        marks = chosen.astype(f32).astype(bf16)
        rank = jnp.dot(marks, before, preferred_element_type=f32)
        return jnp.where(chosen, rank, -1.0)

    slot_of = lax.broadcasted_iota(jnp.int32, (capacity, count), 0).astype(f32)
    slot_in = lax.broadcasted_iota(jnp.int32, (count, capacity), 1).astype(f32)
    pair_count = experts_total // SLOTS
    my_expert = plane * pair_count + core_place * 2 + tp_place // 2
    expert_row = lax.broadcasted_iota(jnp.int32, (experts_total, count), 0)

    def hidden(slot, side):
        if side:
            links.arrived(("rowc", slot), rows.at[slot, 1], core)
        block = rows[slot, side]
        wide = block.astype(f32)
        squares = jnp.mean(wide * wide, axis=-1, keepdims=True)
        norm_scale = lax.rsqrt(squares + EPSILON)
        both = jnp.dot(block, gate_up[...], preferred_element_type=f32) * norm_scale
        gate_value, up_value = both[:, :hidden_units], both[:, hidden_units:]
        result = (gate_value / (1.0 + jnp.exp(-gate_value)) * up_value).astype(bf16)
        rank = ranks(tables[slot, side])
        mine = jnp.sum(jnp.where(expert_row == my_expert, rank, 0.0), axis=0, keepdims=True)
        pick = (slot_of == mine).astype(f32).astype(bf16)
        packed = jnp.dot(pick, result, preferred_element_type=f32).astype(bf16)
        hid_own[slot, side] = packed

    def hid_send(slot, side):
        for q in (1, 2):
            links.send(
                ("h", slot, q, side),
                hid_own.at[slot, side],
                hid.at[slot, q, side],
                (across, across_core)[side][q],
            )
        if side:
            links.send(("hall", slot), hid_own.at[slot, 1], hid.at[slot, 0, 1], core)

    def hid_relay(slot, cc):
        links.arrived(("h", slot, 2, cc), hid.at[slot, 2, cc], across[2])
        links.send(
            ("hall", slot),
            hid.at[slot, 2, cc, upper_cap, :],
            hid.at[slot, 3, cc, upper_cap, :],
            across[1],
        )
        links.arrived(("h", slot, 1, cc), hid.at[slot, 1, cc], across[1])
        links.send(
            ("hall", slot),
            hid.at[slot, 1, cc, lower_cap, :],
            hid.at[slot, 3, cc, lower_cap, :],
            across[2],
        )

    def partial(slot):
        links.arrived(("hall", slot), 3 * size_of(hid.at[slot, 3, 0]), core)
        table = tables[slot, 0]
        rank_column = jnp.transpose(ranks(table))
        weight_column = jnp.transpose(table)
        column = lax.broadcasted_iota(jnp.int32, (count, experts_total), 1)
        mixed_in = jnp.zeros((count, width), f32)
        for cc in range(2):
            for qy in range(2):
                results = [
                    jnp.dot(
                        hid[slot, 2 * qy + qx, cc] if qx + qy + cc else hid_own[slot, 0],
                        down[cc, 2 * qy + qx],
                        preferred_element_type=f32,
                    ).astype(bf16)
                    for qx in range(2)
                ]
                expert = (
                    plane * pair_count
                    + flip_index(core_place, cc) * 2
                    + flip_index(tp_place // 2, qy)
                )
                this = column == expert
                rank = jnp.sum(jnp.where(this, rank_column, 0.0), axis=1, keepdims=True)
                weight = jnp.sum(jnp.where(this, weight_column, 0.0), axis=1, keepdims=True)
                place = (slot_in == rank).astype(f32).astype(bf16)
                both = jnp.dot(place, results[0], preferred_element_type=f32) + jnp.dot(
                    place, results[1], preferred_element_type=f32
                )
                mixed_in = mixed_in + both * weight
        return mixed_in

    tokens = [pl.ds(p * (count // PARTS), count // PARTS) for p in range(PARTS)]

    def send_back(slot):
        value = partial(slot)
        if slot == 0:
            mixed[...] += value
            return
        part_own[slot] = value
        part_send[slot] = value.astype(bf16)
        for p, span in enumerate(tokens):
            links.send(
                ("e", slot, p),
                part_send.at[slot, span],
                part_in.at[slot - 1, span],
                near,
                ("pe", slot, p),
                "end",
            )

    def pass_back(slot):
        for p, span in enumerate(tokens):
            if slot == 0:
                links.arrived(("pm", 1, p), part_in.at[0, span], near, "end")
                links.arrived(("pe", 1, p), part_in.at[0, span], near, "mid")
                links.arrived(("pm", 2, p), part_in.at[3, span], far, "mid")
                continue
            source = 4 if slot == 1 else slot - 1
            if slot == 1:
                links.arrived(("pm", 3, p), part_in.at[source, span], far, "mid")
            else:
                links.arrived(("pe", slot, p), part_in.at[source, span], near, "mid")

            @pl.when(is_mid)
            def _():
                total = part_own[slot, span] + part_in[source, span].astype(f32)
                part_send[slot, span] = total.astype(bf16)

            block = part_send.at[slot, span]
            if slot == 1:
                links.send(("m", 1, p), block, part_in.at[0, span], near, ("pm", 1, p), "mid")
            else:
                target = part_in.at[1 + slot, span]
                links.send(("m", slot, p), block, target, far, ("pm", slot, p), "mid")
        if slot == 0:
            total = mixed[...] + part_in[0].astype(f32)
            out_ref[...] = total.astype(bf16)

            @pl.when(is_mid)
            def _():
                out_ref[...] = (total + part_in[3].astype(f32)).astype(bf16)

    def start_rows():
        for part in range(2):
            line_start(("row", part), rows_at(part))

    steps = {
        "start": start_rows,
        "z": take,
        "p1": share,
        "p2": share_on,
        "pz": share_end,
        "zp": take_wide,
        "x1": spread,
        "x2": spread_on,
        "c3": spread_end,
        "hid": hidden,
        "hs": hid_send,
        "hr": hid_relay,
        "part": send_back,
        "red": pass_back,
    }
    loads[1].wait()
    loads[2].wait()
    links.arrived("downc", down.at[1], core)
    for step, *where in ORDER:
        steps[step](*where)
    links.settle()


def local_fused(
    query_proj,
    key_proj,
    value_proj,
    query_gain,
    key_gain,
    residual,
    out_weight,
    route_expert,
    route_weight,
    expert_gate,
    expert_up,
    expert_down,
):
    token_count, width = query_proj.shape
    local_kv = key_gain.shape[0]
    total = out_weight.shape[0]
    hidden_units = expert_gate.shape[2]
    experts_total = lax.axis_size("sp") * lax.axis_size("tp") // 2
    capacity = 3 * token_count * TOP_K // (2 * experts_total)
    f32, bf16 = jnp.float32, jnp.bfloat16

    vmem = pl.BlockSpec(memory_space=pltpu.VMEM)
    hbm = pl.BlockSpec(memory_space=pl.ANY)
    halves = local_kv // 2
    inputs = (
        query_proj,
        key_proj,
        value_proj,
        query_gain,
        key_gain,
        residual,
        route_expert.T,
        route_weight.T,
    )
    scratch = [pltpu.VMEM(value.shape, value.dtype) for value in inputs]
    scratch += [
        pltpu.VMEM((halves, SLOTS, 2, 2, token_count, LANES), bf16),
        pltpu.VMEM((local_kv, 2 * token_count, LANES), bf16),
        pltpu.VMEM((local_kv, 1, 2 * token_count), f32),
        pltpu.VMEM((local_kv, LANES + 16, 2 * token_count), f32),
        pltpu.VMEM((token_count, total), bf16),
        pltpu.VMEM((token_count, width), f32),
        pltpu.VMEM((SLOTS, 2, token_count, total), bf16),
        pltpu.VMEM((total, width), bf16),
        pltpu.VMEM((total, 2 * hidden_units), bf16),
        pltpu.VMEM((2, 4, hidden_units, width), bf16),
        pltpu.VMEM((SLOTS, 2, experts_total, token_count), f32),
        pltpu.VMEM((SLOTS, 4, 2, capacity, hidden_units), bf16),
        pltpu.VMEM((SLOTS, 2, capacity, hidden_units), bf16),
        pltpu.VMEM((SLOTS, token_count, width), f32),
        pltpu.VMEM((SLOTS, token_count, width), bf16),
        pltpu.VMEM((5, token_count, width), bf16),
        pltpu.SemaphoreType.DMA((12,)),
        pltpu.SemaphoreType.DMA((SEND_SEMS,)),
        pltpu.SemaphoreType.DMA((RECV_SEMS,)),
    ]
    result = pl.pallas_call(
        fused_kernel,
        out_shape=jax.ShapeDtypeStruct((token_count, width), bf16),
        in_specs=[hbm] * 12,
        out_specs=vmem,
        scratch_shapes=scratch,
        compiler_params=pltpu.CompilerParams(
            collective_id=0, has_side_effects=True, vmem_limit_bytes=56 * 1024 * 1024
        ),
    )(*inputs, out_weight, expert_gate, expert_up, expert_down)
    return result


def takes_fused(mesh):
    chips = mesh.shape["sp"] // 2
    experts_total = mesh.shape["sp"] * mesh.shape["tp"] // 2
    return mesh.shape["tp"] == 4 and chips == SLOTS and experts_total == 2 * TOP_K


def solution(mesh):
    in_specs = (
        P("sp", "tp"),
        P("sp", "tp"),
        P("sp", "tp"),
        P("tp", None),
        P("tp", None),
        P("sp", "tp"),
        P(None, "tp"),
        P("sp", None),
        P("sp", None),
        P(("sp", "tp"), None, None),
        P(("sp", "tp"), None, None),
        P(("sp", "tp"), None, None),
    )
    out_specs = P("sp", "tp")
    body = local_fused if takes_fused(mesh) else local
    return jax.shard_map(body, mesh=mesh, in_specs=in_specs, out_specs=out_specs, check_vma=False)
```

```python
import functools
import math

import jax
import jax.numpy as jnp
from jax import lax
from jax.experimental import pallas as pl
from jax.experimental.pallas import tpu as pltpu
from jax.sharding import PartitionSpec as P

HEAD_DIM = 64
TOP_K = 8
GRID_W = 64


EPSILON = 1e-06
ROPE_BASE = 10000.0
KEY_BLOCK = 1024


def rotation_tables(offset, count):
    pair_count = HEAD_DIM // 4
    position = offset + jnp.arange(count, dtype=jnp.int32)
    grid_row = (position // GRID_W).astype(jnp.float32)
    grid_col = (position % GRID_W).astype(jnp.float32)
    inverse = ROPE_BASE ** (-jnp.arange(pair_count, dtype=jnp.float32) / pair_count)
    angles = jnp.stack([grid_row[:, None] * inverse, grid_col[:, None] * inverse], axis=1)
    return (jnp.cos(angles), jnp.sin(angles))


def rotate(vectors, cosine_table, sine_table):
    pair_count = HEAD_DIM // 4
    shaped = vectors.reshape(vectors.shape[:-1] + (2, 2, pair_count))
    first_half = shaped[..., 0, :]
    second_half = shaped[..., 1, :]
    cosine_row = cosine_table[:, None]
    sine_row = sine_table[:, None]
    turned = jnp.stack(
        [
            first_half * cosine_row - second_half * sine_row,
            first_half * sine_row + second_half * cosine_row,
        ],
        axis=-2,
    )
    return turned.reshape(vectors.shape)


def head_norm(vectors, gain):
    scaled = vectors.astype(jnp.float32)
    scaled = scaled * lax.rsqrt(jnp.mean(scaled * scaled, axis=-1, keepdims=True) + EPSILON)
    return scaled * gain


def online_update(running, query_groups, key_block, value_block):
    running_max, running_sum, running_acc = running
    scores = jnp.einsum(
        "tkgd,nkd->kgtn", query_groups, key_block, preferred_element_type=jnp.float32
    ) * HEAD_DIM ** (-0.5)
    new_max = jnp.maximum(running_max, jnp.max(scores, axis=-1))
    rescale = jnp.exp(running_max - new_max)
    weights = jnp.exp(scores - new_max[..., None]).astype(jnp.bfloat16)
    new_sum = running_sum * rescale + jnp.sum(weights.astype(jnp.float32), axis=-1)
    update = jnp.einsum("kgtn,nkd->kgtd", weights, value_block, preferred_element_type=jnp.float32)
    return (new_max, new_sum, running_acc * rescale[..., None] + update)


def local(
    query_proj,
    key_proj,
    value_proj,
    query_gain,
    key_gain,
    residual,
    out_weight,
    route_expert,
    route_weight,
    expert_gate,
    expert_up,
    expert_down,
):
    token_count = query_proj.shape[0]
    local_heads = query_gain.shape[0]
    local_kv = key_gain.shape[0]
    group_size = local_heads // local_kv
    sp_size = lax.axis_size("sp")
    tp_size = lax.axis_size("tp")
    tp_place = lax.axis_index("tp")
    offset = lax.axis_index("sp") * token_count
    cosine_table, sine_table = rotation_tables(offset, token_count)
    query_rot = rotate(
        head_norm(query_proj.reshape(token_count, local_heads, HEAD_DIM), query_gain),
        cosine_table,
        sine_table,
    ).astype(jnp.bfloat16)
    key_rot = rotate(
        head_norm(key_proj.reshape(token_count, local_kv, HEAD_DIM), key_gain),
        cosine_table,
        sine_table,
    ).astype(jnp.bfloat16)
    packed = jnp.concatenate(
        [key_rot.reshape(token_count, local_kv * HEAD_DIM), value_proj], axis=1
    )
    query_groups = query_rot.reshape(token_count, local_kv, group_size, HEAD_DIM)
    initial = (
        jnp.full((local_kv, group_size, token_count), -1e30, jnp.float32),
        jnp.zeros((local_kv, group_size, token_count), jnp.float32),
        jnp.zeros((local_kv, group_size, token_count, HEAD_DIM), jnp.float32),
    )
    incoming = lax.all_gather(packed, "sp", axis=0, tiled=True)
    incoming_len = incoming.shape[0]
    step_len = math.gcd(incoming_len, KEY_BLOCK)

    def one_step(step_index, running):
        block_rows = lax.dynamic_slice_in_dim(incoming, step_index * step_len, step_len, 0)
        key_block = block_rows[:, : local_kv * HEAD_DIM].reshape(step_len, local_kv, HEAD_DIM)
        value_block = block_rows[:, local_kv * HEAD_DIM :].reshape(step_len, local_kv, HEAD_DIM)
        return online_update(running, query_groups, key_block, value_block)

    final_max, final_sum, final_acc = lax.fori_loop(0, incoming_len // step_len, one_step, initial)
    attended = final_acc / final_sum[..., None]
    attended = jnp.transpose(attended, (2, 0, 1, 3)).reshape(token_count, local_heads * HEAD_DIM)
    attended = attended.astype(jnp.bfloat16)
    projected = jnp.dot(
        lax.all_gather(attended, "tp", axis=1, tiled=True),
        out_weight,
        preferred_element_type=jnp.float32,
    )
    mixed_sum = residual.astype(jnp.float32) + projected
    mixed_rows = mixed_sum.astype(jnp.bfloat16)
    full_rows = lax.all_gather(mixed_rows, "tp", axis=1, tiled=True)
    width_total = full_rows.shape[1]
    per_sp = tp_size // 2
    column = tp_place // 2
    experts_total = per_sp * sp_size
    capacity = 3 * token_count * TOP_K // (2 * experts_total)
    slot_count = sp_size * capacity
    flat_choice = route_expert.reshape(token_count * TOP_K)
    onehot = (flat_choice[:, None] == jnp.arange(experts_total, dtype=jnp.int32)[None, :]).astype(
        jnp.int32
    )
    earlier = jnp.cumsum(onehot, axis=0) - onehot
    slot_rank = jnp.sum(earlier * onehot, axis=1)
    mine = flat_choice % per_sp == column
    target = flat_choice // per_sp * capacity + slot_rank
    owner = jnp.arange(token_count * TOP_K, dtype=jnp.int32) // TOP_K
    slot_token = (
        jnp.full((slot_count + 1,), token_count, jnp.int32)
        .at[jnp.where(mine, target, slot_count)]
        .set(owner)[:slot_count]
    )
    padded = jnp.concatenate([full_rows, jnp.zeros((1, width_total), jnp.bfloat16)], axis=0)
    selected = padded[slot_token].reshape(sp_size, capacity, width_total)
    arrived = lax.all_to_all(selected, "sp", split_axis=0, concat_axis=0, tiled=True)
    expert_rows = arrived.reshape(slot_count, width_total)
    squares = jnp.mean(jnp.square(expert_rows.astype(jnp.float32)), axis=-1, keepdims=True)
    norm_scale = lax.rsqrt(squares + EPSILON)
    gate_value = (
        jnp.dot(expert_rows, expert_gate[0], preferred_element_type=jnp.float32) * norm_scale
    )
    up_value = jnp.dot(expert_rows, expert_up[0], preferred_element_type=jnp.float32) * norm_scale
    hidden = (jax.nn.silu(gate_value) * up_value).astype(jnp.bfloat16)
    half_result = jnp.dot(hidden, expert_down[0], preferred_element_type=jnp.float32).astype(
        jnp.bfloat16
    )
    returned = lax.all_to_all(
        half_result.reshape(sp_size, capacity, width_total),
        "sp",
        split_axis=0,
        concat_axis=0,
        tiled=True,
    )
    slot_results = returned.reshape(slot_count, width_total)
    mine_grid = mine.reshape(token_count, TOP_K)
    target_grid = target.reshape(token_count, TOP_K)
    gathered_sum = jnp.zeros((token_count, width_total), jnp.float32)
    for choice_index in range(TOP_K):
        chosen = mine_grid[:, choice_index]
        index = jnp.where(chosen, target_grid[:, choice_index], 0)
        factor = jnp.where(chosen, route_weight[:, choice_index], 0.0)
        picked = slot_results[index].astype(jnp.float32)
        gathered_sum = gathered_sum + factor[:, None] * picked
    routed = lax.psum_scatter(
        gathered_sum.astype(jnp.bfloat16), "tp", scatter_dimension=1, tiled=True
    ).astype(jnp.float32)
    return (mixed_sum + routed).astype(jnp.bfloat16)


def flip_index(index, mask):
    bit = 1
    while bit <= mask:
        if mask & bit:
            index = index + bit - 2 * bit * ((index // bit) % 2)
        bit *= 2
    return index


LANES = 128
SLOTS = 4
SEND_SEMS = 11
RECV_SEMS = 104
PARTS = 4
ORDER = (
    ("start",),
    ("p1",),
    ("x1", 0),
    ("z", 2, 0, "mid"),
    ("p2",),
    ("z", 1, 0, None),
    ("z", 1, 1, None),
    ("z", 2, 1, "mid"),
    ("x1", 1),
    ("z", 3, 0, "mid"),
    ("z", 3, 1, "mid"),
    ("pz",),
    ("z", 2, 0, "end"),
    ("z", 2, 1, "end"),
    ("x1", 2),
    ("z", 3, 0, "end"),
    ("x2", 0),
    ("z", 3, 1, "end"),
    ("x1", 3),
    ("zp", 1, None),
    ("x2", 2),
    ("x2", 1),
    ("zp", 2, "mid"),
    ("x2", 3),
    ("zp", 3, "mid"),
    ("c3", 2),
    ("zp", 2, "end"),
    ("c3", 0),
    ("hid", 2, 0),
    ("hs", 2, 0),
    ("hid", 2, 1),
    ("hs", 2, 1),
    ("c3", 1),
    ("zp", 3, "end"),
    ("c3", 3),
    ("hid", 3, 0),
    ("hs", 3, 0),
    ("hid", 3, 1),
    ("hs", 3, 1),
    ("hr", 3, 0),
    ("hid", 0, 1),
    ("hr", 3, 1),
    ("hr", 2, 1),
    ("hr", 2, 0),
    ("hid", 1, 1),
    ("hid", 1, 0),
    ("hs", 1, 0),
    ("hs", 1, 1),
    ("part", 3),
    ("hs", 0, 1),
    ("hid", 0, 0),
    ("part", 2),
    ("hr", 1, 0),
    ("hr", 1, 1),
    ("hs", 0, 0),
    ("red", 3),
    ("part", 1),
    ("red", 1),
    ("hr", 0, 1),
    ("hr", 0, 0),
    ("red", 2),
    ("part", 0),
    ("red", 0),
)


class Links:
    def __init__(self, send_sem, recv_sem, conditions, counting):
        self.send_sem, self.recv_sem = send_sem, recv_sem
        self.conditions, self.counting = conditions, counting
        self.recv_ids = {}
        self.groups, self.open_group = [], {}

    def copy(self, src, dst, device, send_id, recv_key):
        recv_id = self.recv_ids.setdefault(recv_key, len(self.recv_ids))
        assert recv_id < RECV_SEMS and send_id < SEND_SEMS
        return pltpu.make_async_remote_copy(
            src_ref=src,
            dst_ref=dst,
            send_sem=self.send_sem.at[send_id],
            recv_sem=self.recv_sem.at[recv_id],
            device_id=device,
            device_id_type=pl.DeviceIdType.MESH,
        )

    def counted(self, size):
        lines, width = self.counting.shape
        line = width * 2
        assert size % line == 0 and size // line <= lines
        return self.counting.at[pl.ds(0, size // line), :]

    def send(self, key, src, dst, device, recv_key=None, only=None):
        size = math.prod(src.shape) * jnp.dtype(src.dtype).itemsize
        group = self.open_group.get(only)
        if group is None or self.groups[group][0] + size > math.prod(self.counting.shape) * 2:
            group = self.open_group[only] = len(self.groups)
            self.groups.append([0, only, device])
        self.groups[group][0] += size
        copy = self.copy(src, dst, device, group, key if recv_key is None else recv_key)
        self.when(only, copy.start)

    def arrived(self, key, dst, device, only=None):
        if isinstance(dst, int):
            dst = self.counted(dst)
        self.when(only, self.copy(dst, dst, device, 0, key).wait_recv)

    def settle(self):
        for group, (size, only, device) in enumerate(self.groups):
            block = self.counted(size)
            self.when(only, self.copy(block, block, device, group, next(iter(self.recv_ids))).wait_send)

    def when(self, only, act):
        if only is None:
            act()
        else:
            pl.when(self.conditions[only])(act)


def fused_kernel(
    q_hbm,
    k_hbm,
    v_hbm,
    q_gain_hbm,
    k_gain_hbm,
    residual_hbm,
    expert_hbm,
    weight_hbm,
    out_weight_hbm,
    gate_hbm,
    up_hbm,
    down_hbm,
    out_ref,
    q_ref,
    k_ref,
    v_ref,
    q_gain_ref,
    k_gain_ref,
    residual_ref,
    expert_ref,
    weight_ref,
    kv,
    queries,
    run_max,
    run_acc,
    attended,
    mixed,
    rows,
    out_weight,
    gate_up,
    down,
    tables,
    hid,
    hid_own,
    part_own,
    part_send,
    part_in,
    local_sem,
    send_sem,
    recv_sem,
):
    f32, bf16 = jnp.float32, jnp.bfloat16
    count, width = q_hbm.shape
    pairs = width // LANES
    halves = pairs // 2
    hidden_units = gate_hbm.shape[2]
    capacity = hid.shape[3]
    upper_tok, lower_tok = pl.ds(0, count // 2), pl.ds(count // 2, count // 2)
    shared = count // 4
    rest = count - shared
    plane_tok, line_tok = pl.ds(0, shared), pl.ds(shared, rest)
    plane_half = [pl.ds(p * (shared // 2), shared // 2) for p in range(2)]
    line_half = [pl.ds(shared + p * (rest // 2), rest // 2) for p in range(2)]
    upper_cap, lower_cap = pl.ds(0, capacity // 2), pl.ds(capacity // 2, capacity // 2)

    sp_place, tp_place = lax.axis_index("sp"), lax.axis_index("tp")
    plane, core_place = sp_place // 2, sp_place % 2
    is_mid = (plane == 1) | (plane == 2)
    is_end = (plane == 0) | (plane == 3)

    def at(sp_mask, tp_mask):
        return {"sp": flip_index(sp_place, sp_mask), "tp": flip_index(tp_place, tp_mask)}

    core, near, far = at(1, 0), at(2, 0), at(6, 0)
    across = [None, at(0, 1), at(0, 2), at(0, 3)]
    across_core = [core, at(1, 1), at(1, 2)]
    links = Links(send_sem, recv_sem, {"mid": is_mid, "end": is_end}, out_weight)

    def size_of(ref):
        return math.prod(ref.shape) * jnp.dtype(ref.dtype).itemsize


    quarters = [flip_index(tp_place, q) * width for q in range(4)]

    def columns(q):
        return pl.ds(pl.multiple_of(quarters[q], width), width)

    inputs = [
        (k_hbm, k_ref),
        (k_gain_hbm, k_gain_ref),
        (v_hbm, v_ref),
        (q_hbm, q_ref),
        (q_gain_hbm, q_gain_ref),
        (expert_hbm, expert_ref),
        (weight_hbm, weight_ref),
        (residual_hbm, residual_ref),
    ]
    inputs = [
        pltpu.make_async_copy(src, dst, local_sem.at[4 + i]) for i, (src, dst) in enumerate(inputs)
    ]
    loads = [
        pltpu.make_async_copy(out_weight_hbm, out_weight, local_sem.at[0]),
        pltpu.make_async_copy(
            gate_hbm.at[0], gate_up.at[:, pl.ds(0, hidden_units)], local_sem.at[1]
        ),
        pltpu.make_async_copy(
            up_hbm.at[0], gate_up.at[:, pl.ds(hidden_units, hidden_units)], local_sem.at[2]
        ),
        pltpu.make_async_copy(down_hbm.at[0, :, columns(0)], down.at[0, 0], local_sem.at[3]),
    ]

    for load in inputs:
        load.start()
    barrier = pltpu.get_barrier_semaphore()
    partners = [core, near, far] + across[1:] + across_core[1:]
    for partner in partners:
        pl.semaphore_signal(
            barrier, inc=1, device_id=partner, device_id_type=pl.DeviceIdType.MESH
        )

    lane = lax.broadcasted_iota(jnp.int32, (count, LANES), 1)
    first_head = lane < HEAD_DIM
    quarter = HEAD_DIM // 4
    even_quarter = (lane // quarter) % 2 == 0

    grid_rows = count // GRID_W
    token = lax.broadcasted_iota(jnp.int32, (GRID_W + 8, LANES), 0)
    lane_short = lax.broadcasted_iota(jnp.int32, (GRID_W + 8, LANES), 1)
    place = jnp.where(token < GRID_W, token, sp_place * grid_rows + token - GRID_W)
    power = (lane_short % quarter).astype(f32) * (-math.log(ROPE_BASE) / quarter)
    angle = place.astype(f32) * jnp.exp(power)
    sign = jnp.where((lane_short // quarter) % 2 == 0, -1.0, 1.0)

    def over_tokens(short):
        parts = []
        by_row = ((lane_short[:GRID_W] // quarter) % 4) < 2
        for r in range(grid_rows):
            line = short[GRID_W + r : GRID_W + r + 1, :]
            parts.append(jnp.where(by_row, line, short[:GRID_W, :]))
        return jnp.concatenate(parts, axis=0)

    cosine = over_tokens(jnp.cos(angle))
    sine = over_tokens(jnp.sin(angle) * sign)

    def pair_gain(gain_ref, pair):
        return jnp.concatenate(
            [gain_ref[2 * pair : 2 * pair + 1, :], gain_ref[2 * pair + 1 : 2 * pair + 2, :]],
            axis=1,
        )

    def norm_rotate(block, gain):
        wide = block.astype(f32)
        squares = wide * wide
        low = jnp.sum(jnp.where(first_head, squares, 0.0), axis=-1, keepdims=True)
        high = jnp.sum(jnp.where(first_head, 0.0, squares), axis=-1, keepdims=True)
        mean = jnp.where(first_head, low, high) * (1.0 / HEAD_DIM)
        scaled = wide * lax.rsqrt(mean + EPSILON) * gain
        ahead = pltpu.roll(scaled, LANES - quarter, 1)
        behind = pltpu.roll(scaled, quarter, 1)
        swapped = jnp.where(even_quarter, ahead, behind)
        return scaled * cosine + swapped * sine

    for load in inputs[:3]:
        load.wait()
    for h in range(halves):
        block = pl.ds(h * LANES, LANES)
        flipped = jnp.transpose(v_ref[:, block].astype(f32)).astype(bf16)
        for part in range(count // LANES):
            kv[h, 0, 0, 1, pl.ds(part * LANES, LANES), :] = flipped[
                :, part * LANES : (part + 1) * LANES
            ]
        kv[h, 0, 0, 0] = norm_rotate(k_ref[:, block], pair_gain(k_gain_ref, h)).astype(bf16)

    pl.semaphore_wait(barrier, len(partners))

    def line_start(name, ref_at):
        links.send(None, ref_at(0), ref_at(1), near, (*name, 1))
        links.send(None, ref_at(0), ref_at(2), far, (*name, 2), "mid")

    def line_on(name, slot, ref_at, only=None):
        if only == "end":
            return
        if slot == 1:
            links.send(None, ref_at(1), ref_at(3), far, (*name, 3), "mid")
        else:
            links.send(None, ref_at(slot), ref_at(slot), near, (*name, slot), "mid")

    def line_wait(name, slot, ref_at, only=None):
        links.arrived((*name, slot), ref_at(slot), near, only)
        line_on(name, slot, ref_at, only)

    def kv_at(h):
        return lambda slot: kv.at[h, slot, 0]

    def kv_swap(h, slot, only=None):
        links.send(("kvc", h, slot), kv.at[h, slot, 0], kv.at[h, slot, 1], core, only=only)

    def table_at(slot):
        return tables.at[slot, 0]

    def table_swap(slot, only=None):
        links.send(("kvc", halves - 1, slot), tables.at[slot, 0], tables.at[slot, 1], core, only=only)

    def take_kv(h, slot, only=None):
        last = h == halves - 1
        size = size_of(kv_at(h)(slot)) + (size_of(table_at(slot)) if last else 0)
        links.arrived(("kv", h, slot), size, near, only)
        line_on(("kv", h), slot, kv_at(h), only)
        kv_swap(h, slot, only)
        if last:
            line_on(("kv", h), slot, table_at, only)
            table_swap(slot, only)

    for h in range(halves):
        line_start(("kv", h), kv_at(h))
    for h in range(halves):
        kv_swap(h, 0)
    experts_total = tables.shape[2]
    for load in inputs[5:]:
        load.wait()
    names, factors = expert_ref[...], weight_ref[...]
    wanted = lax.broadcasted_iota(jnp.int32, (experts_total, count), 0)
    table = jnp.zeros((experts_total, count), f32)
    for k in range(TOP_K):
        table = table + jnp.where(names[k : k + 1, :] == wanted, factors[k : k + 1, :], 0.0)
    tables[0, 0] = table
    line_start(("kv", halves - 1), table_at)
    table_swap(0)
    for q in (1, 2, 3):
        links.send("down", down_hbm.at[0, :, columns(q)], down.at[0, q], across[q])
    for load in loads:
        load.start()

    for load in inputs[3:5]:
        load.wait()
    for g in range(pairs):
        turned = norm_rotate(q_ref[:, pl.ds(g * LANES, LANES)], pair_gain(q_gain_ref, g))
        turned = turned.astype(bf16).astype(f32)
        other = pltpu.roll(turned, HEAD_DIM, 1)
        if g % 2 == 0:
            top, bottom = jnp.where(first_head, turned, 0.0), jnp.where(first_head, other, 0.0)
        else:
            top, bottom = jnp.where(first_head, 0.0, other), jnp.where(first_head, 0.0, turned)
        queries[g, pl.ds(0, count), :] = top.astype(bf16)
        queries[g, pl.ds(count, count), :] = bottom.astype(bf16)

    ones = jnp.ones((16, 2 * count), bf16)
    exponent = math.log2(math.e) * HEAD_DIM ** (-0.5)

    def attend(h, slot, sides=(0, 1)):
        held = len(sides) * count

        def one(i, carry):
            g = 2 * h + i
            keys = jnp.concatenate([kv[h, slot, side, 0] for side in sides], axis=0)
            values = [
                kv[h, slot, side, 1, pl.ds(part * LANES, LANES), :]
                for side in sides
                for part in range(count // LANES)
            ]
            values = jnp.concatenate(values, axis=1)
            values = jnp.concatenate([values, ones[:, :held]], axis=0)
            scores = lax.dot_general(
                keys, queries[g], (((1,), (1,)), ((), ())), preferred_element_type=f32
            )
            block_max = jnp.max(scores, axis=0, keepdims=True)
            if slot == 0:
                new_max = block_max
            else:
                old_max = run_max[g]
                new_max = jnp.maximum(old_max, block_max)
            weights = jnp.exp2((scores - new_max) * exponent).astype(bf16)
            update = jnp.dot(values, weights, preferred_element_type=f32)
            if slot:
                rescale = jnp.exp2((old_max - new_max) * exponent)
                update = update + run_acc[g] * rescale
            run_max[g] = new_max
            run_acc[g] = update
            return carry

        if slot == SLOTS - 1 and h == halves - 1 and 1 in sides:
            for i in range(2):
                one(i, 0)
                attend_end(h, (i,))
        else:
            lax.fori_loop(0, 2, one, 0)

    def own_half(q, h):
        offset = quarters[q] + h * 2 * LANES
        return pl.ds(pl.multiple_of(offset, 2 * LANES), 2 * LANES)

    def head_columns(q, g):
        return pl.ds(pl.multiple_of(quarters[q] + g * LANES, LANES), LANES)

    def attend_end(h, heads=(0, 1)):
        for i in heads:
            g = 2 * h + i
            total = run_acc[g]
            out = total[i * HEAD_DIM : (i + 1) * HEAD_DIM] / total[LANES : LANES + 1]
            pair = jnp.concatenate([out[:, :count], out[:, count:]], axis=0)
            attended[:, head_columns(0, g)] = jnp.transpose(pair).astype(bf16)
            block = attended.at[:, head_columns(0, g)]
            for q in (1, 2):
                links.send(None, block, block, across[q], ("att", g, q))

    def attend_relay(g):
        links.arrived(("att", g, 2), attended.at[:, head_columns(2, g)], across[2])
        block = attended.at[upper_tok, head_columns(2, g)]
        links.send(None, block, block, across[1], ("att", g, 3))
        links.arrived(("att", g, 1), attended.at[:, head_columns(1, g)], across[1])
        block = attended.at[lower_tok, head_columns(1, g)]
        links.send(None, block, block, across[2], ("att", g, 3))

    def attend_chunk(h, slot):
        size = size_of(kv.at[h, slot, 1])
        if h == halves - 1:
            size += size_of(tables.at[slot, 1])
        if slot < SLOTS - 1:
            links.arrived(("kvc", h, slot), size, core)
            attend(h, slot)
            return
        attend(h, slot, (0,))
        links.arrived(("kvc", h, slot), size, core)
        attend(h, slot, (1,))

    attend_chunk(0, 0)
    take_kv(0, 1)
    take_kv(0, 2, "mid")
    attend_chunk(1, 0)
    take_kv(1, 1)
    take_kv(1, 2, "mid")
    attend_chunk(0, 1)
    attend_chunk(1, 1)
    take_kv(0, 2, "end")
    attend_chunk(0, 2)
    take_kv(0, 3, "mid")
    take_kv(1, 2, "end")
    attend_chunk(1, 2)
    loads[3].wait()
    links.arrived("down", down.at[0, pl.ds(1, 3)], core)
    links.send("downc", down.at[0], down.at[1], core)
    take_kv(1, 3, "mid")
    take_kv(0, 3, "end")
    attend_chunk(0, 3)
    attend_end(0)
    take_kv(1, 3, "end")
    attend_chunk(1, 3)

    loads[0].wait()
    mixed[...] = residual_ref[...].astype(f32)

    def project(q, h):
        mixed[...] += jnp.dot(
            attended[:, own_half(q, h)],
            out_weight[own_half(q, h), :],
            preferred_element_type=f32,
        )

    for h in range(halves):
        project(0, h)
    for g in range(pairs):
        attend_relay(g)
        if g % 2:
            project(1, g // 2)
            project(2, g // 2)
    for g in range(pairs):
        links.arrived(("att", g, 3), attended.at[:, head_columns(3, g)], across[3])
        if g % 2:
            project(3, g // 2)
    rows[0, 0, :, columns(0)] = mixed[...].astype(bf16)

    def rows_at(part):
        return lambda slot: rows.at[slot, 0, line_half[part], columns(0)]

    def wide_at(slot):
        return rows.at[slot, 0, plane_tok, :]

    def to_core(slot, q):
        links.send(
            ("rowc", slot),
            rows.at[slot, 0, line_tok, columns(q)],
            rows.at[slot, 1, line_tok, columns(q)],
            core,
        )

    def wide_to_core(slot, only=None):
        links.send(
            ("rowc", slot), wide_at(slot), rows.at[slot, 1, plane_tok, :], core, only=only
        )

    def spread_one(name, slot, span):
        block = rows.at[slot, 0, span, columns(0)]
        links.send((name, "x1", slot), block, block, across[1])
        links.send((name, "y1", slot), block, block, across[2])

    def spread_two(name, slot, span, half):
        links.arrived((name, "y1", slot), rows.at[slot, 0, span, columns(2)], across[2])
        block = rows.at[slot, 0, half[0], columns(2)]
        links.send((name, "xy", slot), block, block, across[1])
        links.arrived((name, "x1", slot), rows.at[slot, 0, span, columns(1)], across[1])
        block = rows.at[slot, 0, half[1], columns(1)]
        links.send((name, "xy", slot), block, block, across[2])

    def spread_three(name, slot, span):
        links.arrived((name, "xy", slot), rows.at[slot, 0, span, columns(3)], across[3])

    def spread(slot):
        spread_one("row", slot, line_tok)
        to_core(slot, 0)

    def spread_on(slot):
        spread_two("row", slot, line_tok, line_half)
        to_core(slot, 1)
        to_core(slot, 2)

    def spread_end(slot):
        spread_three("row", slot, line_tok)
        to_core(slot, 3)

    def take(slot, part, only=None):
        line_wait(("row", part), slot, rows_at(part), only)

    def share():
        spread_one("wide", 0, plane_tok)

    def share_on():
        spread_two("wide", 0, plane_tok, plane_half)

    def share_end():
        spread_three("wide", 0, plane_tok)
        line_start(("wide",), wide_at)
        wide_to_core(0)

    def take_wide(slot, only=None):
        line_wait(("wide",), slot, wide_at, only)
        wide_to_core(slot, only)

    before = lax.broadcasted_iota(jnp.int32, (count, count), 0) < lax.broadcasted_iota(
        jnp.int32, (count, count), 1
    )
    before = before.astype(f32).astype(bf16)

    def ranks(table):
        chosen = table > 0.0
        marks = chosen.astype(f32).astype(bf16)
        rank = jnp.dot(marks, before, preferred_element_type=f32)
        return jnp.where(chosen, rank, -1.0)

    slot_of = lax.broadcasted_iota(jnp.int32, (capacity, count), 0).astype(f32)
    slot_in = lax.broadcasted_iota(jnp.int32, (count, capacity), 1).astype(f32)
    pair_count = experts_total // SLOTS
    my_expert = plane * pair_count + core_place * 2 + tp_place // 2
    expert_row = lax.broadcasted_iota(jnp.int32, (experts_total, count), 0)

    def hidden(slot, side):
        if side:
            links.arrived(("rowc", slot), rows.at[slot, 1], core)
        block = rows[slot, side]
        wide = block.astype(f32)
        squares = jnp.mean(wide * wide, axis=-1, keepdims=True)
        norm_scale = lax.rsqrt(squares + EPSILON)
        both = jnp.dot(block, gate_up[...], preferred_element_type=f32) * norm_scale
        gate_value, up_value = both[:, :hidden_units], both[:, hidden_units:]
        result = (gate_value / (1.0 + jnp.exp(-gate_value)) * up_value).astype(bf16)
        rank = ranks(tables[slot, side])
        mine = jnp.sum(jnp.where(expert_row == my_expert, rank, 0.0), axis=0, keepdims=True)
        pick = (slot_of == mine).astype(f32).astype(bf16)
        packed = jnp.dot(pick, result, preferred_element_type=f32).astype(bf16)
        hid_own[slot, side] = packed

    def hid_send(slot, side):
        for q in (1, 2):
            links.send(
                ("h", slot, q, side),
                hid_own.at[slot, side],
                hid.at[slot, q, side],
                (across, across_core)[side][q],
            )
        if side:
            links.send(None, hid_own.at[slot, 1], hid.at[slot, 0, 1], core, ("hall", slot, 1))

    def hid_relay(slot, cc):
        links.arrived(("h", slot, 2, cc), hid.at[slot, 2, cc], across[2])
        links.send(
            ("hall", slot, cc),
            hid.at[slot, 2, cc, upper_cap, :],
            hid.at[slot, 3, cc, upper_cap, :],
            across[1],
        )
        links.arrived(("h", slot, 1, cc), hid.at[slot, 1, cc], across[1])
        links.send(
            ("hall", slot, cc),
            hid.at[slot, 1, cc, lower_cap, :],
            hid.at[slot, 3, cc, lower_cap, :],
            across[2],
        )

    relays = {slot: [] for slot in range(SLOTS)}
    for step, *where in ORDER:
        if step == "hr":
            relays[where[0]].append(where[1])

    def partial(slot):
        table = tables[slot, 0]
        rank_column = jnp.transpose(ranks(table))
        weight_column = jnp.transpose(table)
        column = lax.broadcasted_iota(jnp.int32, (count, experts_total), 1)
        mixed_in = jnp.zeros((count, width), f32)
        for cc in relays[slot]:
            links.arrived(("hall", slot, cc), (1 + cc) * size_of(hid.at[slot, 3, 0]), core)
            for qy in range(2):
                results = [
                    jnp.dot(
                        hid[slot, 2 * qy + qx, cc] if qx + qy + cc else hid_own[slot, 0],
                        down[cc, 2 * qy + qx],
                        preferred_element_type=f32,
                    ).astype(bf16)
                    for qx in range(2)
                ]
                expert = (
                    plane * pair_count
                    + flip_index(core_place, cc) * 2
                    + flip_index(tp_place // 2, qy)
                )
                this = column == expert
                rank = jnp.sum(jnp.where(this, rank_column, 0.0), axis=1, keepdims=True)
                weight = jnp.sum(jnp.where(this, weight_column, 0.0), axis=1, keepdims=True)
                place = (slot_in == rank).astype(f32).astype(bf16)
                both = jnp.dot(place, results[0], preferred_element_type=f32) + jnp.dot(
                    place, results[1], preferred_element_type=f32
                )
                mixed_in = mixed_in + both * weight
        return mixed_in

    tokens = [pl.ds(p * (count // PARTS), count // PARTS) for p in range(PARTS)]

    def send_back(slot):
        value = partial(slot)
        if slot == 0:
            mixed[...] += value
            return
        part_own[slot] = value
        part_send[slot] = value.astype(bf16)
        for p, span in enumerate(tokens):
            links.send(
                ("e", slot, p),
                part_send.at[slot, span],
                part_in.at[slot - 1, span],
                near,
                ("pe", slot, p),
                "end",
            )

    def pass_back(slot):
        for p, span in enumerate(tokens):
            if slot == 0:
                links.arrived(("pm", 1, p), part_in.at[0, span], near, "end")
                links.arrived(("pe", 1, p), part_in.at[0, span], near, "mid")
                links.arrived(("pm", 2, p), part_in.at[3, span], far, "mid")
                continue
            source = 4 if slot == 1 else slot - 1
            if slot == 1:
                links.arrived(("pm", 3, p), part_in.at[source, span], far, "mid")
            else:
                links.arrived(("pe", slot, p), part_in.at[source, span], near, "mid")

            @pl.when(is_mid)
            def _():
                total = part_own[slot, span] + part_in[source, span].astype(f32)
                part_send[slot, span] = total.astype(bf16)

            block = part_send.at[slot, span]
            if slot == 1:
                links.send(("m", 1, p), block, part_in.at[0, span], near, ("pm", 1, p), "mid")
            else:
                target = part_in.at[1 + slot, span]
                links.send(("m", slot, p), block, target, far, ("pm", slot, p), "mid")
        if slot == 0:
            total = mixed[...] + part_in[0].astype(f32)
            out_ref[...] = total.astype(bf16)

            @pl.when(is_mid)
            def _():
                out_ref[...] = (total + part_in[3].astype(f32)).astype(bf16)

    def start_rows():
        for part in range(2):
            line_start(("row", part), rows_at(part))

    steps = {
        "start": start_rows,
        "z": take,
        "p1": share,
        "p2": share_on,
        "pz": share_end,
        "zp": take_wide,
        "x1": spread,
        "x2": spread_on,
        "c3": spread_end,
        "hid": hidden,
        "hs": hid_send,
        "hr": hid_relay,
        "part": send_back,
        "red": pass_back,
    }
    loads[1].wait()
    loads[2].wait()
    links.arrived("downc", down.at[1], core)
    for step, *where in ORDER:
        steps[step](*where)
    links.settle()


def local_fused(
    query_proj,
    key_proj,
    value_proj,
    query_gain,
    key_gain,
    residual,
    out_weight,
    route_expert,
    route_weight,
    expert_gate,
    expert_up,
    expert_down,
):
    token_count, width = query_proj.shape
    local_kv = key_gain.shape[0]
    total = out_weight.shape[0]
    hidden_units = expert_gate.shape[2]
    experts_total = lax.axis_size("sp") * lax.axis_size("tp") // 2
    capacity = 3 * token_count * TOP_K // (2 * experts_total)
    f32, bf16 = jnp.float32, jnp.bfloat16

    vmem = pl.BlockSpec(memory_space=pltpu.VMEM)
    hbm = pl.BlockSpec(memory_space=pl.ANY)
    halves = local_kv // 2
    inputs = (
        query_proj,
        key_proj,
        value_proj,
        query_gain,
        key_gain,
        residual,
        route_expert.T,
        route_weight.T,
    )
    scratch = [pltpu.VMEM(value.shape, value.dtype) for value in inputs]
    scratch += [
        pltpu.VMEM((halves, SLOTS, 2, 2, token_count, LANES), bf16),
        pltpu.VMEM((local_kv, 2 * token_count, LANES), bf16),
        pltpu.VMEM((local_kv, 1, 2 * token_count), f32),
        pltpu.VMEM((local_kv, LANES + 16, 2 * token_count), f32),
        pltpu.VMEM((token_count, total), bf16),
        pltpu.VMEM((token_count, width), f32),
        pltpu.VMEM((SLOTS, 2, token_count, total), bf16),
        pltpu.VMEM((total, width), bf16),
        pltpu.VMEM((total, 2 * hidden_units), bf16),
        pltpu.VMEM((2, 4, hidden_units, width), bf16),
        pltpu.VMEM((SLOTS, 2, experts_total, token_count), f32),
        pltpu.VMEM((SLOTS, 4, 2, capacity, hidden_units), bf16),
        pltpu.VMEM((SLOTS, 2, capacity, hidden_units), bf16),
        pltpu.VMEM((SLOTS, token_count, width), f32),
        pltpu.VMEM((SLOTS, token_count, width), bf16),
        pltpu.VMEM((5, token_count, width), bf16),
        pltpu.SemaphoreType.DMA((12,)),
        pltpu.SemaphoreType.DMA((SEND_SEMS,)),
        pltpu.SemaphoreType.DMA((RECV_SEMS,)),
    ]
    result = pl.pallas_call(
        fused_kernel,
        out_shape=jax.ShapeDtypeStruct((token_count, width), bf16),
        in_specs=[hbm] * 12,
        out_specs=vmem,
        scratch_shapes=scratch,
        compiler_params=pltpu.CompilerParams(
            collective_id=0, has_side_effects=True, vmem_limit_bytes=56 * 1024 * 1024
        ),
    )(*inputs, out_weight, expert_gate, expert_up, expert_down)
    return result


def takes_fused(mesh):
    chips = mesh.shape["sp"] // 2
    experts_total = mesh.shape["sp"] * mesh.shape["tp"] // 2
    return mesh.shape["tp"] == 4 and chips == SLOTS and experts_total == 2 * TOP_K


def solution(mesh):
    in_specs = (
        P("sp", "tp"),
        P("sp", "tp"),
        P("sp", "tp"),
        P("tp", None),
        P("tp", None),
        P("sp", "tp"),
        P(None, "tp"),
        P("sp", None),
        P("sp", None),
        P(("sp", "tp"), None, None),
        P(("sp", "tp"), None, None),
        P(("sp", "tp"), None, None),
    )
    out_specs = P("sp", "tp")
    body = local_fused if takes_fused(mesh) else local
    return jax.shard_map(body, mesh=mesh, in_specs=in_specs, out_specs=out_specs, check_vma=False)
```

```python
import functools
import math

import jax
import jax.numpy as jnp
from jax import lax
from jax.experimental import pallas as pl
from jax.experimental.pallas import tpu as pltpu
from jax.sharding import PartitionSpec as P

HEAD_DIM = 64
TOP_K = 8
GRID_W = 64


EPSILON = 1e-06
ROPE_BASE = 10000.0
KEY_BLOCK = 1024


def rotation_tables(offset, count):
    pair_count = HEAD_DIM // 4
    position = offset + jnp.arange(count, dtype=jnp.int32)
    grid_row = (position // GRID_W).astype(jnp.float32)
    grid_col = (position % GRID_W).astype(jnp.float32)
    inverse = ROPE_BASE ** (-jnp.arange(pair_count, dtype=jnp.float32) / pair_count)
    angles = jnp.stack([grid_row[:, None] * inverse, grid_col[:, None] * inverse], axis=1)
    return (jnp.cos(angles), jnp.sin(angles))


def rotate(vectors, cosine_table, sine_table):
    pair_count = HEAD_DIM // 4
    shaped = vectors.reshape(vectors.shape[:-1] + (2, 2, pair_count))
    first_half = shaped[..., 0, :]
    second_half = shaped[..., 1, :]
    cosine_row = cosine_table[:, None]
    sine_row = sine_table[:, None]
    turned = jnp.stack(
        [
            first_half * cosine_row - second_half * sine_row,
            first_half * sine_row + second_half * cosine_row,
        ],
        axis=-2,
    )
    return turned.reshape(vectors.shape)


def head_norm(vectors, gain):
    scaled = vectors.astype(jnp.float32)
    scaled = scaled * lax.rsqrt(jnp.mean(scaled * scaled, axis=-1, keepdims=True) + EPSILON)
    return scaled * gain


def online_update(running, query_groups, key_block, value_block):
    running_max, running_sum, running_acc = running
    scores = jnp.einsum(
        "tkgd,nkd->kgtn", query_groups, key_block, preferred_element_type=jnp.float32
    ) * HEAD_DIM ** (-0.5)
    new_max = jnp.maximum(running_max, jnp.max(scores, axis=-1))
    rescale = jnp.exp(running_max - new_max)
    weights = jnp.exp(scores - new_max[..., None]).astype(jnp.bfloat16)
    new_sum = running_sum * rescale + jnp.sum(weights.astype(jnp.float32), axis=-1)
    update = jnp.einsum("kgtn,nkd->kgtd", weights, value_block, preferred_element_type=jnp.float32)
    return (new_max, new_sum, running_acc * rescale[..., None] + update)


def local(
    query_proj,
    key_proj,
    value_proj,
    query_gain,
    key_gain,
    residual,
    out_weight,
    route_expert,
    route_weight,
    expert_gate,
    expert_up,
    expert_down,
):
    token_count = query_proj.shape[0]
    local_heads = query_gain.shape[0]
    local_kv = key_gain.shape[0]
    group_size = local_heads // local_kv
    sp_size = lax.axis_size("sp")
    tp_size = lax.axis_size("tp")
    tp_place = lax.axis_index("tp")
    offset = lax.axis_index("sp") * token_count
    cosine_table, sine_table = rotation_tables(offset, token_count)
    query_rot = rotate(
        head_norm(query_proj.reshape(token_count, local_heads, HEAD_DIM), query_gain),
        cosine_table,
        sine_table,
    ).astype(jnp.bfloat16)
    key_rot = rotate(
        head_norm(key_proj.reshape(token_count, local_kv, HEAD_DIM), key_gain),
        cosine_table,
        sine_table,
    ).astype(jnp.bfloat16)
    packed = jnp.concatenate(
        [key_rot.reshape(token_count, local_kv * HEAD_DIM), value_proj], axis=1
    )
    query_groups = query_rot.reshape(token_count, local_kv, group_size, HEAD_DIM)
    initial = (
        jnp.full((local_kv, group_size, token_count), -1e30, jnp.float32),
        jnp.zeros((local_kv, group_size, token_count), jnp.float32),
        jnp.zeros((local_kv, group_size, token_count, HEAD_DIM), jnp.float32),
    )
    incoming = lax.all_gather(packed, "sp", axis=0, tiled=True)
    incoming_len = incoming.shape[0]
    step_len = math.gcd(incoming_len, KEY_BLOCK)

    def one_step(step_index, running):
        block_rows = lax.dynamic_slice_in_dim(incoming, step_index * step_len, step_len, 0)
        key_block = block_rows[:, : local_kv * HEAD_DIM].reshape(step_len, local_kv, HEAD_DIM)
        value_block = block_rows[:, local_kv * HEAD_DIM :].reshape(step_len, local_kv, HEAD_DIM)
        return online_update(running, query_groups, key_block, value_block)

    final_max, final_sum, final_acc = lax.fori_loop(0, incoming_len // step_len, one_step, initial)
    attended = final_acc / final_sum[..., None]
    attended = jnp.transpose(attended, (2, 0, 1, 3)).reshape(token_count, local_heads * HEAD_DIM)
    attended = attended.astype(jnp.bfloat16)
    projected = jnp.dot(
        lax.all_gather(attended, "tp", axis=1, tiled=True),
        out_weight,
        preferred_element_type=jnp.float32,
    )
    mixed_sum = residual.astype(jnp.float32) + projected
    mixed_rows = mixed_sum.astype(jnp.bfloat16)
    full_rows = lax.all_gather(mixed_rows, "tp", axis=1, tiled=True)
    width_total = full_rows.shape[1]
    per_sp = tp_size // 2
    column = tp_place // 2
    experts_total = per_sp * sp_size
    capacity = 3 * token_count * TOP_K // (2 * experts_total)
    slot_count = sp_size * capacity
    flat_choice = route_expert.reshape(token_count * TOP_K)
    onehot = (flat_choice[:, None] == jnp.arange(experts_total, dtype=jnp.int32)[None, :]).astype(
        jnp.int32
    )
    earlier = jnp.cumsum(onehot, axis=0) - onehot
    slot_rank = jnp.sum(earlier * onehot, axis=1)
    mine = flat_choice % per_sp == column
    target = flat_choice // per_sp * capacity + slot_rank
    owner = jnp.arange(token_count * TOP_K, dtype=jnp.int32) // TOP_K
    slot_token = (
        jnp.full((slot_count + 1,), token_count, jnp.int32)
        .at[jnp.where(mine, target, slot_count)]
        .set(owner)[:slot_count]
    )
    padded = jnp.concatenate([full_rows, jnp.zeros((1, width_total), jnp.bfloat16)], axis=0)
    selected = padded[slot_token].reshape(sp_size, capacity, width_total)
    arrived = lax.all_to_all(selected, "sp", split_axis=0, concat_axis=0, tiled=True)
    expert_rows = arrived.reshape(slot_count, width_total)
    squares = jnp.mean(jnp.square(expert_rows.astype(jnp.float32)), axis=-1, keepdims=True)
    norm_scale = lax.rsqrt(squares + EPSILON)
    gate_value = (
        jnp.dot(expert_rows, expert_gate[0], preferred_element_type=jnp.float32) * norm_scale
    )
    up_value = jnp.dot(expert_rows, expert_up[0], preferred_element_type=jnp.float32) * norm_scale
    hidden = (jax.nn.silu(gate_value) * up_value).astype(jnp.bfloat16)
    half_result = jnp.dot(hidden, expert_down[0], preferred_element_type=jnp.float32).astype(
        jnp.bfloat16
    )
    returned = lax.all_to_all(
        half_result.reshape(sp_size, capacity, width_total),
        "sp",
        split_axis=0,
        concat_axis=0,
        tiled=True,
    )
    slot_results = returned.reshape(slot_count, width_total)
    mine_grid = mine.reshape(token_count, TOP_K)
    target_grid = target.reshape(token_count, TOP_K)
    gathered_sum = jnp.zeros((token_count, width_total), jnp.float32)
    for choice_index in range(TOP_K):
        chosen = mine_grid[:, choice_index]
        index = jnp.where(chosen, target_grid[:, choice_index], 0)
        factor = jnp.where(chosen, route_weight[:, choice_index], 0.0)
        picked = slot_results[index].astype(jnp.float32)
        gathered_sum = gathered_sum + factor[:, None] * picked
    routed = lax.psum_scatter(
        gathered_sum.astype(jnp.bfloat16), "tp", scatter_dimension=1, tiled=True
    ).astype(jnp.float32)
    return (mixed_sum + routed).astype(jnp.bfloat16)


def flip_index(index, mask):
    bit = 1
    while bit <= mask:
        if mask & bit:
            index = index + bit - 2 * bit * ((index // bit) % 2)
        bit *= 2
    return index


LANES = 128
SLOTS = 4
SEND_SEMS = 11
RECV_SEMS = 104
PARTS = 4
ORDER = (
    ("start",),
    ("p1",),
    ("x1", 0),
    ("z", 2, 0, "mid"),
    ("p2",),
    ("z", 1, 0, None),
    ("z", 1, 1, None),
    ("z", 2, 1, "mid"),
    ("x1", 1),
    ("z", 3, 0, "mid"),
    ("z", 3, 1, "mid"),
    ("pz",),
    ("z", 2, 0, "end"),
    ("z", 2, 1, "end"),
    ("x1", 2),
    ("z", 3, 0, "end"),
    ("x2", 0),
    ("z", 3, 1, "end"),
    ("x1", 3),
    ("zp", 1, None),
    ("x2", 2),
    ("x2", 1),
    ("zp", 2, "mid"),
    ("x2", 3),
    ("zp", 3, "mid"),
    ("c3", 2),
    ("zp", 2, "end"),
    ("c3", 0),
    ("hid", 2, 0),
    ("hs", 2, 0),
    ("hid", 2, 1),
    ("hs", 2, 1),
    ("c3", 1),
    ("zp", 3, "end"),
    ("c3", 3),
    ("hid", 3, 0),
    ("hs", 3, 0),
    ("hid", 3, 1),
    ("hs", 3, 1),
    ("hr", 3, 0),
    ("hid", 0, 1),
    ("hr", 3, 1),
    ("hr", 2, 1),
    ("hr", 2, 0),
    ("hid", 1, 1),
    ("hid", 1, 0),
    ("hs", 1, 0),
    ("hs", 1, 1),
    ("part", 3),
    ("hs", 0, 1),
    ("hid", 0, 0),
    ("part", 2),
    ("hr", 1, 0),
    ("hr", 1, 1),
    ("hs", 0, 0),
    ("red", 3),
    ("part", 1),
    ("red", 1),
    ("hr", 0, 1),
    ("hr", 0, 0),
    ("red", 2),
    ("part", 0),
    ("red", 0),
)


class Links:
    def __init__(self, send_sem, recv_sem, conditions, counting):
        self.send_sem, self.recv_sem = send_sem, recv_sem
        self.conditions, self.counting = conditions, counting
        self.recv_ids = {}
        self.groups, self.open_group = [], {}

    def copy(self, src, dst, device, send_id, recv_key):
        recv_id = self.recv_ids.setdefault(recv_key, len(self.recv_ids))
        assert recv_id < RECV_SEMS and send_id < SEND_SEMS
        return pltpu.make_async_remote_copy(
            src_ref=src,
            dst_ref=dst,
            send_sem=self.send_sem.at[send_id],
            recv_sem=self.recv_sem.at[recv_id],
            device_id=device,
            device_id_type=pl.DeviceIdType.MESH,
        )

    def counted(self, size):
        lines, width = self.counting.shape
        line = width * 2
        assert size % line == 0 and size // line <= lines
        return self.counting.at[pl.ds(0, size // line), :]

    def send(self, key, src, dst, device, recv_key=None, only=None):
        size = math.prod(src.shape) * jnp.dtype(src.dtype).itemsize
        group = self.open_group.get(only)
        if group is None or self.groups[group][0] + size > math.prod(self.counting.shape) * 2:
            group = self.open_group[only] = len(self.groups)
            self.groups.append([0, only, device])
        self.groups[group][0] += size
        copy = self.copy(src, dst, device, group, key if recv_key is None else recv_key)
        self.when(only, copy.start)

    def arrived(self, key, dst, device, only=None):
        if isinstance(dst, int):
            dst = self.counted(dst)
        self.when(only, self.copy(dst, dst, device, 0, key).wait_recv)

    def settle(self):
        for group, (size, only, device) in enumerate(self.groups):
            block = self.counted(size)
            self.when(only, self.copy(block, block, device, group, next(iter(self.recv_ids))).wait_send)

    def when(self, only, act):
        if only is None:
            act()
        else:
            pl.when(self.conditions[only])(act)


def fused_kernel(
    q_hbm,
    k_hbm,
    v_hbm,
    q_gain_hbm,
    k_gain_hbm,
    residual_hbm,
    expert_hbm,
    weight_hbm,
    out_weight_hbm,
    gate_hbm,
    up_hbm,
    down_hbm,
    out_ref,
    q_ref,
    k_ref,
    v_ref,
    q_gain_ref,
    k_gain_ref,
    residual_ref,
    expert_ref,
    weight_ref,
    kv,
    queries,
    run_max,
    run_acc,
    attended,
    mixed,
    rows,
    out_weight,
    gate_up,
    down,
    tables,
    hid,
    hid_own,
    part_own,
    part_send,
    part_in,
    local_sem,
    send_sem,
    recv_sem,
):
    f32, bf16 = jnp.float32, jnp.bfloat16
    count, width = q_hbm.shape
    pairs = width // LANES
    halves = pairs // 2
    hidden_units = gate_hbm.shape[2]
    capacity = hid.shape[3]
    upper_tok, lower_tok = pl.ds(0, count // 2), pl.ds(count // 2, count // 2)
    shared = count // 4
    rest = count - shared
    plane_tok, line_tok = pl.ds(0, shared), pl.ds(shared, rest)
    plane_half = [pl.ds(p * (shared // 2), shared // 2) for p in range(2)]
    line_half = [pl.ds(shared + p * (rest // 2), rest // 2) for p in range(2)]
    upper_cap, lower_cap = pl.ds(0, capacity // 2), pl.ds(capacity // 2, capacity // 2)

    sp_place, tp_place = lax.axis_index("sp"), lax.axis_index("tp")
    plane, core_place = sp_place // 2, sp_place % 2
    is_mid = (plane == 1) | (plane == 2)
    is_end = (plane == 0) | (plane == 3)

    def at(sp_mask, tp_mask):
        return {"sp": flip_index(sp_place, sp_mask), "tp": flip_index(tp_place, tp_mask)}

    core, near, far = at(1, 0), at(2, 0), at(6, 0)
    across = [None, at(0, 1), at(0, 2), at(0, 3)]
    across_core = [core, at(1, 1), at(1, 2)]
    links = Links(send_sem, recv_sem, {"mid": is_mid, "end": is_end}, out_weight)

    def size_of(ref):
        return math.prod(ref.shape) * jnp.dtype(ref.dtype).itemsize


    quarters = [flip_index(tp_place, q) * width for q in range(4)]

    def columns(q):
        return pl.ds(pl.multiple_of(quarters[q], width), width)

    inputs = [
        (k_hbm, k_ref),
        (k_gain_hbm, k_gain_ref),
        (v_hbm, v_ref),
        (q_hbm, q_ref),
        (q_gain_hbm, q_gain_ref),
        (expert_hbm, expert_ref),
        (weight_hbm, weight_ref),
        (residual_hbm, residual_ref),
    ]
    inputs = [
        pltpu.make_async_copy(src, dst, local_sem.at[4 + i]) for i, (src, dst) in enumerate(inputs)
    ]
    loads = [
        pltpu.make_async_copy(out_weight_hbm, out_weight, local_sem.at[0]),
        pltpu.make_async_copy(
            gate_hbm.at[0], gate_up.at[:, pl.ds(0, hidden_units)], local_sem.at[1]
        ),
        pltpu.make_async_copy(
            up_hbm.at[0], gate_up.at[:, pl.ds(hidden_units, hidden_units)], local_sem.at[2]
        ),
        pltpu.make_async_copy(down_hbm.at[0, :, columns(0)], down.at[0, 0], local_sem.at[3]),
    ]

    for load in inputs:
        load.start()
    barrier = pltpu.get_barrier_semaphore()
    partners = [core, near, far] + across[1:] + across_core[1:]
    for partner in partners:
        pl.semaphore_signal(
            barrier, inc=1, device_id=partner, device_id_type=pl.DeviceIdType.MESH
        )

    lane = lax.broadcasted_iota(jnp.int32, (count, LANES), 1)
    first_head = lane < HEAD_DIM
    quarter = HEAD_DIM // 4
    even_quarter = (lane // quarter) % 2 == 0

    grid_rows = count // GRID_W
    token = lax.broadcasted_iota(jnp.int32, (GRID_W + 8, LANES), 0)
    lane_short = lax.broadcasted_iota(jnp.int32, (GRID_W + 8, LANES), 1)
    place = jnp.where(token < GRID_W, token, sp_place * grid_rows + token - GRID_W)
    power = (lane_short % quarter).astype(f32) * (-math.log(ROPE_BASE) / quarter)
    angle = place.astype(f32) * jnp.exp(power)
    sign = jnp.where((lane_short // quarter) % 2 == 0, -1.0, 1.0)

    def over_tokens(short):
        parts = []
        by_row = ((lane_short[:GRID_W] // quarter) % 4) < 2
        for r in range(grid_rows):
            line = short[GRID_W + r : GRID_W + r + 1, :]
            parts.append(jnp.where(by_row, line, short[:GRID_W, :]))
        return jnp.concatenate(parts, axis=0)

    cosine = over_tokens(jnp.cos(angle))
    sine = over_tokens(jnp.sin(angle) * sign)

    def pair_gain(gain_ref, pair):
        return jnp.concatenate(
            [gain_ref[2 * pair : 2 * pair + 1, :], gain_ref[2 * pair + 1 : 2 * pair + 2, :]],
            axis=1,
        )

    def norm_rotate(block, gain):
        wide = block.astype(f32)
        squares = wide * wide
        low = jnp.sum(jnp.where(first_head, squares, 0.0), axis=-1, keepdims=True)
        high = jnp.sum(jnp.where(first_head, 0.0, squares), axis=-1, keepdims=True)
        mean = jnp.where(first_head, low, high) * (1.0 / HEAD_DIM)
        scaled = wide * lax.rsqrt(mean + EPSILON) * gain
        ahead = pltpu.roll(scaled, LANES - quarter, 1)
        behind = pltpu.roll(scaled, quarter, 1)
        swapped = jnp.where(even_quarter, ahead, behind)
        return scaled * cosine + swapped * sine

    for load in inputs[:3]:
        load.wait()
    for h in range(halves):
        block = pl.ds(h * LANES, LANES)
        flipped = jnp.transpose(v_ref[:, block].astype(f32)).astype(bf16)
        for part in range(count // LANES):
            kv[h, 0, 0, 1, pl.ds(part * LANES, LANES), :] = flipped[
                :, part * LANES : (part + 1) * LANES
            ]
        kv[h, 0, 0, 0] = norm_rotate(k_ref[:, block], pair_gain(k_gain_ref, h)).astype(bf16)

    pl.semaphore_wait(barrier, len(partners))

    def line_start(name, ref_at):
        links.send(None, ref_at(0), ref_at(1), near, (*name, 1))
        links.send(None, ref_at(0), ref_at(2), far, (*name, 2), "mid")

    def line_on(name, slot, ref_at, only=None):
        if only == "end":
            return
        if slot == 1:
            links.send(None, ref_at(1), ref_at(3), far, (*name, 3), "mid")
        else:
            links.send(None, ref_at(slot), ref_at(slot), near, (*name, slot), "mid")

    def line_wait(name, slot, ref_at, only=None):
        links.arrived((*name, slot), ref_at(slot), near, only)
        line_on(name, slot, ref_at, only)

    def kv_at(h):
        return lambda slot: kv.at[h, slot, 0]

    def kv_swap(h, slot, only=None):
        links.send(("kvc", h, slot), kv.at[h, slot, 0], kv.at[h, slot, 1], core, only=only)

    def table_at(slot):
        return tables.at[slot, 0]

    def table_swap(slot, only=None):
        links.send(("kvc", halves - 1, slot), tables.at[slot, 0], tables.at[slot, 1], core, only=only)

    def take_kv(h, slot, only=None):
        last = h == halves - 1
        size = size_of(kv_at(h)(slot)) + (size_of(table_at(slot)) if last else 0)
        links.arrived(("kv", h, slot), size, near, only)
        line_on(("kv", h), slot, kv_at(h), only)
        kv_swap(h, slot, only)
        if last:
            line_on(("kv", h), slot, table_at, only)
            table_swap(slot, only)

    for h in range(halves):
        line_start(("kv", h), kv_at(h))
    for h in range(halves):
        kv_swap(h, 0)
    experts_total = tables.shape[2]
    for load in inputs[5:]:
        load.wait()
    names, factors = expert_ref[...], weight_ref[...]
    wanted = lax.broadcasted_iota(jnp.int32, (experts_total, count), 0)
    table = jnp.zeros((experts_total, count), f32)
    for k in range(TOP_K):
        table = table + jnp.where(names[k : k + 1, :] == wanted, factors[k : k + 1, :], 0.0)
    tables[0, 0] = table
    line_start(("kv", halves - 1), table_at)
    table_swap(0)
    for q in (1, 2, 3):
        links.send("down", down_hbm.at[0, :, columns(q)], down.at[0, q], across[q])
    for load in loads:
        load.start()

    for load in inputs[3:5]:
        load.wait()
    for g in range(pairs):
        turned = norm_rotate(q_ref[:, pl.ds(g * LANES, LANES)], pair_gain(q_gain_ref, g))
        turned = turned.astype(bf16).astype(f32)
        other = pltpu.roll(turned, HEAD_DIM, 1)
        if g % 2 == 0:
            top, bottom = jnp.where(first_head, turned, 0.0), jnp.where(first_head, other, 0.0)
        else:
            top, bottom = jnp.where(first_head, 0.0, other), jnp.where(first_head, 0.0, turned)
        queries[g, pl.ds(0, count), :] = top.astype(bf16)
        queries[g, pl.ds(count, count), :] = bottom.astype(bf16)

    ones = jnp.ones((16, 2 * count), bf16)
    exponent = math.log2(math.e) * HEAD_DIM ** (-0.5)

    def attend(h, slot, sides=(0, 1)):
        held = len(sides) * count

        def one(i, carry):
            g = 2 * h + i
            keys = jnp.concatenate([kv[h, slot, side, 0] for side in sides], axis=0)
            values = [
                kv[h, slot, side, 1, pl.ds(part * LANES, LANES), :]
                for side in sides
                for part in range(count // LANES)
            ]
            values = jnp.concatenate(values, axis=1)
            values = jnp.concatenate([values, ones[:, :held]], axis=0)
            scores = lax.dot_general(
                keys, queries[g], (((1,), (1,)), ((), ())), preferred_element_type=f32
            )
            block_max = jnp.max(scores, axis=0, keepdims=True)
            if slot == 0:
                new_max = block_max
            else:
                old_max = run_max[g]
                new_max = jnp.maximum(old_max, block_max)
            weights = jnp.exp2((scores - new_max) * exponent).astype(bf16)
            update = jnp.dot(values, weights, preferred_element_type=f32)
            if slot:
                rescale = jnp.exp2((old_max - new_max) * exponent)
                update = update + run_acc[g] * rescale
            run_max[g] = new_max
            run_acc[g] = update
            return carry

        if slot == SLOTS - 1 and h == halves - 1 and 1 in sides:
            for i in range(2):
                one(i, 0)
                attend_end(h, (i,))
        else:
            lax.fori_loop(0, 2, one, 0)

    def own_half(q, h):
        offset = quarters[q] + h * 2 * LANES
        return pl.ds(pl.multiple_of(offset, 2 * LANES), 2 * LANES)

    def head_columns(q, g):
        return pl.ds(pl.multiple_of(quarters[q] + g * LANES, LANES), LANES)

    def attend_end(h, heads=(0, 1)):
        for i in heads:
            g = 2 * h + i
            total = run_acc[g]
            out = total[i * HEAD_DIM : (i + 1) * HEAD_DIM] / total[LANES : LANES + 1]
            pair = jnp.concatenate([out[:, :count], out[:, count:]], axis=0)
            attended[:, head_columns(0, g)] = jnp.transpose(pair).astype(bf16)
            block = attended.at[:, head_columns(0, g)]
            for q in (1, 2):
                links.send(None, block, block, across[q], ("att", g, q))

    def attend_relay(g):
        links.arrived(("att", g, 2), attended.at[:, head_columns(2, g)], across[2])
        block = attended.at[upper_tok, head_columns(2, g)]
        links.send(None, block, block, across[1], ("att", g, 3))
        links.arrived(("att", g, 1), attended.at[:, head_columns(1, g)], across[1])
        block = attended.at[lower_tok, head_columns(1, g)]
        links.send(None, block, block, across[2], ("att", g, 3))

    def attend_chunk(h, slot):
        size = size_of(kv.at[h, slot, 1])
        if h == halves - 1:
            size += size_of(tables.at[slot, 1])
        if slot == 0:
            links.arrived(("kvc", h, slot), size, core)
            attend(h, slot)
            return
        attend(h, slot, (0,))
        links.arrived(("kvc", h, slot), size, core)
        attend(h, slot, (1,))

    attend_chunk(0, 0)
    take_kv(0, 1)
    take_kv(0, 2, "mid")
    attend_chunk(1, 0)
    take_kv(1, 1)
    take_kv(1, 2, "mid")
    attend_chunk(0, 1)
    attend_chunk(1, 1)
    take_kv(0, 2, "end")
    attend_chunk(0, 2)
    take_kv(0, 3, "mid")
    take_kv(1, 2, "end")
    attend_chunk(1, 2)
    loads[3].wait()
    links.arrived("down", down.at[0, pl.ds(1, 3)], core)
    links.send("downc", down.at[0], down.at[1], core)
    take_kv(1, 3, "mid")
    take_kv(0, 3, "end")
    attend_chunk(0, 3)
    attend_end(0)
    take_kv(1, 3, "end")
    attend_chunk(1, 3)

    loads[0].wait()
    mixed[...] = residual_ref[...].astype(f32)

    def project(q, h):
        mixed[...] += jnp.dot(
            attended[:, own_half(q, h)],
            out_weight[own_half(q, h), :],
            preferred_element_type=f32,
        )

    for h in range(halves):
        project(0, h)
    for g in range(pairs):
        attend_relay(g)
        if g % 2:
            project(1, g // 2)
            project(2, g // 2)
    for g in range(pairs):
        links.arrived(("att", g, 3), attended.at[:, head_columns(3, g)], across[3])
        if g % 2:
            project(3, g // 2)
    rows[0, 0, :, columns(0)] = mixed[...].astype(bf16)

    def rows_at(part):
        return lambda slot: rows.at[slot, 0, line_half[part], columns(0)]

    def wide_at(slot):
        return rows.at[slot, 0, plane_tok, :]

    def to_core(slot, q):
        links.send(
            ("rowc", slot),
            rows.at[slot, 0, line_tok, columns(q)],
            rows.at[slot, 1, line_tok, columns(q)],
            core,
        )

    def wide_to_core(slot, only=None):
        links.send(
            ("rowc", slot), wide_at(slot), rows.at[slot, 1, plane_tok, :], core, only=only
        )

    def spread_one(name, slot, span):
        block = rows.at[slot, 0, span, columns(0)]
        links.send((name, "x1", slot), block, block, across[1])
        links.send((name, "y1", slot), block, block, across[2])

    def spread_two(name, slot, span, half):
        links.arrived((name, "y1", slot), rows.at[slot, 0, span, columns(2)], across[2])
        block = rows.at[slot, 0, half[0], columns(2)]
        links.send((name, "xy", slot), block, block, across[1])
        links.arrived((name, "x1", slot), rows.at[slot, 0, span, columns(1)], across[1])
        block = rows.at[slot, 0, half[1], columns(1)]
        links.send((name, "xy", slot), block, block, across[2])

    def spread_three(name, slot, span):
        links.arrived((name, "xy", slot), rows.at[slot, 0, span, columns(3)], across[3])

    def spread(slot):
        spread_one("row", slot, line_tok)
        to_core(slot, 0)

    def spread_on(slot):
        spread_two("row", slot, line_tok, line_half)
        to_core(slot, 1)
        to_core(slot, 2)

    def spread_end(slot):
        spread_three("row", slot, line_tok)
        to_core(slot, 3)

    def take(slot, part, only=None):
        line_wait(("row", part), slot, rows_at(part), only)

    def share():
        spread_one("wide", 0, plane_tok)

    def share_on():
        spread_two("wide", 0, plane_tok, plane_half)

    def share_end():
        spread_three("wide", 0, plane_tok)
        line_start(("wide",), wide_at)
        wide_to_core(0)

    def take_wide(slot, only=None):
        line_wait(("wide",), slot, wide_at, only)
        wide_to_core(slot, only)

    before = lax.broadcasted_iota(jnp.int32, (count, count), 0) < lax.broadcasted_iota(
        jnp.int32, (count, count), 1
    )
    before = before.astype(f32).astype(bf16)

    def ranks(table):
        chosen = table > 0.0
        marks = chosen.astype(f32).astype(bf16)
        rank = jnp.dot(marks, before, preferred_element_type=f32)
        return jnp.where(chosen, rank, -1.0)

    slot_of = lax.broadcasted_iota(jnp.int32, (capacity, count), 0).astype(f32)
    slot_in = lax.broadcasted_iota(jnp.int32, (count, capacity), 1).astype(f32)
    pair_count = experts_total // SLOTS
    my_expert = plane * pair_count + core_place * 2 + tp_place // 2
    expert_row = lax.broadcasted_iota(jnp.int32, (experts_total, count), 0)

    def hidden(slot, side):
        if side:
            links.arrived(("rowc", slot), rows.at[slot, 1], core)
        block = rows[slot, side]
        wide = block.astype(f32)
        squares = jnp.mean(wide * wide, axis=-1, keepdims=True)
        norm_scale = lax.rsqrt(squares + EPSILON)
        both = jnp.dot(block, gate_up[...], preferred_element_type=f32) * norm_scale
        gate_value, up_value = both[:, :hidden_units], both[:, hidden_units:]
        result = (gate_value / (1.0 + jnp.exp(-gate_value)) * up_value).astype(bf16)
        rank = ranks(tables[slot, side])
        mine = jnp.sum(jnp.where(expert_row == my_expert, rank, 0.0), axis=0, keepdims=True)
        pick = (slot_of == mine).astype(f32).astype(bf16)
        packed = jnp.dot(pick, result, preferred_element_type=f32).astype(bf16)
        hid_own[slot, side] = packed

    def hid_send(slot, side):
        for q in (1, 2):
            links.send(
                ("h", slot, q, side),
                hid_own.at[slot, side],
                hid.at[slot, q, side],
                (across, across_core)[side][q],
            )
        if side:
            links.send(None, hid_own.at[slot, 1], hid.at[slot, 0, 1], core, ("hall", slot, 1))

    def hid_relay(slot, cc):
        links.arrived(("h", slot, 2, cc), hid.at[slot, 2, cc], across[2])
        links.send(
            ("hall", slot, cc),
            hid.at[slot, 2, cc, upper_cap, :],
            hid.at[slot, 3, cc, upper_cap, :],
            across[1],
        )
        links.arrived(("h", slot, 1, cc), hid.at[slot, 1, cc], across[1])
        links.send(
            ("hall", slot, cc),
            hid.at[slot, 1, cc, lower_cap, :],
            hid.at[slot, 3, cc, lower_cap, :],
            across[2],
        )

    relays = {slot: [] for slot in range(SLOTS)}
    for step, *where in ORDER:
        if step == "hr":
            relays[where[0]].append(where[1])

    def partial(slot):
        table = tables[slot, 0]
        rank_column = jnp.transpose(ranks(table))
        weight_column = jnp.transpose(table)
        column = lax.broadcasted_iota(jnp.int32, (count, experts_total), 1)
        mixed_in = jnp.zeros((count, width), f32)
        for cc in relays[slot]:
            links.arrived(("hall", slot, cc), (1 + cc) * size_of(hid.at[slot, 3, 0]), core)
            for qy in range(2):
                results = [
                    jnp.dot(
                        hid[slot, 2 * qy + qx, cc] if qx + qy + cc else hid_own[slot, 0],
                        down[cc, 2 * qy + qx],
                        preferred_element_type=f32,
                    ).astype(bf16)
                    for qx in range(2)
                ]
                expert = (
                    plane * pair_count
                    + flip_index(core_place, cc) * 2
                    + flip_index(tp_place // 2, qy)
                )
                this = column == expert
                rank = jnp.sum(jnp.where(this, rank_column, 0.0), axis=1, keepdims=True)
                weight = jnp.sum(jnp.where(this, weight_column, 0.0), axis=1, keepdims=True)
                place = (slot_in == rank).astype(f32).astype(bf16)
                both = jnp.dot(place, results[0], preferred_element_type=f32) + jnp.dot(
                    place, results[1], preferred_element_type=f32
                )
                mixed_in = mixed_in + both * weight
        return mixed_in

    tokens = [pl.ds(p * (count // PARTS), count // PARTS) for p in range(PARTS)]

    def send_back(slot):
        value = partial(slot)
        if slot == 0:
            mixed[...] += value
            return
        part_own[slot] = value
        part_send[slot] = value.astype(bf16)
        for p, span in enumerate(tokens):
            links.send(
                ("e", slot, p),
                part_send.at[slot, span],
                part_in.at[slot - 1, span],
                near,
                ("pe", slot, p),
                "end",
            )

    def pass_back(slot):
        for p, span in enumerate(tokens):
            if slot == 0:
                links.arrived(("pm", 1, p), part_in.at[0, span], near, "end")
                links.arrived(("pe", 1, p), part_in.at[0, span], near, "mid")
                links.arrived(("pm", 2, p), part_in.at[3, span], far, "mid")
                continue
            source = 4 if slot == 1 else slot - 1
            if slot == 1:
                links.arrived(("pm", 3, p), part_in.at[source, span], far, "mid")
            else:
                links.arrived(("pe", slot, p), part_in.at[source, span], near, "mid")

            @pl.when(is_mid)
            def _():
                total = part_own[slot, span] + part_in[source, span].astype(f32)
                part_send[slot, span] = total.astype(bf16)

            block = part_send.at[slot, span]
            if slot == 1:
                links.send(("m", 1, p), block, part_in.at[0, span], near, ("pm", 1, p), "mid")
            else:
                target = part_in.at[1 + slot, span]
                links.send(("m", slot, p), block, target, far, ("pm", slot, p), "mid")
        if slot == 0:
            total = mixed[...] + part_in[0].astype(f32)
            out_ref[...] = total.astype(bf16)

            @pl.when(is_mid)
            def _():
                out_ref[...] = (total + part_in[3].astype(f32)).astype(bf16)

    def start_rows():
        for part in range(2):
            line_start(("row", part), rows_at(part))

    steps = {
        "start": start_rows,
        "z": take,
        "p1": share,
        "p2": share_on,
        "pz": share_end,
        "zp": take_wide,
        "x1": spread,
        "x2": spread_on,
        "c3": spread_end,
        "hid": hidden,
        "hs": hid_send,
        "hr": hid_relay,
        "part": send_back,
        "red": pass_back,
    }
    loads[1].wait()
    loads[2].wait()
    links.arrived("downc", down.at[1], core)
    for step, *where in ORDER:
        steps[step](*where)
    links.settle()


def local_fused(
    query_proj,
    key_proj,
    value_proj,
    query_gain,
    key_gain,
    residual,
    out_weight,
    route_expert,
    route_weight,
    expert_gate,
    expert_up,
    expert_down,
):
    token_count, width = query_proj.shape
    local_kv = key_gain.shape[0]
    total = out_weight.shape[0]
    hidden_units = expert_gate.shape[2]
    experts_total = lax.axis_size("sp") * lax.axis_size("tp") // 2
    capacity = 3 * token_count * TOP_K // (2 * experts_total)
    f32, bf16 = jnp.float32, jnp.bfloat16

    vmem = pl.BlockSpec(memory_space=pltpu.VMEM)
    hbm = pl.BlockSpec(memory_space=pl.ANY)
    halves = local_kv // 2
    inputs = (
        query_proj,
        key_proj,
        value_proj,
        query_gain,
        key_gain,
        residual,
        route_expert.T,
        route_weight.T,
    )
    scratch = [pltpu.VMEM(value.shape, value.dtype) for value in inputs]
    scratch += [
        pltpu.VMEM((halves, SLOTS, 2, 2, token_count, LANES), bf16),
        pltpu.VMEM((local_kv, 2 * token_count, LANES), bf16),
        pltpu.VMEM((local_kv, 1, 2 * token_count), f32),
        pltpu.VMEM((local_kv, LANES + 16, 2 * token_count), f32),
        pltpu.VMEM((token_count, total), bf16),
        pltpu.VMEM((token_count, width), f32),
        pltpu.VMEM((SLOTS, 2, token_count, total), bf16),
        pltpu.VMEM((total, width), bf16),
        pltpu.VMEM((total, 2 * hidden_units), bf16),
        pltpu.VMEM((2, 4, hidden_units, width), bf16),
        pltpu.VMEM((SLOTS, 2, experts_total, token_count), f32),
        pltpu.VMEM((SLOTS, 4, 2, capacity, hidden_units), bf16),
        pltpu.VMEM((SLOTS, 2, capacity, hidden_units), bf16),
        pltpu.VMEM((SLOTS, token_count, width), f32),
        pltpu.VMEM((SLOTS, token_count, width), bf16),
        pltpu.VMEM((5, token_count, width), bf16),
        pltpu.SemaphoreType.DMA((12,)),
        pltpu.SemaphoreType.DMA((SEND_SEMS,)),
        pltpu.SemaphoreType.DMA((RECV_SEMS,)),
    ]
    result = pl.pallas_call(
        fused_kernel,
        out_shape=jax.ShapeDtypeStruct((token_count, width), bf16),
        in_specs=[hbm] * 12,
        out_specs=vmem,
        scratch_shapes=scratch,
        compiler_params=pltpu.CompilerParams(
            collective_id=0, has_side_effects=True, vmem_limit_bytes=56 * 1024 * 1024
        ),
    )(*inputs, out_weight, expert_gate, expert_up, expert_down)
    return result


def takes_fused(mesh):
    chips = mesh.shape["sp"] // 2
    experts_total = mesh.shape["sp"] * mesh.shape["tp"] // 2
    return mesh.shape["tp"] == 4 and chips == SLOTS and experts_total == 2 * TOP_K


def solution(mesh):
    in_specs = (
        P("sp", "tp"),
        P("sp", "tp"),
        P("sp", "tp"),
        P("tp", None),
        P("tp", None),
        P("sp", "tp"),
        P(None, "tp"),
        P("sp", None),
        P("sp", None),
        P(("sp", "tp"), None, None),
        P(("sp", "tp"), None, None),
        P(("sp", "tp"), None, None),
    )
    out_specs = P("sp", "tp")
    body = local_fused if takes_fused(mesh) else local
    return jax.shard_map(body, mesh=mesh, in_specs=in_specs, out_specs=out_specs, check_vma=False)
```
